256 devices in a mesh: sp: 32 (over z, x), fs: 4 (over y), tp: 2 (over core).
Axes of the slice: x: 4, y: 4, z: 8, core: 2. Of those that a mesh axis runs over, the one named last changes fastest.
Arguments:
- tokens: bfloat16 [4, 8192, 2048], P('fs', 'sp', 'tp'), may hold values from -6 to 6
- norm_gain: float32 [2048], replicated, may hold values from 0.1 to 1.9
- query_weight: bfloat16 [2048, 1024], P(('sp', 'fs'), 'tp'), may hold values from -0.125 to 0.125
- forget_weight: bfloat16 [2048, 1024], P(('sp', 'fs'), 'tp'), may hold values from -0.125 to 0.125
- value_weight: bfloat16 [2048, 1024], P(('sp', 'fs'), 'tp'), may hold values from -0.125 to 0.125
- outgate_weight: bfloat16 [2048, 1024], P(('sp', 'fs'), 'tp'), may hold values from -0.125 to 0.125
- pool_in_weight: bfloat16 [2048, 1024], P(('sp', 'fs'), 'tp'), may hold values from -0.125 to 0.125
- forget_room: float32 [1024], P('tp'), may hold values from 0 to 0.06
- decay_shift: float32 [4, 8192, 8], P('fs', 'sp', 'tp'), may hold values from -0.6 to 0
- head_gain: float32 [128], replicated, may hold values from 0.1 to 1.9
- start_state: float32 [4, 8, 128, 128], P('fs', 'tp'), may hold values from -0.03314563 to 0.03314563
- pool_map: bfloat16 [4, 256, 256], P('tp'), may hold values from -0.375 to 0.375
- pool_scale: float32 [1024], P('tp'), may hold values from 0.1 to 1.9
- out_rec_weight: bfloat16 [1024, 2048], P('tp', ('sp', 'fs')), may hold values from -0.125 to 0.125
- out_pool_weight: bfloat16 [1024, 2048], P('tp', ('sp', 'fs')), may hold values from -0.125 to 0.125
Outputs:
- mixed: bfloat16 [4, 8192, 2048], P('fs', ('sp', 'tp'))
The draws below stay inside these ranges and needn't reach their ends.
All inputs are finite; a program needn't handle non-finite values.
Results may differ from the reference program's by a relative error of at most 0.013.
Values may be sent and summed in bfloat16 or wider, within the bound.
A program may use at most 128 MiB of HBM per device.

```python
import jax
import jax.numpy as jnp
from jax import lax

D = 2048
REC_HEADS = 8
HEAD = 128
POOL_GROUPS = 4
POOL_DIM = 256
D_REC = 1024
D_POOL = 1024
WIDEST = 16
TOK_DEV = 256
BLOCK = 128
STREAM_EXTENT = 8192
SEQUENCE_COUNT = 4
N_TP = 2


def fast_heads(key):
    uniforms = jax.random.uniform(jax.random.fold_in(key, 11), (REC_HEADS,))
    return uniforms < 0.5


def draw_forget_room(key, part):
    fast_mask = fast_heads(key)
    spread = jax.random.uniform(jax.random.fold_in(key, 1), (REC_HEADS, HEAD))
    slow_room = 0.3 * jnp.exp(spread * jnp.log(4.0)) / STREAM_EXTENT
    fast_room = 0.02 * jnp.exp(spread * jnp.log(3.0))
    return jnp.where(fast_mask[:, None], fast_room, slow_room).reshape(REC_HEADS * HEAD).astype(jnp.float32)


def draw_decay_shift(key, part):
    fast_mask = fast_heads(key)
    device_blocks = STREAM_EXTENT // TOK_DEV
    spread = jax.random.uniform(jax.random.fold_in(key, 2), (SEQUENCE_COUNT, device_blocks, REC_HEADS))
    factor = jnp.exp(spread * jnp.log(4.0))
    fading_rate = jnp.where(fast_mask[None, None, :], 0.005 * factor, 0.15 * factor / STREAM_EXTENT)
    fading_rate = jnp.repeat(fading_rate, TOK_DEV, axis=1)
    pulse_locations = jax.random.randint(jax.random.fold_in(key, 3), (SEQUENCE_COUNT, 2), 0, STREAM_EXTENT)
    criterion_parts = jnp.log(0.6 + 0.2 * jax.random.uniform(jax.random.fold_in(key, 4), (SEQUENCE_COUNT, 2, REC_HEADS)))
    pulse_consensus = (jnp.arange(STREAM_EXTENT)[None, :, None] == pulse_locations[:, None, :]).astype(jnp.float32)
    pulse_markers = jnp.einsum('ydw,ywu->ydu', pulse_consensus, criterion_parts)
    return (pulse_markers - fading_rate).astype(jnp.float32)


def block_scale(rng, shape, pieces, smallest, high):
    level = 1.0
    for dim, shards_of in pieces:
        draws = jax.random.uniform(jax.random.fold_in(jax.random.fold_in(rng, 6), dim), (shards_of,), jnp.float32, smallest / len(pieces), high / len(pieces))
        level = level * jnp.repeat(jnp.exp(draws), shape[dim] // shards_of).reshape((-1,) + (1,) * (len(shape) - 1 - dim))
    return level


def noise(key, dims, deviation, most, pieces=(), held_as=jnp.bfloat16):
    values = deviation * jax.random.normal(key, dims, jnp.float32)
    if pieces:
        values = values * block_scale(key, dims, pieces, -0.22, 0.18)
    return jnp.clip(values, -most, most).astype(held_as)


def setup_inputs(seed: int = 0) -> dict:
    arg_keys = jax.random.split(jax.random.key(seed), 16)
    return {
        "tokens": noise(arg_keys[0], (SEQUENCE_COUNT, STREAM_EXTENT, D), 1.0, 6.0, ((0, 4), (1, 32), (2, 2))),
        "norm_gain": jnp.clip(1.0 + 0.18 * jax.random.normal(arg_keys[1], (D,), jnp.float32), 0.1, 1.9),
        "query_weight": noise(arg_keys[2], (D, D_REC), D ** -0.5, 0.125, ((0, 128), (1, 2))),
        "forget_weight": noise(arg_keys[3], (D, D_REC), D ** -0.5, 0.125, ((0, 128), (1, 2))),
        "value_weight": noise(arg_keys[4], (D, D_REC), D ** -0.5, 0.125, ((0, 128), (1, 2))),
        "outgate_weight": noise(arg_keys[5], (D, D_REC), D ** -0.5, 0.125, ((0, 128), (1, 2))),
        "pool_in_weight": noise(arg_keys[6], (D, D_POOL), D ** -0.5, 0.125, ((0, 128), (1, 2))),
        "forget_room": draw_forget_room(jax.random.fold_in(arg_keys[15], 71), 0),
        "decay_shift": draw_decay_shift(jax.random.fold_in(arg_keys[15], 71), 0),
        "head_gain": jnp.clip(1.0 + 0.18 * jax.random.normal(arg_keys[9], (HEAD,), jnp.float32), 0.1, 1.9),
        "start_state": noise(arg_keys[10], (SEQUENCE_COUNT, REC_HEADS, HEAD, HEAD), (0.5 * STREAM_EXTENT ** -0.5), 0.03314563, ((0, 4), (1, 2)), jnp.float32),
        "pool_map": noise(arg_keys[11], (POOL_GROUPS, POOL_DIM, POOL_DIM), POOL_DIM ** -0.5, 0.375, ((0, 2),)),
        "pool_scale": jnp.clip(1.0 + 0.18 * jax.random.normal(arg_keys[12], (D_POOL,), jnp.float32), 0.1, 1.9),
        "out_rec_weight": noise(arg_keys[13], (D_REC, D), (D_REC + D_POOL) ** -0.5, 0.125, ((0, 2), (1, 128))),
        "out_pool_weight": noise(arg_keys[14], (D_POOL, D), (D_REC + D_POOL) ** -0.5, 0.125, ((0, 2), (1, 128))),
    }


EPSILON = 1e-06

def rms_scale(entry_vectors):
    return lax.rsqrt(lax.optimization_barrier(jnp.mean(entry_vectors * entry_vectors, axis=-1, keepdims=True)) + EPSILON)

def rounded(entry_vectors):
    return lax.optimization_barrier(entry_vectors.astype(jnp.bfloat16)).astype(jnp.float32)

def recurrence(query_rows, forget_logits, value_rows, outgate, forget_room, lagged_tokens, head_gain, memory_start):
    length = query_rows.shape[0]
    head_count = query_rows.shape[1] // HEAD
    blocks = length // BLOCK
    queries = jax.nn.silu(query_rows.astype(jnp.float32)) * HEAD ** (-0.5)
    keyed = forget_room[None, :] * (1.0 - jax.nn.sigmoid(forget_logits.astype(jnp.float32)))
    log_decay = jnp.log1p(-keyed).reshape(length, head_count, HEAD) + lagged_tokens[:, :, None]

    def to_blocks(entry_vectors):
        return entry_vectors.reshape(blocks, BLOCK, head_count, HEAD).transpose(0, 2, 1, 3)
    causal = jnp.tril(jnp.ones((BLOCK, BLOCK), jnp.float32))

    def advance(memory, inputs):
        query_block, key_block, value_block, decay_block = inputs
        within = jnp.cumsum(decay_block, axis=1)
        centre = within[:, BLOCK // 2 - 1:BLOCK // 2]
        ending = within[:, BLOCK - 1:BLOCK]
        scores = jnp.einsum('hcd,hsd->hcs', rounded(query_block * jnp.exp(within - centre)), rounded(key_block * jnp.exp(centre - within))) * causal
        inside = jnp.einsum('hcs,hse->hce', rounded(scores), value_block)
        carried = jnp.einsum('hcd,hde->hce', rounded(query_block * jnp.exp(within)), rounded(memory))
        added = jnp.einsum('hcd,hce->hde', rounded(key_block * jnp.exp(ending - within)), value_block)
        memory = jnp.exp(ending[:, 0, :])[:, :, None] * memory + added
        return (memory, inside + carried)
    inputs = (to_blocks(queries), to_blocks(keyed), to_blocks(value_rows.astype(jnp.float32)), to_blocks(log_decay.reshape(length, head_count * HEAD)))
    _, outputs = lax.scan(advance, memory_start, inputs)
    outputs = outputs.transpose(0, 2, 1, 3).reshape(length, head_count, HEAD)
    gating = jax.nn.silu(outgate.astype(jnp.float32)).reshape(length, head_count, HEAD)
    result = outputs * rms_scale(outputs) * head_gain * gating
    return result.reshape(length, head_count * HEAD).astype(jnp.bfloat16)

def pooling(pool_input, pool_map, pool_scale):
    length = pool_input.shape[0]
    columns = pool_input.shape[1]
    entry_vectors = pool_input.astype(jnp.float32)
    front_filled = jnp.concatenate([jnp.zeros((WIDEST, columns), jnp.float32), entry_vectors], axis=0)
    group_index = (jnp.arange(columns, dtype=jnp.int32) // POOL_DIM).astype(jnp.int32)
    reach = jnp.left_shift(jnp.int32(2), group_index)
    window_sum = jnp.zeros((length, columns), jnp.float32)
    for offset in range(WIDEST):
        window_sum = window_sum + front_filled[WIDEST - offset:WIDEST - offset + length] * (offset < reach).astype(jnp.float32)
    position = jnp.arange(length, dtype=jnp.int32)
    amount = jnp.minimum(position[:, None] + 1, reach[None, :]).astype(jnp.float32)
    pooled = (window_sum / amount - entry_vectors).astype(jnp.bfloat16)
    mapped = jnp.einsum('tgc,gcd->tgd', pooled.reshape(length, POOL_GROUPS, POOL_DIM).astype(jnp.float32), pool_map.astype(jnp.float32))
    return (mapped.reshape(length, columns) * pool_scale).astype(jnp.bfloat16)

def reference(tokens, norm_gain, query_weight, forget_weight, value_weight, outgate_weight, pool_in_weight, forget_room, decay_shift, head_gain, start_state, pool_map, pool_scale, out_rec_weight, out_pool_weight):
    rec_part = D_REC // N_TP
    pool_part = D_POOL // N_TP

    def one_sequence(inputs):
        token_rows, lagged_tokens, memory_start = inputs
        widened = token_rows.astype(jnp.float32)
        rescaled_input = (widened * rms_scale(widened) * norm_gain).astype(jnp.bfloat16)
        projected = [jnp.dot(rescaled_input, weight, preferred_element_type=jnp.float32).astype(jnp.bfloat16) for weight in (query_weight, forget_weight, value_weight, outgate_weight, pool_in_weight)]
        rec_out = recurrence(projected[0], projected[1], projected[2], projected[3], forget_room, lagged_tokens, head_gain, memory_start)
        pool_out = pooling(projected[4], pool_map, pool_scale)
        summed = jnp.zeros((token_rows.shape[0], D), jnp.float32)
        for device_part in range(N_TP):
            partial_rows = jnp.dot(rec_out[:, device_part * rec_part:(device_part + 1) * rec_part], out_rec_weight[device_part * rec_part:(device_part + 1) * rec_part], preferred_element_type=jnp.float32)
            partial_rows = partial_rows + jnp.dot(pool_out[:, device_part * pool_part:(device_part + 1) * pool_part], out_pool_weight[device_part * pool_part:(device_part + 1) * pool_part], preferred_element_type=jnp.float32)
            summed = summed + partial_rows.astype(jnp.bfloat16).astype(jnp.float32)
        return summed.astype(jnp.bfloat16)
    return lax.map(one_sequence, (tokens, decay_shift, start_state))
```

```python
import jax
import jax.numpy as jnp
from jax import lax
from jax.experimental import pallas as pl
from jax.experimental.pallas import tpu as pltpu
from jax.sharding import Mesh
from jax.sharding import PartitionSpec as P

HEAD = 128
POOL_DIM = 256
BLOCK = 128
SP_FS = ("sp_0", "sp_1", "fs")
SP = ("sp_0", "sp_1")
SP_TP = ("sp_0", "sp_1", "tp")
EPSILON = 1e-06
MESH = pl.DeviceIdType.MESH
NSEM = 160
NZ, NX, NF = 8, 4, 4
WX1, WZ1, WX2, WZ2 = 256, 384, 384, 640
F32, BF16 = jnp.float32, jnp.bfloat16
NT = (((1,), (1,)), ((), ()))
TN = (((0,), (0,)), ((), ()))


def dot(a, b, dims=(((1,), (0,)), ((), ()))):
    return lax.dot_general(a, b, dims, preferred_element_type=F32)


def pack_state(state, decay):
    high = decay.astype(BF16).astype(F32)
    rest = decay - high
    mid = rest.astype(BF16).astype(F32)
    low = rest - mid
    row = lax.broadcasted_iota(jnp.int32, (16, HEAD), 0)
    tail = jnp.where(row == 0, high, jnp.where(row == 1, mid, jnp.where(row == 2, low, 0.0)))
    return jnp.concatenate([state, tail], axis=0).astype(BF16)


def unpack_state(packed):
    whole = packed.astype(F32)
    decay = jnp.sum(whole[HEAD : HEAD + 16], axis=0, keepdims=True)
    return whole[:HEAD], decay


def kernel(
    tok,
    ix1,
    iz1,
    ix2,
    iz2,
    room,
    shift,
    hgain,
    start,
    out,
    T,
    GX1,
    GZ1,
    GX2,
    GZ2,
    SH,
    ST,
    K,
    V,
    Q,
    G,
    C,
    QE,
    INS,
    A0,
    SL,
    SR,
    ZS,
    ZR,
    ES,
    ER,
    EXT,
    BS,
    BR,
    RO,
    PO,
    ACT,
    PS,
    PR,
    send_sems,
    recv_sems,
):
    z, x = lax.axis_index("sp_0"), lax.axis_index("sp_1")
    f, c = lax.axis_index("fs"), lax.axis_index("tp")
    zat = lambda k: lax.rem(z + (k + NZ), NZ)
    xat = lambda k: lax.rem(x + (k + NX), NX)
    fat = lambda k: lax.rem(f + (k + NF), NF)
    other = 1 - c
    here = z * NX + x
    after = lax.rem(here + 1, NZ * NX)
    ahead = lax.rem(here + NZ * NX - 1, NZ * NX)
    nxt = {"sp_0": after // NX, "sp_1": lax.rem(after, NX)}
    prv = {"sp_0": ahead // NX, "sp_1": lax.rem(ahead, NX)}

    barrier = pltpu.get_barrier_semaphore()
    met = [{"tp": other}, nxt, prv]
    met += [{"fs": fat(k)} for k in (1, 2, 3)] + [{"sp_1": xat(k)} for k in (1, 2, 3)]
    met += [{"sp_0": zat(k)} for k in range(1, NZ)]
    for who in met:
        pl.semaphore_signal(barrier, inc=1, device_id=who, device_id_type=MESH)

    count = [0]
    sent = []

    def sem():
        count[0] += 1
        assert count[0] <= NSEM
        return count[0] - 1

    def copy(n, src, dst, who):
        return pltpu.make_async_remote_copy(
            src_ref=src,
            dst_ref=dst,
            send_sem=send_sems.at[n],
            recv_sem=recv_sems.at[n],
            device_id=who,
            device_id_type=MESH,
        )

    def send(n, src, dst, who):
        made = copy(n, src, dst, who)
        made.start()
        sent.append(made)

    def landed(n, dst, who):
        copy(n, dst, dst, who).wait_recv()

    mine = pl.ds(pl.multiple_of(f * 16, 16), 16)
    for buffer, own in ((GX1, ix1), (GZ1, iz1), (GX2, ix2), (GZ2, iz2)):
        buffer[z, x, mine, :] = own[f]
    T[c, f] = tok[...]
    SH[f] = shift[...]

    pl.semaphore_wait(barrier, len(met))

    def over_y(pairs):
        waits = []
        for k in (1, 3, 2):
            to = fat(k)
            for buffer, own in pairs:
                n = sem()
                send(n, own.at[to], buffer.at[z, x, mine, :], {"fs": to})
                theirs = pl.ds(pl.multiple_of(fat(-k) * 16, 16), 16)
                waits.append((n, buffer.at[z, x, theirs, :], {"fs": to}))
        return waits

    y1 = over_y(((GX1, ix1), (GZ1, iz1)))
    shift_waits = []
    for k in (1, 3, 2):
        n = sem()
        send(n, shift, SH.at[f], {"fs": fat(k)})
        shift_waits.append((n, SH.at[fat(-k)], {"fs": fat(k)}))

    first, second = pl.ds(0, 128), pl.ds(128, 128)
    relay_waits = []

    def relay(seq, rows):
        n = sem()
        send(n, T.at[c, seq, rows, :], T.at[c, seq, rows, :], {"tp": other})
        relay_waits.append((n, T.at[other, seq, rows, :], {"tp": other}))

    right, left = {"fs": fat(1)}, {"fs": fat(3)}
    tr = [sem(), sem(), sem()]
    tl = [sem(), sem(), sem()]
    for i, (a, b) in enumerate(((first, second), (second, first))):
        send(tr[i], tok.at[a, :], T.at[c, f, a, :], right)
        send(tl[i], tok.at[b, :], T.at[c, f, b, :], left)
    n = sem()
    send(n, tok, T.at[c, f], {"tp": other})
    relay_waits.append((n, T.at[other, f], {"tp": other}))

    def token_steps():
        landed(tr[0], T.at[c, fat(-1), first, :], right)
        send(tr[2], T.at[c, fat(-1), first, :], T.at[c, fat(-1), first, :], right)
        relay(fat(-1), first)
        landed(tl[0], T.at[c, fat(1), second, :], left)
        send(tl[2], T.at[c, fat(1), second, :], T.at[c, fat(1), second, :], left)
        relay(fat(1), second)
        yield
        landed(tr[1], T.at[c, fat(-1), second, :], right)
        relay(fat(-1), second)
        landed(tl[1], T.at[c, fat(1), first, :], left)
        relay(fat(1), first)
        yield
        landed(tr[2], T.at[c, fat(-2), first, :], right)
        relay(fat(-2), first)
        landed(tl[2], T.at[c, fat(2), second, :], left)
        relay(fat(2), second)
        yield

    def plane(GX, GZ, waits):
        zr, zl = {"sp_0": zat(1)}, {"sp_0": zat(-1)}
        xr, xl = {"sp_1": xat(1)}, {"sp_1": xat(-1)}
        low, high = pl.ds(0, 32), pl.ds(32, 32)
        lowx, highx = pl.ds(0, 2), pl.ds(2, 2)
        for w in waits:
            landed(*w)
        xs = []
        for k in (1, 3, 2):
            n = sem()
            send(n, GX.at[z, x], GX.at[z, x], {"sp_1": xat(k)})
            xs.append((n, GX.at[z, xat(-k)], {"sp_1": xat(k)}))
        nr, nl = [sem() for _ in range(4)], [sem() for _ in range(4)]
        send(nr[0], GZ.at[z, x], GZ.at[z, x], zr)
        send(nl[0], GZ.at[z, x], GZ.at[z, x], zl)
        forwards = []
        last = []

        def spread(offset):
            at = zat(offset)
            a, b, e = sem(), sem(), sem()
            send(a, GZ.at[at, x], GZ.at[at, x], xr)
            send(b, GZ.at[at, x], GZ.at[at, x], xl)
            forwards.append((offset, a, b, e))

        def forward():
            for offset, a, b, e in forwards:
                at = zat(offset)
                landed(a, GZ.at[at, xat(-1)], xr)
                if 0 <= offset < 4:
                    send(e, GZ.at[at, xat(-1)], GZ.at[at, xat(-1)], xr)
                landed(b, GZ.at[at, xat(1)], xl)
                if not 0 <= offset < 4:
                    send(e, GZ.at[at, xat(1)], GZ.at[at, xat(1)], xl)
                last.append((e, GZ.at[at, xat(2)], xr))
            forwards.clear()

        spread(0)
        yield
        for w in xs:
            landed(*w)
        mr, ml = [sem() for _ in range(4)], [sem() for _ in range(4)]
        send(mr[0], GX.at[z], GX.at[z], zr)
        send(ml[0], GX.at[z], GX.at[z], zl)
        for k in (1, 2, 3, 4):
            back, front = zat(-k), zat(k)
            if k < 4:
                landed(nr[k - 1], GZ.at[back, x], zr)
                rows = (GZ.at[back, x], GZ.at[back, x, low, :])[k == 3]
                send(nr[k], rows, rows, zr)
                landed(nl[k - 1], GZ.at[front, x], zl)
                rows = (GZ.at[front, x], GZ.at[front, x, high, :])[k == 3]
                send(nl[k], rows, rows, zl)
                pending = list(forwards)
                spread(-k)
                spread(k)
                added = forwards[len(pending) :]
                forwards[:] = pending
                forward()
                forwards[:] = added
                landed(mr[k - 1], GX.at[back], zr)
                rows = (GX.at[back], GX.at[back, lowx])[k == 3]
                send(mr[k], rows, rows, zr)
                landed(ml[k - 1], GX.at[front], zl)
                rows = (GX.at[front], GX.at[front, highx])[k == 3]
                send(ml[k], rows, rows, zl)
            else:
                landed(nr[3], GZ.at[back, x, low, :], zr)
                landed(nl[3], GZ.at[back, x, high, :], zl)
                spread(4)
                forward()
                landed(mr[3], GX.at[back, lowx], zr)
                landed(ml[3], GX.at[back, highx], zl)
            yield
        for w in last:
            landed(*w)
        yield

    one = plane(GX1, GZ1, y1)
    tokens = token_steps()
    next(one)
    y2 = over_y(((GX2, ix2), (GZ2, iz2)))

    ns = [sem() for _ in range(3)]

    @pl.when(f == x)
    def _():
        ST[...] = start[f]
        for i, k in enumerate((1, 2, 3)):
            copy(ns[i], start.at[fat(k)], ST, {"fs": fat(k)}).start()

    next(one)
    next(tokens)
    next(one)
    two = plane(GX2, GZ2, y2)
    next(two)
    next(one)
    next(tokens)
    next(one)
    next(tokens)
    next(one)
    for w in relay_waits + shift_waits:
        landed(*w)

    i0 = lax.broadcasted_iota(jnp.int32, (BLOCK, BLOCK), 0)
    i1 = lax.broadcasted_iota(jnp.int32, (BLOCK, BLOCK), 1)
    causal = i0 >= i1
    tril = jnp.where(causal, 1.0, 0.0).astype(BF16)
    my_room = room[pl.ds(f, 1), :]

    def project(s, _):
        x0, x1 = T[0, s], T[1, s]
        half = NZ // 2
        pa = dot(x0, GX1[:half].reshape(1024, WX1)) + dot(x1, GX1[half:].reshape(1024, WX1))
        pb = dot(x0, GZ1[:half].reshape(1024, WZ1)) + dot(x1, GZ1[half:].reshape(1024, WZ1))
        w0, w1 = x0.astype(F32), x1.astype(F32)
        square = jnp.sum(w0 * w0 + w1 * w1, axis=1, keepdims=True)
        scale = lax.rsqrt(square * (1.0 / 2048) + EPSILON)
        pa, pb = pa * scale, pb * scale
        keys = my_room * jax.nn.sigmoid(-pa[:, :128])
        query = pa[:, 128:]
        Q[s] = query * jax.nn.sigmoid(query) * HEAD ** (-0.5)
        K[s] = keys
        value = pb[:, :128].astype(BF16)
        V[s] = value
        gate = pb[:, 128:256]
        G[s] = gate * jax.nn.sigmoid(gate) * hgain[...]
        pool = pb[:, 256:].astype(BF16)
        EXT[s, 128:384, :] = pool
        BS[s] = pool[240:256]
        lag = SH[s, pl.ds(f, 1), :]
        ends, adds = [], []
        for b in range(2):
            rows = slice(b * BLOCK, (b + 1) * BLOCK)
            lags = jnp.transpose(jnp.broadcast_to(lag[:, rows], (BLOCK, BLOCK)))
            decay = jnp.log1p(-keys[rows]) + lags
            high = decay.astype(BF16)
            rest = decay - high.astype(F32)
            mid = rest.astype(BF16)
            low = (rest - mid.astype(F32)).astype(BF16)
            within = dot(tril, high) + dot(tril, mid) + dot(tril, low)
            C[s, rows, :] = within
            end = within[BLOCK - 1 :]
            adds.append(dot(value[rows], (keys[rows] * jnp.exp(end - within)).astype(BF16), TN))
            ends.append(end)
        A0[s] = adds[0]
        SL[s] = pack_state(jnp.exp(ends[1]) * adds[0] + adds[1], ends[0] + ends[1])
        return 0

    lax.fori_loop(0, 4, project, 0)

    sx = []
    SR[x] = SL[x]
    for k in (1, 3, 2):
        n = sem()
        send(n, SL.at[xat(k)], SR.at[x], {"sp_1": xat(k)})
        sx.append((n, SR.at[xat(-k)], {"sp_1": xat(k)}))
    nb = sem()
    send(nb, BS, BR, nxt)
    next(two)

    for w in sx:
        landed(*w)
    state, decay = unpack_state(SR[0])
    for i in range(1, NX):
        later, fade = unpack_state(SR[i])
        state, decay = jnp.exp(fade) * state + later, decay + fade
    ZS[...] = pack_state(state, decay)
    sz = []
    for k in (4, 3, 5, 2, 6, 1, 7):
        n = sem()
        send(n, ZS, ZR.at[z], {"sp_0": zat(k)})
        sz.append((n, ZR.at[zat(-k)], {"sp_0": zat(k)}))

    def inner(s, _):
        for b in range(2):
            rows = slice(b * BLOCK, (b + 1) * BLOCK)
            within = C[s, rows, :]
            centre = within[BLOCK // 2 - 1 : BLOCK // 2]
            query, keys = Q[s, rows, :], K[s, rows, :]
            scores = dot(
                (query * jnp.exp(within - centre)).astype(BF16),
                (keys * jnp.exp(centre - within)).astype(BF16),
                NT,
            )
            scores = jnp.where(causal, scores, 0.0).astype(BF16)
            INS[s, rows, :] = dot(scores, V[s, rows, :])
            QE[s, rows, :] = (query * jnp.exp(within)).astype(BF16)
        return 0

    lax.fori_loop(0, 4, inner, 0)
    next(two)

    landed(nb, BR, nxt)
    span = lax.shift_left(jnp.int32(2), c * 2 + f // 2)
    ti = lax.broadcasted_iota(jnp.int32, (256, 384), 0)
    si = lax.broadcasted_iota(jnp.int32, (256, 384), 1) - 128
    band = jnp.where((si <= ti) & (si > ti - span) & (si >= -16), 1.0, 0.0).astype(BF16)
    position = here * 256 + lax.broadcasted_iota(jnp.int32, (256, 128), 0)
    amount = jnp.minimum(position + 1, span).astype(F32)

    def pool(s, _):
        EXT[s, 0:128, :] = jnp.zeros((128, 128), BF16)

        @pl.when(here > 0)
        def _():
            EXT[s, 112:128, :] = BR[s]

        window = dot(band, EXT[s])
        PO[s] = (window / amount - EXT[s, 128:384, :].astype(F32)).astype(BF16)
        return 0

    lax.fori_loop(0, 4, pool, 0)
    act_waits = []

    def give_back(buffer, slot):
        ACT[slot + f] = buffer[f]
        for k in (1, 3, 2):
            n = sem()
            send(n, buffer.at[fat(k)], ACT.at[slot + f], {"fs": fat(k)})
            act_waits.append((n, ACT.at[slot + fat(-k)], {"fs": fat(k)}))

    give_back(PO, 4)

    for w in sz:
        landed(*w)
    for i, k in enumerate((1, 2, 3)):

        @pl.when(fat(-k) == x)
        def _(i=i, k=k):
            landed(ns[i], ST, {"fs": fat(k)})

    def pass_z(i, state):
        later, fade = unpack_state(ZR[i])
        return jnp.exp(fade) * state + later

    state = lax.fori_loop(0, z, pass_z, ST[...].astype(F32))
    for i in range(NX):
        ES[i] = state.astype(BF16)
        if i < NX - 1:
            later, fade = unpack_state(SR[i])
            state = jnp.exp(fade) * state + later
    sb = []
    ER[x] = ES[x]
    for k in (1, 3, 2):
        n = sem()
        send(n, ES.at[xat(k)], ER.at[x], {"sp_1": xat(k)})
        sb.append((n, ER.at[xat(-k)], {"sp_1": xat(k)}))
    next(two)
    for w in sb:
        landed(*w)

    def finish(s, _):
        entering = ER[s].astype(F32)
        middle = jnp.exp(C[s, BLOCK - 1 : BLOCK, :]) * entering + A0[s]
        for b, state in enumerate((ER[s], middle.astype(BF16))):
            rows = slice(b * BLOCK, (b + 1) * BLOCK)
            raw = INS[s, rows, :] + dot(QE[s, rows, :], state, NT)
            square = jnp.mean(raw * raw, axis=1, keepdims=True)
            RO[s, rows, :] = (raw * lax.rsqrt(square + EPSILON) * G[s, rows, :]).astype(BF16)
        return 0

    lax.fori_loop(0, 4, finish, 0)
    give_back(RO, 0)
    next(two)
    next(two)
    for w in act_waits:
        landed(*w)

    def rows_of(core):
        rows = pl.ds(pl.multiple_of(core * 128, 128), 128)
        parts = [ACT[i, rows, :] for i in range(8)]
        return jnp.concatenate(parts[:3], axis=1), jnp.concatenate(parts[3:], axis=1)

    ax, az = rows_of(other)
    for i in range(4):
        wx = GX2[2 * i : 2 * i + 2].reshape(512, WX2)
        wz = GZ2[2 * i : 2 * i + 2].reshape(512, WZ2)
        PS[:, 512 * i : 512 * i + 512] = (dot(ax, wx, NT) + dot(az, wz, NT)).astype(BF16)
    n = sem()
    send(n, PS, PR, {"tp": other})
    ax, az = rows_of(c)
    own = []
    for i in range(4):
        wx = GX2[2 * i : 2 * i + 2].reshape(512, WX2)
        wz = GZ2[2 * i : 2 * i + 2].reshape(512, WZ2)
        own.append((dot(ax, wx, NT) + dot(az, wz, NT)).astype(BF16))
    landed(n, PR, {"tp": other})
    for i in range(4):
        cols = slice(512 * i, 512 * i + 512)
        out[:, cols] = (own[i].astype(F32) + PR[:, cols].astype(F32)).astype(BF16)

    for made in sent:
        made.wait_send()

    @pl.when(f == x)
    def _():
        for i, k in enumerate((1, 2, 3)):
            copy(ns[i], start.at[fat(k)], ST, {"fs": fat(k)}).wait_send()


def per_device(
    tokens,
    norm_gain,
    query_weight,
    forget_weight,
    value_weight,
    outgate_weight,
    pool_in_weight,
    forget_room,
    decay_shift,
    head_gain,
    start_state,
    pool_map,
    pool_scale,
    out_rec_weight,
    out_pool_weight,
):
    row = lax.axis_index(SP_FS) * 16
    gain = lax.dynamic_slice(norm_gain, (row,), (16,))[:, None]

    def split(w):
        return w.reshape(16, 4, 128).transpose(1, 0, 2)

    def scaled(w):
        return split((w.astype(F32) * gain).astype(BF16))

    folded = jnp.einsum(
        "rgc,gcd->rgd",
        pool_in_weight.reshape(16, 2, POOL_DIM),
        pool_map,
        preferred_element_type=F32,
    ).reshape(16, 512)
    pool = split((folded * gain * pool_scale[None, :]).astype(BF16))
    out_t = jnp.concatenate([out_rec_weight, out_pool_weight], axis=0).T
    out_all = jnp.broadcast_to(out_t[None], (4, 16, 1024))
    ix1 = jnp.concatenate([scaled(forget_weight), scaled(query_weight)], axis=2)
    iz1 = jnp.concatenate([scaled(value_weight), scaled(outgate_weight), pool], axis=2)
    ix2, iz2 = out_all[:, :, :WX2], out_all[:, :, WX2:]
    shift = jnp.pad(decay_shift[0].T, ((0, 4), (0, 0)))
    start = start_state[0].transpose(0, 2, 1).astype(BF16)

    vmem = lambda *shape: pltpu.VMEM(shape, F32)
    half = lambda *shape: pltpu.VMEM(shape, BF16)
    mixed = pl.pallas_call(
        kernel,
        out_shape=jax.ShapeDtypeStruct((128, 2048), BF16),
        in_specs=[pl.BlockSpec(memory_space=pltpu.VMEM)] * 9,
        out_specs=pl.BlockSpec(memory_space=pltpu.VMEM),
        scratch_shapes=[
            half(2, 4, 256, 1024),
            half(NZ, NX, 64, WX1),
            half(NZ, NX, 64, WZ1),
            half(NZ, NX, 64, WX2),
            half(NZ, NX, 64, WZ2),
            vmem(4, 8, 256),
            half(128, 128),
            vmem(4, 256, 128),
            half(4, 256, 128),
            vmem(4, 256, 128),
            vmem(4, 256, 128),
            vmem(4, 256, 128),
            half(4, 256, 128),
            vmem(4, 256, 128),
            vmem(4, 128, 128),
            half(4, 144, 128),
            half(4, 144, 128),
            half(144, 128),
            half(NZ, 144, 128),
            half(4, 128, 128),
            half(4, 128, 128),
            half(4, 384, 128),
            half(4, 16, 128),
            half(4, 16, 128),
            half(4, 256, 128),
            half(4, 256, 128),
            half(8, 256, 128),
            half(128, 2048),
            half(128, 2048),
            pltpu.SemaphoreType.DMA((NSEM,)),
            pltpu.SemaphoreType.DMA((NSEM,)),
        ],
        compiler_params=pltpu.CompilerParams(
            collective_id=0, has_side_effects=True, vmem_limit_bytes=60 * 1024 * 1024
        ),
    )(
        tokens[0],
        ix1,
        iz1,
        ix2,
        iz2,
        forget_room.reshape(4, 128),
        shift,
        head_gain.reshape(1, 128),
        start,
    )
    return mixed[None]


def solution(mesh):
    finer = Mesh(
        mesh.devices.reshape(8, 4, mesh.shape["fs"], mesh.shape["tp"]), ("sp_0", "sp_1", "fs", "tp")
    )
    placed = (
        P("fs", SP, "tp"),
        P(),
        P(SP_FS, "tp"),
        P(SP_FS, "tp"),
        P(SP_FS, "tp"),
        P(SP_FS, "tp"),
        P(SP_FS, "tp"),
        P("tp"),
        P("fs", SP, "tp"),
        P(),
        P("fs", "tp", None, None),
        P("tp", None, None),
        P("tp"),
        P("tp", SP_FS),
        P("tp", SP_FS),
    )
    return jax.shard_map(
        per_device, mesh=finer, in_specs=placed, out_specs=P("fs", SP_TP, None), check_vma=False
    )
```

```python
import jax
import jax.numpy as jnp
from jax import lax
from jax.experimental import pallas as pl
from jax.experimental.pallas import tpu as pltpu
from jax.sharding import Mesh
from jax.sharding import PartitionSpec as P

HEAD = 128
POOL_DIM = 256
BLOCK = 128
SP_FS = ("sp_0", "sp_1", "fs")
SP = ("sp_0", "sp_1")
SP_TP = ("sp_0", "sp_1", "tp")
EPSILON = 1e-06
MESH = pl.DeviceIdType.MESH
NSEM = 288
NZ, NX, NF = 8, 4, 4
WX, WZ, WB, WBX = (256, 256), (256, 128, 384), 384, 128
F32, BF16 = jnp.float32, jnp.bfloat16
NT = (((1,), (1,)), ((), ()))
TN = (((0,), (0,)), ((), ()))


def dot(a, b, dims=(((1,), (0,)), ((), ()))):
    return lax.dot_general(a, b, dims, preferred_element_type=F32)


def pack_state(state, decay):
    high, mid, low = three_parts(decay)
    row = lax.broadcasted_iota(jnp.int32, (16, HEAD), 0)
    tail = jnp.where(row == 0, high, jnp.where(row == 1, mid, jnp.where(row == 2, low, 0.0)))
    return jnp.concatenate([state, tail], axis=0).astype(BF16)


def three_parts(value):
    high = value.astype(BF16).astype(F32)
    rest = value - high
    mid = rest.astype(BF16).astype(F32)
    return high, mid, rest - mid


def unpack_state(packed):
    whole = packed.astype(F32)
    decay = jnp.sum(whole[HEAD : HEAD + 16], axis=0, keepdims=True)
    return whole[:HEAD], decay


def kernel(
    tok,
    iz1,
    ix2,
    iz2,
    ix3,
    iz3,
    ib,
    room,
    shift,
    hgain,
    start,
    out,
    T,
    GZ1,
    GX2,
    GZ2,
    GX3,
    GZ3,
    GB,
    SH,
    ST,
    K,
    V,
    Q,
    G,
    C,
    QE,
    INS,
    A0,
    SL,
    SR,
    ZS,
    ZR,
    ES,
    ER,
    EXT,
    BS,
    BR,
    RO,
    PO,
    ACT,
    PS,
    PR,
    SC,
    send_sems,
    recv_sems,
):
    z, x = lax.axis_index("sp_0"), lax.axis_index("sp_1")
    f, c = lax.axis_index("fs"), lax.axis_index("tp")
    zat = lambda k: lax.rem(z + (k + NZ), NZ)
    xat = lambda k: lax.rem(x + (k + NX), NX)
    fat = lambda k: lax.rem(f + (k + NF), NF)
    other = 1 - c
    here = z * NX + x
    after = lax.rem(here + 1, NZ * NX)
    ahead = lax.rem(here + NZ * NX - 1, NZ * NX)
    nxt = {"sp_0": after // NX, "sp_1": lax.rem(after, NX)}
    prv = {"sp_0": ahead // NX, "sp_1": lax.rem(ahead, NX)}

    barrier = pltpu.get_barrier_semaphore()
    met = [{"tp": other}, nxt, prv]
    met += [{"fs": fat(k)} for k in (1, 2, 3)] + [{"sp_1": xat(k)} for k in (1, 2, 3)]
    met += [{"sp_0": zat(k)} for k in range(1, NZ)]
    for who in met:
        pl.semaphore_signal(barrier, inc=1, device_id=who, device_id_type=MESH)

    count = [0]
    sent = []

    def sem():
        count[0] += 1
        assert count[0] <= NSEM
        return count[0] - 1

    def copy(n, src, dst, who):
        return pltpu.make_async_remote_copy(
            src_ref=src,
            dst_ref=dst,
            send_sem=send_sems.at[n],
            recv_sem=recv_sems.at[n],
            device_id=who,
            device_id_type=MESH,
        )

    def send(n, src, dst, who):
        made = copy(n, src, dst, who)
        made.start()
        sent.append(made)

    def landed(n, dst, who):
        copy(n, dst, dst, who).wait_recv()

    mine = pl.ds(pl.multiple_of(f * 16, 16), 16)
    pieces = ((GZ1, iz1), (GX2, ix2), (GZ2, iz2), (GX3, ix3), (GZ3, iz3))
    for buffer, own in pieces:
        buffer[z, x, mine, :] = own[f]
    GB[z, x, mine, :] = ib[...]
    T[c, f] = tok[...]
    SH[f] = shift[...]

    pl.semaphore_wait(barrier, len(met))

    def over_y(pairs):
        waits = []
        for k in (1, 3, 2):
            to = fat(k)
            for buffer, own in pairs:
                n = sem()
                send(n, own.at[to], buffer.at[z, x, mine, :], {"fs": to})
                theirs = pl.ds(pl.multiple_of(fat(-k) * 16, 16), 16)
                waits.append((n, buffer.at[z, x, theirs, :], {"fs": to}))
        return waits

    y1 = over_y(pieces[:1])
    y2 = over_y(pieces[1:3])
    y3 = over_y(pieces[3:])
    shift_waits = []
    for k in (1, 3, 2):
        n = sem()
        send(n, shift, SH.at[f], {"fs": fat(k)})
        shift_waits.append((n, SH.at[fat(-k)], {"fs": fat(k)}))

    first, second = pl.ds(0, 128), pl.ds(128, 128)
    relay_waits = []

    def relay(seq, rows):
        n = sem()
        send(n, T.at[c, seq, rows, :], T.at[c, seq, rows, :], {"tp": other})
        relay_waits.append((n, T.at[other, seq, rows, :], {"tp": other}))

    right, left = {"fs": fat(1)}, {"fs": fat(3)}
    tr = [sem(), sem(), sem()]
    tl = [sem(), sem(), sem()]
    for i, (a, b) in enumerate(((first, second), (second, first))):
        send(tr[i], tok.at[a, :], T.at[c, f, a, :], right)
        send(tl[i], tok.at[b, :], T.at[c, f, b, :], left)
    n = sem()
    send(n, tok, T.at[c, f], {"tp": other})
    relay_waits.append((n, T.at[other, f], {"tp": other}))

    def token_steps():
        landed(tr[0], T.at[c, fat(-1), first, :], right)
        send(tr[2], T.at[c, fat(-1), first, :], T.at[c, fat(-1), first, :], right)
        relay(fat(-1), first)
        landed(tl[0], T.at[c, fat(1), second, :], left)
        send(tl[2], T.at[c, fat(1), second, :], T.at[c, fat(1), second, :], left)
        relay(fat(1), second)
        yield
        landed(tr[1], T.at[c, fat(-1), second, :], right)
        relay(fat(-1), second)
        landed(tl[1], T.at[c, fat(1), first, :], left)
        relay(fat(1), first)
        yield
        landed(tr[2], T.at[c, fat(-2), first, :], right)
        relay(fat(-2), first)
        landed(tl[2], T.at[c, fat(2), second, :], left)
        relay(fat(2), second)
        yield

    def plane(waits, vx, vz):
        zr, zl = {"sp_0": zat(1)}, {"sp_0": zat(-1)}
        xr, xl = {"sp_1": xat(1)}, {"sp_1": xat(-1)}
        whole, lowx, highx = pl.ds(0, 4), pl.ds(0, 2), pl.ds(2, 2)
        for w in waits:
            landed(*w)
        xs = []
        for k in (1, 3, 2) if vx else ():
            n = sem()
            send(n, vx(z, x), vx(z, x), {"sp_1": xat(k)})
            xs.append((n, vx(z, xat(-k)), {"sp_1": xat(k)}))
        nr, nl = [sem() for _ in range(4)], [sem() for _ in range(4)]
        send(nr[0], vz(z, x), vz(z, x), zr)
        send(nl[0], vz(z, x), vz(z, x), zl)
        forwards = []
        last = []

        def spread(offset):
            at = zat(offset)
            a, b, e = sem(), sem(), sem()
            send(a, vz(at, x), vz(at, x), xr)
            send(b, vz(at, x), vz(at, x), xl)
            forwards.append((offset, a, b, e))

        def forward(ready):
            for offset, a, b, e in ready:
                at = zat(offset)
                landed(a, vz(at, xat(-1)), xr)
                if 0 <= offset < 4:
                    send(e, vz(at, xat(-1)), vz(at, xat(-1)), xr)
                landed(b, vz(at, xat(1)), xl)
                if not 0 <= offset < 4:
                    send(e, vz(at, xat(1)), vz(at, xat(1)), xl)
                last.append((e, vz(at, xat(2)), xr))

        spread(0)
        yield
        if vx:
            for w in xs:
                landed(*w)
            mr, ml = [sem() for _ in range(4)], [sem() for _ in range(4)]
            send(mr[0], vx(z, whole), vx(z, whole), zr)
            send(ml[0], vx(z, whole), vx(z, whole), zl)
            yield
        for k in (1, 2, 3):
            back, front = zat(-k), zat(k)
            landed(nr[k - 1], vz(back, x), zr)
            part = vz(back, x, 1 if k == 3 else 0)
            send(nr[k], part, part, zr)
            landed(nl[k - 1], vz(front, x), zl)
            part = vz(front, x, 2 if k == 3 else 0)
            send(nl[k], part, part, zl)
            ready = list(forwards)
            forwards.clear()
            spread(-k)
            spread(k)
            if vx:
                landed(mr[k - 1], vx(back, whole), zr)
                part = vx(back, lowx if k == 3 else whole)
                send(mr[k], part, part, zr)
                landed(ml[k - 1], vx(front, whole), zl)
                part = vx(front, highx if k == 3 else whole)
                send(ml[k], part, part, zl)
            forward(ready)
            yield
        far = zat(4)
        landed(nr[3], vz(far, x, 1), zr)
        landed(nl[3], vz(far, x, 2), zl)
        spread(4)
        forward(forwards)
        if vx:
            landed(mr[3], vx(far, lowx), zr)
            landed(ml[3], vx(far, highx), zl)
        yield
        for w in last:
            landed(*w)
        yield

    def views(GX, GZ):
        halves = (None, pl.ds(0, 32), pl.ds(32, 32))

        def vz(zi, xi, part=0):
            return GZ.at[zi, xi, halves[part], :] if part else GZ.at[zi, xi]

        return (GX is not None) and (lambda zi, xi: GX.at[zi, xi]), vz

    lanes = (pl.ds(WBX, WB - WBX), pl.ds(WBX, 128), pl.ds(WBX + 128, 128))
    late = plane(
        (),
        lambda zi, xi: GB.at[zi, xi, mine, pl.ds(0, WBX)],
        lambda zi, xi, part=0: GB.at[zi, xi, mine, lanes[part]],
    )

    def late_over_y():
        first, second = pl.ds(0, 4), pl.ds(4, 4)

        def part(k, half):
            rows = pl.ds(pl.multiple_of(fat(k) * 16, 16), 16)
            return GB.at[half, :, rows, :]

        br, bl = [sem() for _ in range(3)], [sem() for _ in range(3)]
        for i, (a, b) in enumerate(((first, second), (second, first))):
            send(br[i], part(0, a), part(0, a), right)
            send(bl[i], part(0, b), part(0, b), left)
        yield
        landed(br[0], part(-1, first), right)
        send(br[2], part(-1, first), part(-1, first), right)
        landed(bl[0], part(1, second), left)
        send(bl[2], part(1, second), part(1, second), left)
        yield
        landed(br[1], part(-1, second), right)
        landed(bl[1], part(1, first), left)
        landed(br[2], part(-2, first), right)
        landed(bl[2], part(2, second), left)
        yield

    one = plane(y1, *views(None, GZ1))
    two = plane(y2, *views(GX2, GZ2))
    three = plane(y3, *views(GX3, GZ3))
    tokens = token_steps()

    ns = [sem() for _ in range(3)]

    @pl.when(f == x)
    def _():
        ST[...] = start[f]
        for i, k in enumerate((1, 2, 3)):
            copy(ns[i], start.at[fat(k)], ST, {"fs": fat(k)}).start()

    next(late)
    next(one)
    next(two)
    next(late)
    next(one)
    next(tokens)
    next(one)
    next(two)
    next(late)
    next(one)
    next(tokens)
    next(one)
    next(late)
    next(two)
    next(three)
    next(one)
    for w in relay_waits + shift_waits:
        landed(*w)
    relay_waits.clear()

    i0 = lax.broadcasted_iota(jnp.int32, (BLOCK, BLOCK), 0)
    i1 = lax.broadcasted_iota(jnp.int32, (BLOCK, BLOCK), 1)
    causal = i0 >= i1
    tril = jnp.where(causal, 1.0, 0.0).astype(BF16)
    ones = jnp.ones((BLOCK, BLOCK), BF16)
    my_room = room[pl.ds(f, 1), :]

    half = NZ // 2

    def each(body):
        for s in range(4):
            body(s, 0)

    def through(s, *weights):
        low = jnp.concatenate([w[:half].reshape(1024, w.shape[-1]) for w in weights], axis=1)
        high = jnp.concatenate([w[half:].reshape(1024, w.shape[-1]) for w in weights], axis=1)
        return (dot(T[0, s], low) + dot(T[1, s], high)) * SC[s]

    def project(s, _):
        w0, w1 = T[0, s].astype(F32), T[1, s].astype(F32)
        square = jnp.sum(w0 * w0 + w1 * w1, axis=1, keepdims=True)
        SC[s] = lax.rsqrt(square * (1.0 / 2048) + EPSILON)
        both = through(s, GZ1)
        keys = my_room * jax.nn.sigmoid(-both[:, :128])
        K[s] = keys
        value = both[:, 128:].astype(BF16)
        V[s] = value
        lag = SH[s, pl.ds(f, 1), :]
        ends, adds = [], []
        for b in range(2):
            rows = slice(b * BLOCK, (b + 1) * BLOCK)
            lags = three_parts(lag[:, rows])
            spread = [jnp.where(causal, jnp.broadcast_to(p, (BLOCK, BLOCK)), 0.0).astype(BF16) for p in lags]
            parts = [p.astype(BF16) for p in three_parts(jnp.log1p(-keys[rows]))]
            within = dot(
                jnp.concatenate([tril] * 3 + spread, axis=1),
                jnp.concatenate(parts + [ones] * 3, axis=0),
            )
            C[s, rows, :] = within
            end = within[BLOCK - 1 :]
            adds.append(dot(value[rows], (keys[rows] * jnp.exp(end - within)).astype(BF16), TN))
            ends.append(end)
        A0[s] = adds[0]
        SL[s] = pack_state(jnp.exp(ends[1]) * adds[0] + adds[1], ends[0] + ends[1])
        return 0

    for k in (0, -1, 1):
        project(fat(k), 0)
    next(two)
    next(three)
    next(late)
    next(tokens)
    for w in relay_waits:
        landed(*w)
    project(fat(2), 0)

    def project_rest(s, _):
        rest = through(s, GX2, GZ2)
        query = rest[:, :128]
        Q[s] = query * jax.nn.sigmoid(query) * HEAD ** (-0.5)
        gate = rest[:, 128:256]
        G[s] = gate * jax.nn.sigmoid(gate) * hgain[...]
        pool = rest[:, 256:].astype(BF16)
        EXT[s, 128:384, :] = pool
        BS[s] = pool[240:256]
        return 0

    sx = []
    SR[x] = SL[x]
    for k in (1, 3, 2):
        n = sem()
        send(n, SL.at[xat(k)], SR.at[x], {"sp_1": xat(k)})
        sx.append((n, SR.at[xat(-k)], {"sp_1": xat(k)}))
    next(two)
    next(late)
    next(three)
    for w in sx:
        landed(*w)
    state, decay = unpack_state(SR[0])
    for i in range(1, NX):
        later, fade = unpack_state(SR[i])
        state, decay = jnp.exp(fade) * state + later, decay + fade
    ZS[...] = pack_state(state, decay)
    sz = []
    for k in (4, 3, 5, 2, 6, 1, 7):
        n = sem()
        send(n, ZS, ZR.at[z], {"sp_0": zat(k)})
        sz.append((n, ZR.at[zat(-k)], {"sp_0": zat(k)}))

    next(two)
    next(late)
    late = late_over_y()
    next(late)
    next(two)
    each(project_rest)
    nb = sem()
    send(nb, BS, BR, nxt)

    def inner(s, _):
        for b in range(2):
            rows = slice(b * BLOCK, (b + 1) * BLOCK)
            within = C[s, rows, :]
            centre = within[BLOCK // 2 - 1 : BLOCK // 2]
            query, keys = Q[s, rows, :], K[s, rows, :]
            scores = dot(
                (query * jnp.exp(within - centre)).astype(BF16),
                (keys * jnp.exp(centre - within)).astype(BF16),
                NT,
            )
            scores = jnp.where(causal, scores, 0.0).astype(BF16)
            INS[s, rows, :] = dot(scores, V[s, rows, :])
            QE[s, rows, :] = (query * jnp.exp(within)).astype(BF16)
        return 0

    each(inner)
    next(three)
    next(late)

    landed(nb, BR, nxt)
    span = lax.shift_left(jnp.int32(2), c * 2 + f // 2)
    ti = lax.broadcasted_iota(jnp.int32, (256, 384), 0)
    si = lax.broadcasted_iota(jnp.int32, (256, 384), 1) - 128
    band = jnp.where((si <= ti) & (si > ti - span) & (si >= -16), 1.0, 0.0).astype(BF16)
    position = here * 256 + lax.broadcasted_iota(jnp.int32, (256, 128), 0)
    amount = jnp.minimum(position + 1, span).astype(F32)

    def pool(s, _):
        EXT[s, 0:128, :] = jnp.zeros((128, 128), BF16)

        @pl.when(here > 0)
        def _():
            EXT[s, 112:128, :] = BR[s]

        window = dot(band, EXT[s])
        PO[s] = (window / amount - EXT[s, 128:384, :].astype(F32)).astype(BF16)
        return 0

    each(pool)
    act_waits = []

    def give_back(buffer, slot):
        ACT[slot + f] = buffer[f]
        for k in (1, 3, 2):
            n = sem()
            send(n, buffer.at[fat(k)], ACT.at[slot + f], {"fs": fat(k)})
            act_waits.append((n, ACT.at[slot + fat(-k)], {"fs": fat(k)}))

    give_back(PO, 4)

    for w in sz:
        landed(*w)
    for i, k in enumerate((1, 2, 3)):

        @pl.when(fat(-k) == x)
        def _(i=i, k=k):
            landed(ns[i], ST, {"fs": fat(k)})

    def pass_z(i, state):
        later, fade = unpack_state(ZR[i])
        return jnp.exp(fade) * state + later

    state = lax.fori_loop(0, z, pass_z, ST[...].astype(F32))
    for i in range(NX):
        ES[i] = state.astype(BF16)
        if i < NX - 1:
            later, fade = unpack_state(SR[i])
            state = jnp.exp(fade) * state + later
    sb = []
    ER[x] = ES[x]
    for k in (1, 3, 2):
        n = sem()
        send(n, ES.at[xat(k)], ER.at[x], {"sp_1": xat(k)})
        sb.append((n, ER.at[xat(-k)], {"sp_1": xat(k)}))
    next(three)
    for w in sb:
        landed(*w)

    def finish(s, _):
        entering = ER[s].astype(F32)
        middle = jnp.exp(C[s, BLOCK - 1 : BLOCK, :]) * entering + A0[s]
        for b, state in enumerate((ER[s], middle.astype(BF16))):
            rows = slice(b * BLOCK, (b + 1) * BLOCK)
            raw = INS[s, rows, :] + dot(QE[s, rows, :], state, NT)
            square = jnp.mean(raw * raw, axis=1, keepdims=True)
            RO[s, rows, :] = (raw * lax.rsqrt(square + EPSILON) * G[s, rows, :]).astype(BF16)
        return 0

    each(finish)
    give_back(RO, 0)
    next(three)
    next(three)
    next(late)
    for w in act_waits:
        landed(*w)

    a, b, d = (
        jnp.concatenate([ACT[i] for i in range(*span)], axis=1) for span in ((0, 2), (2, 5), (5, 8))
    )
    my_rows = pl.ds(pl.multiple_of(c * 128, 128), 128)
    their_rows = pl.ds(pl.multiple_of(other * 128, 128), 128)
    swaps = []
    for i in range(4):
        at, cols = slice(2 * i, 2 * i + 2), slice(512 * i, 512 * i + 512)
        total = dot(a, GX3[at].reshape(512, 256), NT)
        total += dot(b, GZ3[at].reshape(512, WZ[2]), NT)
        total += dot(d, GB[at].reshape(512, WB), NT)
        PS[:, cols] = total.astype(BF16)
        n = sem()
        send(n, PS.at[their_rows, pl.ds(512 * i, 512)], PR.at[:, pl.ds(512 * i, 512)], {"tp": other})
        swaps.append((n, PR.at[:, pl.ds(512 * i, 512)], {"tp": other}))
    for w in swaps:
        landed(*w)
    out[...] = (PS[my_rows, :].astype(F32) + PR[...].astype(F32)).astype(BF16)

    for made in sent:
        made.wait_send()

    @pl.when(f == x)
    def _():
        for i, k in enumerate((1, 2, 3)):
            copy(ns[i], start.at[fat(k)], ST, {"fs": fat(k)}).wait_send()


def per_device(
    tokens,
    norm_gain,
    query_weight,
    forget_weight,
    value_weight,
    outgate_weight,
    pool_in_weight,
    forget_room,
    decay_shift,
    head_gain,
    start_state,
    pool_map,
    pool_scale,
    out_rec_weight,
    out_pool_weight,
):
    row = lax.axis_index(SP_FS) * 16
    gain = lax.dynamic_slice(norm_gain, (row,), (16,))[:, None]

    def split(w):
        return w.reshape(16, 4, 128).transpose(1, 0, 2)

    def scaled(w):
        return split((w.astype(F32) * gain).astype(BF16))

    folded = jnp.einsum(
        "rgc,gcd->rgd",
        pool_in_weight.reshape(16, 2, POOL_DIM),
        pool_map,
        preferred_element_type=F32,
    ).reshape(16, 512)
    pool = split((folded * gain * pool_scale[None, :]).astype(BF16))
    out_t = jnp.concatenate([out_rec_weight, out_pool_weight], axis=0).T
    out_all = jnp.broadcast_to(out_t[None], (4, 16, 1024))
    iz1 = jnp.concatenate([scaled(forget_weight), scaled(value_weight)], axis=2)
    ix2 = jnp.concatenate([scaled(query_weight), scaled(outgate_weight)], axis=2)
    iz2 = pool
    ix3, iz3, ib = out_all[:, :, :256], out_all[:, :, 256:640], out_t[:, 640:]
    shift = jnp.pad(decay_shift[0].T, ((0, 4), (0, 0)))
    start = start_state[0].transpose(0, 2, 1).astype(BF16)

    vmem = lambda *shape: pltpu.VMEM(shape, F32)
    half = lambda *shape: pltpu.VMEM(shape, BF16)
    mixed = pl.pallas_call(
        kernel,
        out_shape=jax.ShapeDtypeStruct((128, 2048), BF16),
        in_specs=[pl.BlockSpec(memory_space=pltpu.VMEM)] * 11,
        out_specs=pl.BlockSpec(memory_space=pltpu.VMEM),
        scratch_shapes=[
            half(2, 4, 256, 1024),
            half(NZ, NX, 64, WZ[0]),
            half(NZ, NX, 64, WX[0]),
            half(NZ, NX, 64, WZ[1]),
            half(NZ, NX, 64, WX[1]),
            half(NZ, NX, 64, WZ[2]),
            half(NZ, NX, 64, WB),
            vmem(4, 8, 256),
            half(128, 128),
            vmem(4, 256, 128),
            half(4, 256, 128),
            vmem(4, 256, 128),
            vmem(4, 256, 128),
            vmem(4, 256, 128),
            half(4, 256, 128),
            vmem(4, 256, 128),
            vmem(4, 128, 128),
            half(4, 144, 128),
            half(4, 144, 128),
            half(144, 128),
            half(NZ, 144, 128),
            half(4, 128, 128),
            half(4, 128, 128),
            half(4, 384, 128),
            half(4, 16, 128),
            half(4, 16, 128),
            half(4, 256, 128),
            half(4, 256, 128),
            half(8, 256, 128),
            half(256, 2048),
            half(128, 2048),
            vmem(4, 256, 1),
            pltpu.SemaphoreType.DMA((NSEM,)),
            pltpu.SemaphoreType.DMA((NSEM,)),
        ],
        compiler_params=pltpu.CompilerParams(
            collective_id=0, has_side_effects=True, vmem_limit_bytes=60 * 1024 * 1024
        ),
    )(
        tokens[0],
        iz1,
        ix2,
        iz2,
        ix3,
        iz3,
        ib,
        forget_room.reshape(4, 128),
        shift,
        head_gain.reshape(1, 128),
        start,
    )
    return mixed[None]


def solution(mesh):
    finer = Mesh(
        mesh.devices.reshape(8, 4, mesh.shape["fs"], mesh.shape["tp"]), ("sp_0", "sp_1", "fs", "tp")
    )
    placed = (
        P("fs", SP, "tp"),
        P(),
        P(SP_FS, "tp"),
        P(SP_FS, "tp"),
        P(SP_FS, "tp"),
        P(SP_FS, "tp"),
        P(SP_FS, "tp"),
        P("tp"),
        P("fs", SP, "tp"),
        P(),
        P("fs", "tp", None, None),
        P("tp", None, None),
        P("tp"),
        P("tp", SP_FS),
        P("tp", SP_FS),
    )
    return jax.shard_map(
        per_device, mesh=finer, in_specs=placed, out_specs=P("fs", SP_TP, None), check_vma=False
    )
```

```python
import jax
import jax.numpy as jnp
from jax import lax
from jax.experimental import pallas as pl
from jax.experimental.pallas import tpu as pltpu
from jax.sharding import Mesh
from jax.sharding import PartitionSpec as P

HEAD = 128
POOL_DIM = 256
BLOCK = 128
SP_FS = ("sp_0", "sp_1", "fs")
SP = ("sp_0", "sp_1")
SP_TP = ("sp_0", "sp_1", "tp")
EPSILON = 1e-06
MESH = pl.DeviceIdType.MESH
NRECV, NSEND = 77, 64
NZ, NX, NF = 8, 4, 4
WX, WZ, WB, WBX = (256, 256), (256, 128, 384), 384, 128
F32, BF16 = jnp.float32, jnp.bfloat16
NT = (((1,), (1,)), ((), ()))
TN = (((0,), (0,)), ((), ()))


def dot(a, b, dims=(((1,), (0,)), ((), ()))):
    return lax.dot_general(a, b, dims, preferred_element_type=F32)


def pack_state(state, decay):
    high, mid, low = three_parts(decay)
    row = lax.broadcasted_iota(jnp.int32, (16, HEAD), 0)
    tail = jnp.where(row == 0, high, jnp.where(row == 1, mid, jnp.where(row == 2, low, 0.0)))
    return jnp.concatenate([state, tail], axis=0).astype(BF16)


def three_parts(value):
    high = value.astype(BF16).astype(F32)
    rest = value - high
    mid = rest.astype(BF16).astype(F32)
    return high, mid, rest - mid


def unpack_state(packed):
    whole = packed.astype(F32)
    decay = jnp.sum(whole[HEAD : HEAD + 16], axis=0, keepdims=True)
    return whole[:HEAD], decay


def kernel(
    tok,
    gain,
    wq,
    wf,
    wv,
    wo,
    wp,
    room,
    shift,
    hgain,
    start,
    pmap,
    pscale,
    worec,
    wopool,
    out,
    T,
    GZ1,
    GX2,
    GZ2,
    GX3,
    GZ3,
    GB,
    SH,
    ST,
    K,
    V,
    Q,
    G,
    C,
    QE,
    INS,
    A0,
    SL,
    SR,
    ZS,
    ZR,
    ES,
    ER,
    EXT,
    BS,
    BR,
    RO,
    PO,
    ACT,
    PS,
    PR,
    SC,
    SS,
    iz1,
    ix2,
    iz2,
    ixz3,
    send_sems,
    recv_sems,
):
    z, x = lax.axis_index("sp_0"), lax.axis_index("sp_1")
    f, c = lax.axis_index("fs"), lax.axis_index("tp")
    zat = lambda k: lax.rem(z + (k + NZ), NZ)
    xat = lambda k: lax.rem(x + (k + NX), NX)
    fat = lambda k: lax.rem(f + (k + NF), NF)
    other = 1 - c
    here = z * NX + x
    after = lax.rem(here + 1, NZ * NX)
    ahead = lax.rem(here + NZ * NX - 1, NZ * NX)
    nxt = {"sp_0": after // NX, "sp_1": lax.rem(after, NX)}
    prv = {"sp_0": ahead // NX, "sp_1": lax.rem(ahead, NX)}

    barrier = pltpu.get_barrier_semaphore()
    met = [{"tp": other}, nxt, prv]
    met += [{"fs": fat(k)} for k in (1, 2, 3)] + [{"sp_1": xat(k)} for k in (1, 2, 3)]
    met += [{"sp_0": zat(k)} for k in range(1, NZ)]
    for who in met:
        pl.semaphore_signal(barrier, inc=1, device_id=who, device_id_type=MESH)

    count = [0]
    sent = []

    def sem():
        count[0] += 1
        assert count[0] <= NRECV
        return count[0] - 1

    def copy(n, src, dst, who, slot=0):
        return pltpu.make_async_remote_copy(
            src_ref=src,
            dst_ref=dst,
            send_sem=send_sems.at[slot],
            recv_sem=recv_sems.at[n],
            device_id=who,
            device_id_type=MESH,
        )

    def send(n, src, dst, who):
        slot = len(sent) % NSEND
        if len(sent) >= NSEND:
            sent[-NSEND].wait_send()
        made = copy(n, src, dst, who, slot)
        made.start()
        sent.append(made)

    def landed(n, dst):
        copy(n, dst, dst, {"tp": other}).wait_recv()

    rank = here * NF + f
    row = lax.broadcasted_iota(jnp.int32, (16, 128), 0)
    lane = lax.broadcasted_iota(jnp.int32, (16, 128), 1)
    gains = jnp.broadcast_to(gain[pl.ds(rank // 8, 1), :], (16, 128))
    gains = jnp.where(lane == lax.rem(rank, 8) * 16 + row, gains, 0.0)
    gains = jnp.sum(gains, axis=1, keepdims=True)
    weights = [(w[...].astype(F32) * gains).astype(BF16) for w in (wf, wv, wq, wo)]
    folded = [dot(wp[:, 256 * i : 256 * i + 256], pmap[i]) for i in range(2)]
    weights.append((jnp.concatenate(folded, axis=1) * gains * pscale[...]).astype(BF16))
    eye = jnp.where(lane[:, :16] == row[:, :16], 1.0, 0.0).astype(BF16)
    turned = [dot(eye, w[...], NT).astype(BF16) for w in (worec, wopool)]
    turned = jnp.concatenate(turned, axis=1)
    for i in range(NF):
        chunk = [w[:, 128 * i : 128 * i + 128] for w in weights]
        iz1[i] = jnp.concatenate(chunk[:2], axis=1)
        ix2[i] = jnp.concatenate(chunk[2:4], axis=1)
        iz2[i] = chunk[4]
    ixz3[...] = turned[:, :640]
    mine = pl.ds(pl.multiple_of(f * 16, 16), 16)
    pieces = ((GZ1, iz1), (GX2, ix2), (GZ2, iz2))
    for buffer, own in pieces:
        buffer[z, x, mine, :] = own[f]
    GX3[z, x, mine, :] = turned[:, :256]
    GZ3[z, x, mine, :] = turned[:, 256:640]
    GB[z, x, mine, :] = turned[:, 640:]
    T[c, f] = tok[...]
    SH[f] = jnp.transpose(shift[...])
    for i in range(NF):
        SS[i] = jnp.transpose(start[0, i]).astype(BF16)

    pl.semaphore_wait(barrier, len(met))

    def over_y(pairs):
        ns = [sem() for _ in pairs]
        for k in (1, 3, 2):
            to = fat(k)
            for n, (buffer, own) in zip(ns, pairs):
                send(n, own.at[to], buffer.at[z, x, mine, :], {"fs": to})
        return [(n, buffer.at[z, x, pl.ds(0, 48), :]) for n, (buffer, _) in zip(ns, pairs)]

    def over_out():
        ns = sem(), sem()
        for k in (1, 3, 2):
            to = {"fs": fat(k)}
            send(ns[0], ixz3.at[:, pl.ds(0, 256)], GX3.at[z, x, mine, :], to)
            send(ns[1], ixz3.at[:, pl.ds(256, 384)], GZ3.at[z, x, mine, :], to)
        return [(n, b.at[z, x, pl.ds(0, 48), :]) for n, b in zip(ns, (GX3, GZ3))]

    y1 = over_y(pieces[:1])
    y2 = over_y(pieces[1:3])
    y3 = over_out()
    nshift = sem()
    for k in (1, 3, 2):
        send(nshift, SH.at[f], SH.at[f], {"fs": fat(k)})

    first, second = pl.ds(0, 128), pl.ds(128, 128)
    right, left = {"fs": fat(1)}, {"fs": fat(3)}
    nt = [sem() for _ in range(3)]
    near, far_off = sem(), sem()

    def relay(n, seq, rows):
        send(n, T.at[c, seq, rows, :], T.at[c, seq, rows, :], {"tp": other})

    for i, (a, b) in enumerate(((first, second), (second, first))):
        send(nt[i], tok.at[a, :], T.at[c, f, a, :], right)
        send(nt[i], tok.at[b, :], T.at[c, f, b, :], left)
    send(near, tok, T.at[c, f], {"tp": other})

    def token_steps():
        landed(nt[0], T.at[c, fat(1)])
        send(nt[2], T.at[c, fat(-1), first, :], T.at[c, fat(-1), first, :], right)
        send(nt[2], T.at[c, fat(1), second, :], T.at[c, fat(1), second, :], left)
        relay(near, fat(-1), first)
        relay(near, fat(1), second)
        yield
        landed(nt[1], T.at[c, fat(1)])
        relay(near, fat(-1), second)
        relay(near, fat(1), first)
        yield
        landed(nt[2], T.at[c, fat(2)])
        relay(far_off, fat(2), first)
        relay(far_off, fat(2), second)
        yield

    def plane(waits, vx, vz):
        zr, zl = {"sp_0": zat(1)}, {"sp_0": zat(-1)}
        xr, xl = {"sp_1": xat(1)}, {"sp_1": xat(-1)}
        whole, lowx, highx = pl.ds(0, 4), pl.ds(0, 2), pl.ds(2, 2)
        for w in waits:
            landed(*w)
        if vx:
            xs = sem()
            for k in (1, 3, 2):
                send(xs, vx(z, x), vx(z, x), {"sp_1": xat(k)})
        nz = [sem() for _ in range(4)]
        send(nz[0], vz(z, x), vz(z, x), zr)
        send(nz[0], vz(z, x), vz(z, x), zl)
        forwards = []
        last = sem()

        def spread(offsets):
            n = sem()
            for offset in offsets:
                at = zat(offset)
                send(n, vz(at, x), vz(at, x), xr)
                send(n, vz(at, x), vz(at, x), xl)
            forwards.append((n, offsets))

        def forward(ready):
            for n, offsets in ready:
                landed(n, vz(z, pl.ds(0, 2 * len(offsets))))
                for offset in offsets:
                    at = zat(offset)
                    if 0 <= offset < 4:
                        send(last, vz(at, xat(-1)), vz(at, xat(-1)), xr)
                    else:
                        send(last, vz(at, xat(1)), vz(at, xat(1)), xl)

        spread((0,))
        yield
        if vx:
            landed(xs, vx(z, pl.ds(0, 3)))
            mz = [sem() for _ in range(4)]
            send(mz[0], vx(z, whole), vx(z, whole), zr)
            send(mz[0], vx(z, whole), vx(z, whole), zl)
            yield
        for k in (1, 2, 3):
            back, front = zat(-k), zat(k)
            landed(nz[k - 1], vz(z, pl.ds(0, 2)))
            part = vz(back, x, 1 if k == 3 else 0)
            send(nz[k], part, part, zr)
            part = vz(front, x, 2 if k == 3 else 0)
            send(nz[k], part, part, zl)
            ready = list(forwards)
            forwards.clear()
            spread((-k, k))
            if vx:
                landed(mz[k - 1], vx(pl.ds(0, 2), whole))
                part = vx(back, lowx if k == 3 else whole)
                send(mz[k], part, part, zr)
                part = vx(front, highx if k == 3 else whole)
                send(mz[k], part, part, zl)
            forward(ready)
            yield
        far = zat(4)
        landed(nz[3], vz(far, x))
        spread((4,))
        forward(forwards)
        if vx:
            landed(mz[3], vx(far, whole))
        yield
        landed(last, vz(pl.ds(0, NZ), x))
        yield

    def views(GX, GZ):
        halves = (None, pl.ds(0, 32), pl.ds(32, 32))

        def vz(zi, xi, part=0):
            return GZ.at[zi, xi, halves[part], :] if part else GZ.at[zi, xi]

        return (GX is not None) and (lambda zi, xi: GX.at[zi, xi]), vz

    lanes = (pl.ds(WBX, WB - WBX), pl.ds(WBX, 128), pl.ds(WBX + 128, 128))
    late = plane(
        (),
        lambda zi, xi: GB.at[zi, xi, mine, pl.ds(0, WBX)],
        lambda zi, xi, part=0: GB.at[zi, xi, mine, lanes[part]],
    )

    def late_over_y():
        first, second = pl.ds(0, 4), pl.ds(4, 4)

        def part(k, half):
            rows = pl.ds(pl.multiple_of(fat(k) * 16, 16), 16)
            return GB.at[half, :, rows, :]

        near, far = sem(), sem()
        for n, (a, b) in ((near, (first, second)), (far, (second, first))):
            send(n, part(0, a), part(0, a), right)
            send(n, part(0, b), part(0, b), left)
        yield
        landed(near, part(0, pl.ds(0, NZ)))
        send(far, part(-1, first), part(-1, first), right)
        send(far, part(1, second), part(1, second), left)
        yield
        landed(far, GB.at[:, :, pl.ds(0, 32), :])
        yield

    one = plane(y1, *views(None, GZ1))
    two = plane(y2, *views(GX2, GZ2))
    three = plane(y3, *views(GX3, GZ3))
    tokens = token_steps()

    ns = sem()

    def start_copies():
        return [copy(ns, SS.at[fat(k)], ST, {"fs": fat(k)}, NSEND + i) for i, k in enumerate((1, 2, 3))]

    @pl.when(f == x)
    def _():
        ST[...] = SS[f]
        for made in start_copies():
            made.start()

    next(late)
    next(one)
    next(two)
    next(late)
    next(one)
    next(tokens)
    next(one)
    next(two)
    next(late)
    next(one)
    next(tokens)
    next(one)
    next(late)
    next(two)
    next(three)
    next(one)
    landed(near, T.at[other, pl.ds(0, 3)])
    landed(nshift, SH.at[pl.ds(0, 3)])

    i0 = lax.broadcasted_iota(jnp.int32, (BLOCK, BLOCK), 0)
    i1 = lax.broadcasted_iota(jnp.int32, (BLOCK, BLOCK), 1)
    causal = i0 >= i1
    tril = jnp.where(causal, 1.0, 0.0).astype(BF16)
    ones = jnp.ones((BLOCK, BLOCK), BF16)
    my_room = room[pl.ds(f, 1), :]

    half = NZ // 2

    def each(body):
        for s in range(4):
            body(s, 0)

    def through(s, *weights):
        low = jnp.concatenate([w[:half].reshape(1024, w.shape[-1]) for w in weights], axis=1)
        high = jnp.concatenate([w[half:].reshape(1024, w.shape[-1]) for w in weights], axis=1)
        return (dot(T[0, s], low) + dot(T[1, s], high)) * SC[s]

    def project(s, _):
        w0, w1 = T[0, s].astype(F32), T[1, s].astype(F32)
        square = jnp.sum(w0 * w0 + w1 * w1, axis=1, keepdims=True)
        SC[s] = lax.rsqrt(square * (1.0 / 2048) + EPSILON)
        both = through(s, GZ1)
        keys = my_room * jax.nn.sigmoid(-both[:, :128])
        K[s] = keys
        value = both[:, 128:].astype(BF16)
        V[s] = value
        lag = SH[s, pl.ds(f, 1), :]
        ends, adds = [], []
        for b in range(2):
            rows = slice(b * BLOCK, (b + 1) * BLOCK)
            lags = three_parts(lag[:, rows])
            spread = [jnp.where(causal, jnp.broadcast_to(p, (BLOCK, BLOCK)), 0.0).astype(BF16) for p in lags]
            parts = [p.astype(BF16) for p in three_parts(jnp.log1p(-keys[rows]))]
            within = dot(
                jnp.concatenate([tril] * 3 + spread, axis=1),
                jnp.concatenate(parts + [ones] * 3, axis=0),
            )
            C[s, rows, :] = within
            end = within[BLOCK - 1 :]
            adds.append(dot(value[rows], (keys[rows] * jnp.exp(end - within)).astype(BF16), TN))
            ends.append(end)
        A0[s] = adds[0]
        SL[s] = pack_state(jnp.exp(ends[1]) * adds[0] + adds[1], ends[0] + ends[1])
        return 0

    for k in (0, -1, 1):
        project(fat(k), 0)
    next(two)
    next(three)
    next(late)
    next(tokens)
    landed(far_off, T.at[other, 0])
    project(fat(2), 0)

    def project_rest(s, _):
        rest = through(s, GX2, GZ2)
        query = rest[:, :128]
        Q[s] = query * jax.nn.sigmoid(query) * HEAD ** (-0.5)
        gate = rest[:, 128:256]
        G[s] = gate * jax.nn.sigmoid(gate) * hgain[...]
        pool = rest[:, 256:].astype(BF16)
        EXT[s, 128:384, :] = pool
        BS[s] = pool[240:256]
        return 0

    sx = sem()
    SR[x] = SL[x]
    for k in (1, 3, 2):
        send(sx, SL.at[xat(k)], SR.at[x], {"sp_1": xat(k)})
    next(two)
    next(late)
    next(three)
    landed(sx, SR.at[pl.ds(0, 3)])
    state, decay = unpack_state(SR[0])
    for i in range(1, NX):
        later, fade = unpack_state(SR[i])
        state, decay = jnp.exp(fade) * state + later, decay + fade
    ZS[...] = pack_state(state, decay)
    sz = sem()
    for k in (4, 3, 5, 2, 6, 1, 7):
        send(sz, ZS, ZR.at[z], {"sp_0": zat(k)})
    next(two)
    next(late)
    late = late_over_y()
    next(late)
    next(two)
    each(project_rest)
    nb = sem()
    send(nb, BS, BR, nxt)

    def inner(s, _):
        for b in range(2):
            rows = slice(b * BLOCK, (b + 1) * BLOCK)
            within = C[s, rows, :]
            centre = within[BLOCK // 2 - 1 : BLOCK // 2]
            query, keys = Q[s, rows, :], K[s, rows, :]
            scores = dot(
                (query * jnp.exp(within - centre)).astype(BF16),
                (keys * jnp.exp(centre - within)).astype(BF16),
                NT,
            )
            scores = jnp.where(causal, scores, 0.0).astype(BF16)
            INS[s, rows, :] = dot(scores, V[s, rows, :])
            QE[s, rows, :] = (query * jnp.exp(within)).astype(BF16)
        return 0

    each(inner)
    next(three)
    next(late)

    landed(nb, BR)
    span = lax.shift_left(jnp.int32(2), c * 2 + f // 2)
    ti = lax.broadcasted_iota(jnp.int32, (256, 384), 0)
    si = lax.broadcasted_iota(jnp.int32, (256, 384), 1) - 128
    band = jnp.where((si <= ti) & (si > ti - span) & (si >= -16), 1.0, 0.0).astype(BF16)
    position = here * 256 + lax.broadcasted_iota(jnp.int32, (256, 128), 0)
    amount = jnp.minimum(position + 1, span).astype(F32)

    def pool(s, _):
        EXT[s, 0:128, :] = jnp.zeros((128, 128), BF16)

        @pl.when(here > 0)
        def _():
            EXT[s, 112:128, :] = BR[s]

        window = dot(band, EXT[s])
        PO[s] = (window / amount - EXT[s, 128:384, :].astype(F32)).astype(BF16)
        return 0

    each(pool)

    def give_back(buffer, slot):
        n = sem()
        ACT[slot + f] = buffer[f]
        for k in (1, 3, 2):
            send(n, buffer.at[fat(k)], ACT.at[slot + f], {"fs": fat(k)})
        return n

    given_pool = give_back(PO, 4)

    landed(sz, ZR.at[pl.ds(0, NZ - 1)])

    @pl.when(f != x)
    def _():
        landed(ns, ST)

    def pass_z(i, state):
        later, fade = unpack_state(ZR[i])
        return jnp.exp(fade) * state + later

    state = lax.fori_loop(0, z, pass_z, ST[...].astype(F32))
    for i in range(NX):
        ES[i] = state.astype(BF16)
        if i < NX - 1:
            later, fade = unpack_state(SR[i])
            state = jnp.exp(fade) * state + later
    sb = sem()
    ER[x] = ES[x]
    for k in (1, 3, 2):
        send(sb, ES.at[xat(k)], ER.at[x], {"sp_1": xat(k)})
    next(three)
    landed(sb, ER.at[pl.ds(0, 3)])

    def finish(s, _):
        entering = ER[s].astype(F32)
        middle = jnp.exp(C[s, BLOCK - 1 : BLOCK, :]) * entering + A0[s]
        for b, state in enumerate((ER[s], middle.astype(BF16))):
            rows = slice(b * BLOCK, (b + 1) * BLOCK)
            raw = INS[s, rows, :] + dot(QE[s, rows, :], state, NT)
            square = jnp.mean(raw * raw, axis=1, keepdims=True)
            RO[s, rows, :] = (raw * lax.rsqrt(square + EPSILON) * G[s, rows, :]).astype(BF16)
        return 0

    each(finish)
    given_rec = give_back(RO, 0)
    next(three)
    next(three)
    next(late)
    landed(given_pool, ACT.at[pl.ds(0, 3)])
    landed(given_rec, ACT.at[pl.ds(0, 3)])

    a, b, d = (
        jnp.concatenate([ACT[i] for i in range(*span)], axis=1) for span in ((0, 2), (2, 5), (5, 8))
    )
    my_rows = pl.ds(pl.multiple_of(c * 128, 128), 128)
    their_rows = pl.ds(pl.multiple_of(other * 128, 128), 128)
    swap = sem()
    for i in range(4):
        at, cols = slice(2 * i, 2 * i + 2), slice(512 * i, 512 * i + 512)
        total = dot(a, GX3[at].reshape(512, 256), NT)
        total += dot(b, GZ3[at].reshape(512, WZ[2]), NT)
        total += dot(d, GB[at].reshape(512, WB), NT)
        PS[:, cols] = total.astype(BF16)
        send(swap, PS.at[their_rows, pl.ds(512 * i, 512)], PR.at[:, pl.ds(512 * i, 512)], {"tp": other})
    landed(swap, PR)
    out[...] = (PS[my_rows, :].astype(F32) + PR[...].astype(F32)).astype(BF16)

    for made in sent[-NSEND:]:
        made.wait_send()

    @pl.when(f == x)
    def _():
        for made in start_copies():
            made.wait_send()


def per_device(
    tokens,
    norm_gain,
    query_weight,
    forget_weight,
    value_weight,
    outgate_weight,
    pool_in_weight,
    forget_room,
    decay_shift,
    head_gain,
    start_state,
    pool_map,
    pool_scale,
    out_rec_weight,
    out_pool_weight,
):
    vmem = lambda *shape: pltpu.VMEM(shape, F32)
    half = lambda *shape: pltpu.VMEM(shape, BF16)
    mixed = pl.pallas_call(
        kernel,
        out_shape=jax.ShapeDtypeStruct((128, 2048), BF16),
        in_specs=[pl.BlockSpec(memory_space=pltpu.VMEM)] * 15,
        out_specs=pl.BlockSpec(memory_space=pltpu.VMEM),
        scratch_shapes=[
            half(2, 4, 256, 1024),
            half(NZ, NX, 64, WZ[0]),
            half(NZ, NX, 64, WX[0]),
            half(NZ, NX, 64, WZ[1]),
            half(NZ, NX, 64, WX[1]),
            half(NZ, NX, 64, WZ[2]),
            half(NZ, NX, 64, WB),
            vmem(4, 4, 256),
            half(128, 128),
            vmem(4, 256, 128),
            half(4, 256, 128),
            vmem(4, 256, 128),
            vmem(4, 256, 128),
            vmem(4, 256, 128),
            half(4, 256, 128),
            vmem(4, 256, 128),
            vmem(4, 128, 128),
            half(4, 144, 128),
            half(4, 144, 128),
            half(144, 128),
            half(NZ, 144, 128),
            half(4, 128, 128),
            half(4, 128, 128),
            half(4, 384, 128),
            half(4, 16, 128),
            half(4, 16, 128),
            half(4, 256, 128),
            half(4, 256, 128),
            half(8, 256, 128),
            half(256, 2048),
            half(128, 2048),
            vmem(4, 256, 1),
            half(4, 128, 128),
            half(4, 16, 256),
            half(4, 16, 256),
            half(4, 16, 128),
            half(16, 640),
            pltpu.SemaphoreType.DMA((NSEND + 3,)),
            pltpu.SemaphoreType.DMA((NRECV,)),
        ],
        compiler_params=pltpu.CompilerParams(
            collective_id=0, has_side_effects=True, vmem_limit_bytes=60 * 1024 * 1024
        ),
    )(
        tokens[0],
        norm_gain.reshape(16, 128),
        query_weight,
        forget_weight,
        value_weight,
        outgate_weight,
        pool_in_weight,
        forget_room.reshape(4, 128),
        decay_shift[0],
        head_gain.reshape(1, 128),
        start_state,
        pool_map,
        pool_scale.reshape(1, 512),
        out_rec_weight,
        out_pool_weight,
    )
    return mixed[None]


def solution(mesh):
    finer = Mesh(
        mesh.devices.reshape(8, 4, mesh.shape["fs"], mesh.shape["tp"]), ("sp_0", "sp_1", "fs", "tp")
    )
    placed = (
        P("fs", SP, "tp"),
        P(),
        P(SP_FS, "tp"),
        P(SP_FS, "tp"),
        P(SP_FS, "tp"),
        P(SP_FS, "tp"),
        P(SP_FS, "tp"),
        P("tp"),
        P("fs", SP, "tp"),
        P(),
        P("fs", "tp", None, None),
        P("tp", None, None),
        P("tp"),
        P("tp", SP_FS),
        P("tp", SP_FS),
    )
    return jax.shard_map(
        per_device, mesh=finer, in_specs=placed, out_specs=P("fs", SP_TP, None), check_vma=False
    )
```

```python
import functools

import jax
import jax.numpy as jnp
from jax import lax
from jax.experimental import pallas as pl
from jax.experimental.pallas import tpu as pltpu
from jax.sharding import Mesh
from jax.sharding import PartitionSpec as P

HEAD = 128
POOL_DIM = 256
BLOCK = 128
SP_FS = ("sp_0", "sp_1", "fs")
SP = ("sp_0", "sp_1")
SP_TP = ("sp_0", "sp_1", "tp")
EPSILON = 1e-06
MESH = pl.DeviceIdType.MESH
ORDER = (
    "LZ0", "LZ1", "LF0", "1Z0", "2Z0", "3Z0", "LZ2", "1Z1", "1Z2", "T1", "LX0", "3X0", "1F0", "2X0",
    "1Z3", "1Z4", "2Z1", "1F1", "LZ3", "LX1", "1F2", "T2", "1F3", "SQ", "1F4", "3X1", "3F0", "3Z1",
    "2X1", "LF1", "LF2", "LF3", "LZ4", "T3", "LX2", "1L", "PR3", "PR1", "2Z2", "3Z2", "3F1", "LF4",
    "2X2", "LX3", "2Z3", "3Z3", "SUMX", "2F0", "2X3", "LX4", "2Z4", "LL", "Y0", "2F1", "2F2", "3Z4",
    "3F2", "2F3", "3X2", "3F3", "2F4", "3F4", "Y1", "PASSZ", "2L", "2X4", "REST", "3L", "INNER",
    "FIN", "3X3", "POOL", "Y2", "3X4",
)
NRECV, NSEND = 77, 64
NZ, NX, NF = 8, 4, 4
WX, WZ, WB, WBX = (256, 256), (256, 128, 384), 384, 128
F32, BF16 = jnp.float32, jnp.bfloat16
NT = (((1,), (1,)), ((), ()))
TN = (((0,), (0,)), ((), ()))


def dot(a, b, dims=(((1,), (0,)), ((), ()))):
    return lax.dot_general(a, b, dims, preferred_element_type=F32)


def pack_state(state, decay):
    high, mid, low = three_parts(decay)
    row = lax.broadcasted_iota(jnp.int32, (16, HEAD), 0)
    tail = jnp.where(row == 0, high, jnp.where(row == 1, mid, jnp.where(row == 2, low, 0.0)))
    return jnp.concatenate([state, tail], axis=0).astype(BF16)


def three_parts(value):
    high = value.astype(BF16).astype(F32)
    rest = value - high
    mid = rest.astype(BF16).astype(F32)
    return high, mid, rest - mid


def unpack_state(packed):
    whole = packed.astype(F32)
    decay = jnp.sum(whole[HEAD : HEAD + 16], axis=0, keepdims=True)
    return whole[:HEAD], decay


def kernel(
    tok,
    gain,
    wq,
    wf,
    wv,
    wo,
    wp,
    room,
    shift,
    hgain,
    start,
    pmap,
    pscale,
    worec,
    wopool,
    out,
    T,
    GZ1,
    GX2,
    GZ2,
    GX3,
    GZ3,
    GB,
    SH,
    ST,
    K,
    V,
    Q,
    G,
    C,
    QE,
    INS,
    A0,
    SL,
    SR,
    ZS,
    ZR,
    ES,
    ER,
    EXT,
    BS,
    BR,
    RO,
    PO,
    ACT,
    PS,
    PR,
    SC,
    SS,
    iz1,
    ix2,
    iz2,
    ixz3,
    send_sems,
    recv_sems,
):
    z, x = lax.axis_index("sp_0"), lax.axis_index("sp_1")
    f, c = lax.axis_index("fs"), lax.axis_index("tp")
    zat = lambda k: lax.rem(z + (k + NZ), NZ)
    xat = lambda k: lax.rem(x + (k + NX), NX)
    fat = lambda k: lax.rem(f + (k + NF), NF)
    other = 1 - c
    here = z * NX + x
    after = lax.rem(here + 1, NZ * NX)
    ahead = lax.rem(here + NZ * NX - 1, NZ * NX)
    nxt = {"sp_0": after // NX, "sp_1": lax.rem(after, NX)}
    prv = {"sp_0": ahead // NX, "sp_1": lax.rem(ahead, NX)}

    barrier = pltpu.get_barrier_semaphore()
    met = [{"tp": other}, nxt, prv]
    met += [{"fs": fat(k)} for k in (1, 2, 3)] + [{"sp_1": xat(k)} for k in (1, 2, 3)]
    met += [{"sp_0": zat(k)} for k in range(1, NZ)]
    for who in met:
        pl.semaphore_signal(barrier, inc=1, device_id=who, device_id_type=MESH)

    count = [0]
    sent = []

    def sem():
        count[0] += 1
        assert count[0] <= NRECV
        return count[0] - 1

    def copy(n, src, dst, who, slot=0):
        return pltpu.make_async_remote_copy(
            src_ref=src,
            dst_ref=dst,
            send_sem=send_sems.at[slot],
            recv_sem=recv_sems.at[n],
            device_id=who,
            device_id_type=MESH,
        )

    def send(n, src, dst, who):
        slot = len(sent) % NSEND
        if len(sent) >= NSEND:
            sent[-NSEND].wait_send()
        made = copy(n, src, dst, who, slot)
        made.start()
        sent.append(made)

    def landed(n, dst):
        copy(n, dst, dst, {"tp": other}).wait_recv()

    rank = here * NF + f
    row = lax.broadcasted_iota(jnp.int32, (16, 128), 0)
    lane = lax.broadcasted_iota(jnp.int32, (16, 128), 1)
    gains = jnp.broadcast_to(gain[pl.ds(rank // 8, 1), :], (16, 128))
    gains = jnp.where(lane == lax.rem(rank, 8) * 16 + row, gains, 0.0)
    gains = jnp.sum(gains, axis=1, keepdims=True)
    weights = [(w[...].astype(F32) * gains).astype(BF16) for w in (wf, wv, wq, wo)]
    folded = [dot(wp[:, 256 * i : 256 * i + 256], pmap[i]) for i in range(2)]
    weights.append((jnp.concatenate(folded, axis=1) * gains * pscale[...]).astype(BF16))
    eye = jnp.where(lane[:, :16] == row[:, :16], 1.0, 0.0).astype(BF16)
    turned = [dot(eye, w[...], NT).astype(BF16) for w in (worec, wopool)]
    turned = jnp.concatenate(turned, axis=1)
    for i in range(NF):
        chunk = [w[:, 128 * i : 128 * i + 128] for w in weights]
        iz1[i] = jnp.concatenate(chunk[:2], axis=1)
        ix2[i] = jnp.concatenate(chunk[2:4], axis=1)
        iz2[i] = chunk[4]
    ixz3[...] = turned[:, :640]
    mine = pl.ds(pl.multiple_of(f * 16, 16), 16)
    pieces = ((GZ1, iz1), (GX2, ix2), (GZ2, iz2))
    for buffer, own in pieces:
        buffer[z, x, mine, :] = own[f]
    GX3[z, x, mine, :] = turned[:, :256]
    GZ3[z, x, mine, :] = turned[:, 256:640]
    GB[z, x, mine, :] = turned[:, 640:]
    T[c, f] = tok[...]
    SH[f] = jnp.transpose(shift[...])
    for i in range(NF):
        SS[i] = jnp.transpose(start[0, i]).astype(BF16)

    pl.semaphore_wait(barrier, len(met))

    def over_y(pairs):
        ns = [sem() for _ in pairs]
        for k in (1, 3, 2):
            to = fat(k)
            for n, (buffer, own) in zip(ns, pairs):
                send(n, own.at[to], buffer.at[z, x, mine, :], {"fs": to})
        return [(n, buffer.at[z, x, pl.ds(0, 48), :]) for n, (buffer, _) in zip(ns, pairs)]

    def over_out():
        ns = sem(), sem()
        for k in (1, 3, 2):
            to = {"fs": fat(k)}
            send(ns[0], ixz3.at[:, pl.ds(0, 256)], GX3.at[z, x, mine, :], to)
            send(ns[1], ixz3.at[:, pl.ds(256, 384)], GZ3.at[z, x, mine, :], to)
        return [(n, b.at[z, x, pl.ds(0, 48), :]) for n, b in zip(ns, (GX3, GZ3))]

    y1 = over_y(pieces[:1])
    y2 = over_y(pieces[1:3])
    y3 = over_out()
    nshift = sem()
    for k in (1, 3, 2):
        send(nshift, SH.at[f], SH.at[f], {"fs": fat(k)})

    first, second = pl.ds(0, 128), pl.ds(128, 128)
    right, left = {"fs": fat(1)}, {"fs": fat(3)}
    nt = [sem() for _ in range(3)]
    near, far_off = sem(), sem()

    def relay(n, seq, rows):
        send(n, T.at[c, seq, rows, :], T.at[c, seq, rows, :], {"tp": other})

    for i, (a, b) in enumerate(((first, second), (second, first))):
        send(nt[i], tok.at[a, :], T.at[c, f, a, :], right)
        send(nt[i], tok.at[b, :], T.at[c, f, b, :], left)
    send(near, tok, T.at[c, f], {"tp": other})

    def tokens_1():
        landed(nt[0], T.at[c, fat(1)])
        send(nt[2], T.at[c, fat(-1), first, :], T.at[c, fat(-1), first, :], right)
        send(nt[2], T.at[c, fat(1), second, :], T.at[c, fat(1), second, :], left)
        relay(near, fat(-1), first)
        relay(near, fat(1), second)

    def tokens_2():
        landed(nt[1], T.at[c, fat(1)])
        relay(near, fat(-1), second)
        relay(near, fat(1), first)

    def tokens_3():
        landed(nt[2], T.at[c, fat(2)])
        relay(far_off, fat(2), first)
        relay(far_off, fat(2), second)

    steps = {"T1": tokens_1, "T2": tokens_2, "T3": tokens_3}

    def plane(name, waits, vx, vz, direct=False):
        zr, zl = {"sp_0": zat(1)}, {"sp_0": zat(-1)}
        xr, xl = {"sp_1": xat(1)}, {"sp_1": xat(-1)}
        whole, lowx, highx = pl.ds(0, 4), pl.ds(0, 2), pl.ds(2, 2)
        nz, ns, last = [sem() for _ in range(4)], [sem() for _ in range(5)], sem()
        if vx:
            xs, mz = sem(), [sem() for _ in range(4)]
        offsets = ((0,), (-1, 1), (-2, 2), (-3, 3), (4,))

        def spread(k):
            for offset in offsets[k]:
                at = zat(offset)
                send(ns[k], vz(at, x), vz(at, x), xr)
                send(ns[k], vz(at, x), vz(at, x), xl)

        def z_step(k):
            if k == 0:
                for w in waits:
                    landed(*w)
                if vx:
                    for i in (1, 3, 2):
                        send(xs, vx(z, x), vx(z, x), {"sp_1": xat(i)})
                for i in (1, 2, 4, 3) if direct else (1,):
                    for step in (i, -i) if i < 4 else (i,):
                        send(nz[i - 1], vz(z, x), vz(z, x), {"sp_0": zat(step)})
            else:
                landed(nz[k - 1], vz(z, pl.ds(0, 2)) if k < 4 else vz(z, x))
                if k < 4 and not direct:
                    part = vz(zat(-k), x, 1 if k == 3 else 0)
                    send(nz[k], part, part, zr)
                    part = vz(zat(k), x, 2 if k == 3 else 0)
                    send(nz[k], part, part, zl)
            spread(k)

        def x_step(k):
            if k == 0:
                landed(xs, vx(z, pl.ds(0, 3)))
                send(mz[0], vx(z, whole), vx(z, whole), zr)
                send(mz[0], vx(z, whole), vx(z, whole), zl)
                return
            landed(mz[k - 1], vx(pl.ds(0, 2), whole) if k < 4 else vx(z, whole))
            if k < 4:
                part = vx(zat(-k), lowx if k == 3 else whole)
                send(mz[k], part, part, zr)
                part = vx(zat(k), highx if k == 3 else whole)
                send(mz[k], part, part, zl)

        def f_step(k):
            landed(ns[k], vz(z, pl.ds(0, 2 * len(offsets[k]))))
            for offset in offsets[k]:
                at = zat(offset)
                if 0 <= offset < 4:
                    send(last, vz(at, xat(-1)), vz(at, xat(-1)), xr)
                else:
                    send(last, vz(at, xat(1)), vz(at, xat(1)), xl)

        for k in range(5):
            steps[f"{name}Z{k}"] = functools.partial(z_step, k)
            steps[f"{name}F{k}"] = functools.partial(f_step, k)
            if vx:
                steps[f"{name}X{k}"] = functools.partial(x_step, k)
        steps[f"{name}L"] = lambda: landed(last, vz(pl.ds(0, NZ), x))

    def views(GX, GZ):
        halves = (None, pl.ds(0, 32), pl.ds(32, 32))

        def vz(zi, xi, part=0):
            return GZ.at[zi, xi, halves[part], :] if part else GZ.at[zi, xi]

        return (GX is not None) and (lambda zi, xi: GX.at[zi, xi]), vz

    lanes = (pl.ds(WBX, WB - WBX), pl.ds(WBX, 128), pl.ds(WBX + 128, 128))
    plane(
        "L",
        (),
        lambda zi, xi: GB.at[zi, xi, mine, pl.ds(0, WBX)],
        lambda zi, xi, part=0: GB.at[zi, xi, mine, lanes[part]],
    )

    half_z, other_half = pl.ds(0, 4), pl.ds(4, 4)
    ny = sem(), sem()

    def late_part(k, half):
        rows = pl.ds(pl.multiple_of(fat(k) * 16, 16), 16)
        return GB.at[half, :, rows, :]

    def late_y0():
        for n, (a, b) in zip(ny, ((half_z, other_half), (other_half, half_z))):
            send(n, late_part(0, a), late_part(0, a), right)
            send(n, late_part(0, b), late_part(0, b), left)

    def late_y1():
        landed(ny[0], late_part(0, pl.ds(0, NZ)))
        send(ny[1], late_part(-1, half_z), late_part(-1, half_z), right)
        send(ny[1], late_part(1, other_half), late_part(1, other_half), left)

    def late_y2():
        landed(ny[1], GB.at[:, :, pl.ds(0, 32), :])

    steps.update(Y0=late_y0, Y1=late_y1, Y2=late_y2)
    plane("1", y1, *views(None, GZ1), direct=True)
    plane("2", y2, *views(GX2, GZ2))
    plane("3", y3, *views(GX3, GZ3))

    ns = sem()

    def start_copies():
        return [copy(ns, SS.at[fat(k)], ST, {"fs": fat(k)}, NSEND + i) for i, k in enumerate((1, 2, 3))]

    @pl.when(f == x)
    def _():
        ST[...] = SS[f]
        for made in start_copies():
            made.start()

    def squares(s):
        w0, w1 = T[0, s].astype(F32), T[1, s].astype(F32)
        square = jnp.sum(w0 * w0 + w1 * w1, axis=1, keepdims=True)
        SC[s] = lax.rsqrt(square * (1.0 / 2048) + EPSILON)

    i0 = lax.broadcasted_iota(jnp.int32, (BLOCK, BLOCK), 0)
    i1 = lax.broadcasted_iota(jnp.int32, (BLOCK, BLOCK), 1)
    causal = i0 >= i1
    tril = jnp.where(causal, 1.0, 0.0).astype(BF16)
    ones = jnp.ones((BLOCK, BLOCK), BF16)
    my_room = room[pl.ds(f, 1), :]

    half = NZ // 2

    def each(body):
        for s in range(4):
            body(s, 0)

    def through(s, *weights):
        low = jnp.concatenate([w[:half].reshape(1024, w.shape[-1]) for w in weights], axis=1)
        high = jnp.concatenate([w[half:].reshape(1024, w.shape[-1]) for w in weights], axis=1)
        return (dot(T[0, s], low) + dot(T[1, s], high)) * SC[s]

    def project(s, _):
        both = through(s, GZ1)
        keys = my_room * jax.nn.sigmoid(-both[:, :128])
        K[s] = keys
        value = both[:, 128:].astype(BF16)
        V[s] = value
        lag = SH[s, pl.ds(f, 1), :]
        ends, adds = [], []
        for b in range(2):
            rows = slice(b * BLOCK, (b + 1) * BLOCK)
            lags = three_parts(lag[:, rows])
            spread = [jnp.where(causal, jnp.broadcast_to(p, (BLOCK, BLOCK)), 0.0).astype(BF16) for p in lags]
            parts = [p.astype(BF16) for p in three_parts(jnp.log1p(-keys[rows]))]
            within = dot(
                jnp.concatenate([tril] * 3 + spread, axis=1),
                jnp.concatenate(parts + [ones] * 3, axis=0),
            )
            C[s, rows, :] = within
            end = within[BLOCK - 1 :]
            adds.append(dot(value[rows], (keys[rows] * jnp.exp(end - within)).astype(BF16), TN))
            ends.append(end)
        A0[s] = adds[0]
        SL[s] = pack_state(jnp.exp(ends[1]) * adds[0] + adds[1], ends[0] + ends[1])
        return 0

    sx, sz, sb, nb = sem(), sem(), sem(), sem()

    def squares_near():
        landed(near, T.at[other, pl.ds(0, 3)])
        for k in (0, -1, 1):
            squares(fat(k))

    def project_near():
        landed(nshift, SH.at[pl.ds(0, 3)])
        for k in (0, -1, 1):
            project(fat(k), 0)

    def project_far():
        landed(far_off, T.at[other, 0])
        squares(fat(2))
        project(fat(2), 0)
        SR[x] = SL[x]
        for k in (1, 3, 2):
            send(sx, SL.at[xat(k)], SR.at[x], {"sp_1": xat(k)})

    def total_x():
        landed(sx, SR.at[pl.ds(0, 3)])
        state, decay = unpack_state(SR[0])
        for i in range(1, NX):
            later, fade = unpack_state(SR[i])
            state, decay = jnp.exp(fade) * state + later, decay + fade
        ZS[...] = pack_state(state, decay)
        for k in (4, 3, 5, 2, 6, 1, 7):
            send(sz, ZS, ZR.at[z], {"sp_0": zat(k)})

    def project_rest(s, _):
        rest = through(s, GX2, GZ2)
        query = rest[:, :128]
        Q[s] = query * jax.nn.sigmoid(query) * HEAD ** (-0.5)
        gate = rest[:, 128:256]
        G[s] = gate * jax.nn.sigmoid(gate) * hgain[...]
        pool = rest[:, 256:].astype(BF16)
        EXT[s, 128:384, :] = pool
        BS[s] = pool[240:256]
        return 0

    def rest():
        each(project_rest)
        send(nb, BS, BR, nxt)

    def inner(s, _):
        for b in range(2):
            rows = slice(b * BLOCK, (b + 1) * BLOCK)
            within = C[s, rows, :]
            centre = within[BLOCK // 2 - 1 : BLOCK // 2]
            query, keys = Q[s, rows, :], K[s, rows, :]
            scores = dot(
                (query * jnp.exp(within - centre)).astype(BF16),
                (keys * jnp.exp(centre - within)).astype(BF16),
                NT,
            )
            scores = jnp.where(causal, scores, 0.0).astype(BF16)
            INS[s, rows, :] = dot(scores, V[s, rows, :])
            QE[s, rows, :] = (query * jnp.exp(within)).astype(BF16)
        return 0

    span = lax.shift_left(jnp.int32(2), c * 2 + f // 2)
    ti = lax.broadcasted_iota(jnp.int32, (256, 384), 0)
    si = lax.broadcasted_iota(jnp.int32, (256, 384), 1) - 128
    band = jnp.where((si <= ti) & (si > ti - span) & (si >= -16), 1.0, 0.0).astype(BF16)
    position = here * 256 + lax.broadcasted_iota(jnp.int32, (256, 128), 0)
    amount = jnp.minimum(position + 1, span).astype(F32)

    def pool(s, _):
        EXT[s, 0:128, :] = jnp.zeros((128, 128), BF16)

        @pl.when(here > 0)
        def _():
            EXT[s, 112:128, :] = BR[s]

        window = dot(band, EXT[s])
        PO[s] = (window / amount - EXT[s, 128:384, :].astype(F32)).astype(BF16)
        return 0

    def give_back(buffer, slot):
        n = sem()
        ACT[slot + f] = buffer[f]
        for k in (1, 3, 2):
            send(n, buffer.at[fat(k)], ACT.at[slot + f], {"fs": fat(k)})
        return n

    given = []

    def pooling():
        landed(nb, BR)
        each(pool)
        given.append(give_back(PO, 4))

    def pass_z(i, state):
        later, fade = unpack_state(ZR[i])
        return jnp.exp(fade) * state + later

    def from_z():
        landed(sz, ZR.at[pl.ds(0, NZ - 1)])

        @pl.when(f != x)
        def _():
            landed(ns, ST)

        state = lax.fori_loop(0, z, pass_z, ST[...].astype(F32))
        for i in range(NX):
            ES[i] = state.astype(BF16)
            if i < NX - 1:
                later, fade = unpack_state(SR[i])
                state = jnp.exp(fade) * state + later
        ER[x] = ES[x]
        for k in (1, 3, 2):
            send(sb, ES.at[xat(k)], ER.at[x], {"sp_1": xat(k)})

    def finish(s, _):
        entering = ER[s].astype(F32)
        middle = jnp.exp(C[s, BLOCK - 1 : BLOCK, :]) * entering + A0[s]
        for b, state in enumerate((ER[s], middle.astype(BF16))):
            rows = slice(b * BLOCK, (b + 1) * BLOCK)
            raw = INS[s, rows, :] + dot(QE[s, rows, :], state, NT)
            square = jnp.mean(raw * raw, axis=1, keepdims=True)
            RO[s, rows, :] = (raw * lax.rsqrt(square + EPSILON) * G[s, rows, :]).astype(BF16)
        return 0

    def finishing():
        landed(sb, ER.at[pl.ds(0, 3)])
        each(finish)
        given.append(give_back(RO, 0))

    steps.update(
        SQ=squares_near,
        PR3=project_near,
        PR1=project_far,
        SUMX=total_x,
        REST=rest,
        INNER=lambda: each(inner),
        POOL=pooling,
        PASSZ=from_z,
        FIN=finishing,
    )
    order = ORDER
    assert sorted(order) == sorted(steps)
    for step in order:
        with jax.named_scope(step):
            steps[step]()

    for n in given:
        landed(n, ACT.at[pl.ds(0, 3)])

    a, b, d = (
        jnp.concatenate([ACT[i] for i in range(*span)], axis=1) for span in ((0, 2), (2, 5), (5, 8))
    )
    my_rows = pl.ds(pl.multiple_of(c * 128, 128), 128)
    their_rows = pl.ds(pl.multiple_of(other * 128, 128), 128)
    swap = sem()
    for i in range(4):
        at, cols = slice(2 * i, 2 * i + 2), slice(512 * i, 512 * i + 512)
        total = dot(a, GX3[at].reshape(512, 256), NT)
        total += dot(b, GZ3[at].reshape(512, WZ[2]), NT)
        total += dot(d, GB[at].reshape(512, WB), NT)
        PS[:, cols] = total.astype(BF16)
        send(swap, PS.at[their_rows, pl.ds(512 * i, 512)], PR.at[:, pl.ds(512 * i, 512)], {"tp": other})
    landed(swap, PR)
    out[...] = (PS[my_rows, :].astype(F32) + PR[...].astype(F32)).astype(BF16)

    for made in sent[-NSEND:]:
        made.wait_send()

    @pl.when(f == x)
    def _():
        for made in start_copies():
            made.wait_send()


def per_device(
    tokens,
    norm_gain,
    query_weight,
    forget_weight,
    value_weight,
    outgate_weight,
    pool_in_weight,
    forget_room,
    decay_shift,
    head_gain,
    start_state,
    pool_map,
    pool_scale,
    out_rec_weight,
    out_pool_weight,
):
    vmem = lambda *shape: pltpu.VMEM(shape, F32)
    half = lambda *shape: pltpu.VMEM(shape, BF16)
    mixed = pl.pallas_call(
        kernel,
        out_shape=jax.ShapeDtypeStruct((128, 2048), BF16),
        in_specs=[pl.BlockSpec(memory_space=pltpu.VMEM)] * 15,
        out_specs=pl.BlockSpec(memory_space=pltpu.VMEM),
        scratch_shapes=[
            half(2, 4, 256, 1024),
            half(NZ, NX, 64, WZ[0]),
            half(NZ, NX, 64, WX[0]),
            half(NZ, NX, 64, WZ[1]),
            half(NZ, NX, 64, WX[1]),
            half(NZ, NX, 64, WZ[2]),
            half(NZ, NX, 64, WB),
            vmem(4, 4, 256),
            half(128, 128),
            vmem(4, 256, 128),
            half(4, 256, 128),
            vmem(4, 256, 128),
            vmem(4, 256, 128),
            vmem(4, 256, 128),
            half(4, 256, 128),
            vmem(4, 256, 128),
            vmem(4, 128, 128),
            half(4, 144, 128),
            half(4, 144, 128),
            half(144, 128),
            half(NZ, 144, 128),
            half(4, 128, 128),
            half(4, 128, 128),
            half(4, 384, 128),
            half(4, 16, 128),
            half(4, 16, 128),
            half(4, 256, 128),
            half(4, 256, 128),
            half(8, 256, 128),
            half(256, 2048),
            half(128, 2048),
            vmem(4, 256, 1),
            half(4, 128, 128),
            half(4, 16, 256),
            half(4, 16, 256),
            half(4, 16, 128),
            half(16, 640),
            pltpu.SemaphoreType.DMA((NSEND + 3,)),
            pltpu.SemaphoreType.DMA((NRECV,)),
        ],
        compiler_params=pltpu.CompilerParams(
            collective_id=0, has_side_effects=True, vmem_limit_bytes=60 * 1024 * 1024
        ),
    )(
        tokens[0],
        norm_gain.reshape(16, 128),
        query_weight,
        forget_weight,
        value_weight,
        outgate_weight,
        pool_in_weight,
        forget_room.reshape(4, 128),
        decay_shift[0],
        head_gain.reshape(1, 128),
        start_state,
        pool_map,
        pool_scale.reshape(1, 512),
        out_rec_weight,
        out_pool_weight,
    )
    return mixed[None]


def solution(mesh):
    finer = Mesh(
        mesh.devices.reshape(8, 4, mesh.shape["fs"], mesh.shape["tp"]), ("sp_0", "sp_1", "fs", "tp")
    )
    placed = (
        P("fs", SP, "tp"),
        P(),
        P(SP_FS, "tp"),
        P(SP_FS, "tp"),
        P(SP_FS, "tp"),
        P(SP_FS, "tp"),
        P(SP_FS, "tp"),
        P("tp"),
        P("fs", SP, "tp"),
        P(),
        P("fs", "tp", None, None),
        P("tp", None, None),
        P("tp"),
        P("tp", SP_FS),
        P("tp", SP_FS),
    )
    return jax.shard_map(
        per_device, mesh=finer, in_specs=placed, out_specs=P("fs", SP_TP, None), check_vma=False
    )
```

```python
import functools

import jax
import jax.numpy as jnp
from jax import lax
from jax.experimental import pallas as pl
from jax.experimental.pallas import tpu as pltpu
from jax.sharding import Mesh
from jax.sharding import PartitionSpec as P

HEAD = 128
POOL_DIM = 256
BLOCK = 128
SP_FS = ("sp_0", "sp_1", "fs")
SP = ("sp_0", "sp_1")
SP_TP = ("sp_0", "sp_1", "tp")
EPSILON = 1e-06
MESH = pl.DeviceIdType.MESH
ORDER = (
    "LZ0", "LZ1", "LF0", "1Z0", "LX0", "2Z0", "LZ2", "LF1", "1Z1", "1F0", "1Z2", "2X0", "LF2", "T1",
    "3Z0", "1Z3", "1Z4", "LX1", "2Z1", "LZ3", "T2", "1F1", "1F2", "2X1", "SQ", "1F3", "LX2", "LZ4",
    "1F4", "3X0", "3Z1", "LF3", "2Z2", "T3", "LF4", "2X2", "1L", "PR3", "PR1", "2Z3", "3X1", "LX3",
    "LL", "2X3", "3Z2", "2Z4", "SUMX", "3F0", "2F0", "2F1", "2F2", "2F3", "LX4", "Y0", "3F1", "2F4",
    "3Z3", "2X4", "3F2", "2L", "REST", "Y1", "3X2", "3F3", "INNER", "PASSZ", "POOL", "3Z4", "3X3",
    "FIN", "Y2", "3F4", "3X4", "3L", "OUTP",
)
NRECV, NSEND, NLONG = 77, 40, 13
NZ, NX, NF = 8, 4, 4
WX, WZ, WB, WBX = (256, 256), (256, 128, 384), 384, 128
F32, BF16 = jnp.float32, jnp.bfloat16
NT = (((1,), (1,)), ((), ()))
TN = (((0,), (0,)), ((), ()))


def dot(a, b, dims=(((1,), (0,)), ((), ()))):
    return lax.dot_general(a, b, dims, preferred_element_type=F32)


def pack_state(state, decay):
    high, mid, low = three_parts(decay)
    row = lax.broadcasted_iota(jnp.int32, (16, HEAD), 0)
    tail = jnp.where(row == 0, high, jnp.where(row == 1, mid, jnp.where(row == 2, low, 0.0)))
    return jnp.concatenate([state, tail], axis=0).astype(BF16)


def three_parts(value):
    high = value.astype(BF16).astype(F32)
    rest = value - high
    mid = rest.astype(BF16).astype(F32)
    return high, mid, rest - mid


def unpack_state(packed):
    whole = packed.astype(F32)
    decay = jnp.sum(whole[HEAD : HEAD + 16], axis=0, keepdims=True)
    return whole[:HEAD], decay


def kernel(
    tok,
    gain,
    wq,
    wf,
    wv,
    wo,
    wp,
    room,
    shift,
    hgain,
    start,
    pmap,
    pscale,
    worec,
    wopool,
    out,
    T,
    GZ1,
    GX2,
    GZ2,
    GX3,
    GZ3,
    GB,
    SH,
    ST,
    K,
    V,
    Q,
    G,
    C,
    QE,
    INS,
    A0,
    SL,
    SR,
    ZS,
    ZR,
    ES,
    ER,
    EXT,
    BS,
    BR,
    RO,
    PO,
    ACT,
    PS,
    PR,
    SC,
    SS,
    S0,
    PM,
    PT,
    iz1,
    ix2,
    iz2,
    ixz3,
    send_sems,
    recv_sems,
    local_sems,
):
    z, x = lax.axis_index("sp_0"), lax.axis_index("sp_1")
    f, c = lax.axis_index("fs"), lax.axis_index("tp")
    zat = lambda k: lax.rem(z + (k + NZ), NZ)
    xat = lambda k: lax.rem(x + (k + NX), NX)
    fat = lambda k: lax.rem(f + (k + NF), NF)
    other = 1 - c
    here = z * NX + x
    after = lax.rem(here + 1, NZ * NX)
    ahead = lax.rem(here + NZ * NX - 1, NZ * NX)
    nxt = {"sp_0": after // NX, "sp_1": lax.rem(after, NX)}
    prv = {"sp_0": ahead // NX, "sp_1": lax.rem(ahead, NX)}

    taken = [
        pltpu.make_async_copy(source, target, local_sems.at[i])
        for i, (source, target) in enumerate(((pmap, PM), (tok, T.at[c, 1]), (start.at[0], S0)))
    ]
    for made in taken:
        made.start()

    barrier = pltpu.get_barrier_semaphore()
    met = [{"tp": other}, nxt, prv]
    met += [{"fs": fat(k)} for k in (1, 2, 3)] + [{"sp_1": xat(k)} for k in (1, 2, 3)]
    met += [{"sp_0": zat(k)} for k in range(1, NZ)]
    for who in met:
        pl.semaphore_signal(barrier, inc=1, device_id=who, device_id_type=MESH)

    count = [0]
    sent, sent_long = [], []

    def sem():
        count[0] += 1
        assert count[0] <= NRECV
        return count[0] - 1

    def copy(n, src, dst, who, slot=0):
        return pltpu.make_async_remote_copy(
            src_ref=src,
            dst_ref=dst,
            send_sem=send_sems.at[slot],
            recv_sem=recv_sems.at[n],
            device_id=who,
            device_id_type=MESH,
        )

    def send(n, src, dst, who, long=False):
        made_before, slots, base = (sent_long, NLONG, NSEND) if long else (sent, NSEND, 0)
        if len(made_before) >= slots:
            made_before[-slots].wait_send()
        made = copy(n, src, dst, who, base + len(made_before) % slots)
        made.start()
        made_before.append(made)

    def landed(n, dst):
        copy(n, dst, dst, {"tp": other}).wait_recv()

    rank = here * NF + f
    row = lax.broadcasted_iota(jnp.int32, (16, 128), 0)
    lane = lax.broadcasted_iota(jnp.int32, (16, 128), 1)
    gains = jnp.broadcast_to(gain[pl.ds(rank // 8, 1), :], (16, 128))
    gains = jnp.where(lane == lax.rem(rank, 8) * 16 + row, gains, 0.0)
    gains = jnp.sum(gains, axis=1, keepdims=True)
    taken[0].wait()
    weights = [(w[...].astype(F32) * gains).astype(BF16) for w in (wf, wv, wq, wo)]
    folded = [dot(wp[:, 256 * i : 256 * i + 256], PM[i]) for i in range(2)]
    weights.append((jnp.concatenate(folded, axis=1) * gains * pscale[...]).astype(BF16))
    turned = jnp.concatenate([worec[...], wopool[...]], axis=1)
    for i in range(NF):
        chunk = [w[:, 128 * i : 128 * i + 128] for w in weights]
        iz1[i] = jnp.concatenate(chunk[:2], axis=1)
        ix2[i] = jnp.concatenate(chunk[2:4], axis=1)
        iz2[i] = chunk[4]
    ixz3[...] = turned[:, :640]
    mine = pl.ds(pl.multiple_of(f * 16, 16), 16)
    pieces = ((GZ1, iz1), (GX2, ix2), (GZ2, iz2))
    for buffer, own in pieces:
        buffer[z, x, mine, :] = own[f]
    GX3[z, x, mine, :] = turned[:, :256]
    GZ3[z, x, mine, :] = turned[:, 256:640]
    GB[z, x, mine, :] = turned[:, 640:]
    SH[1] = shift[...]
    taken[1].wait()

    pl.semaphore_wait(barrier, len(met))

    def over_y(pairs):
        ns = [sem() for _ in pairs]
        for k in (1, 3, 2):
            to = fat(k)
            for n, (buffer, own) in zip(ns, pairs):
                send(n, own.at[to], buffer.at[z, x, mine, :], {"fs": to})
        return [(n, buffer.at[z, x, pl.ds(0, 48), :]) for n, (buffer, _) in zip(ns, pairs)]

    def over_out():
        ns = sem(), sem()
        for k in (1, 3, 2):
            to = {"fs": fat(k)}
            send(ns[0], ixz3.at[:, pl.ds(0, 256)], GX3.at[z, x, mine, :], to)
            send(ns[1], ixz3.at[:, pl.ds(256, 384)], GZ3.at[z, x, mine, :], to)
        return [(n, b.at[z, x, pl.ds(0, 48), :]) for n, b in zip(ns, (GX3, GZ3))]

    y1 = over_y(pieces[:1])
    y2 = over_y(pieces[1:3])
    y3 = over_out()
    nshift = sem()
    for k in (1, 3, 2):
        send(nshift, SH.at[1], SH.at[(5 - k) % 4], {"fs": fat(k)})

    first, second = pl.ds(0, 128), pl.ds(128, 128)
    right, left = {"fs": fat(1)}, {"fs": fat(3)}
    nt = [sem() for _ in range(3)]
    near, far_off = sem(), sem()

    def relay(n, seq, rows):
        send(n, T.at[c, seq, rows, :], T.at[c, seq, rows, :], {"tp": other}, True)

    for i, (a, b) in enumerate(((first, second), (second, first))):
        send(nt[i], T.at[c, 1, a, :], T.at[c, 0, a, :], right, True)
        send(nt[i], T.at[c, 1, b, :], T.at[c, 2, b, :], left, True)
    send(near, T.at[c, 1], T.at[c, 1], {"tp": other}, True)

    def tokens_1():
        landed(nt[0], T.at[c, 0])
        send(nt[2], T.at[c, 0, first, :], T.at[c, 3, first, :], right, True)
        send(nt[2], T.at[c, 2, second, :], T.at[c, 3, second, :], left, True)
        relay(near, 0, first)
        relay(near, 2, second)

    def tokens_2():
        landed(nt[1], T.at[c, 0])
        relay(near, 0, second)
        relay(near, 2, first)

    def tokens_3():
        landed(nt[2], T.at[c, 3])
        relay(far_off, 3, first)
        relay(far_off, 3, second)

    steps = {"T1": tokens_1, "T2": tokens_2, "T3": tokens_3}

    def plane(name, waits, vx, vz, direct=False):
        zr, zl = {"sp_0": zat(1)}, {"sp_0": zat(-1)}
        xr, xl = {"sp_1": xat(1)}, {"sp_1": xat(-1)}
        whole, lowx, highx = pl.ds(0, 4), pl.ds(0, 2), pl.ds(2, 2)
        nz, ns, last = [sem() for _ in range(4)], [sem() for _ in range(5)], sem()
        if vx:
            xs, mz = sem(), [sem() for _ in range(4)]
        offsets = ((0,), (-1, 1), (-2, 2), (-3, 3), (4,))

        def spread(k):
            for offset in offsets[k]:
                at = zat(offset)
                send(ns[k], vz(at, x), vz(at, x), xr)
                send(ns[k], vz(at, x), vz(at, x), xl)

        def z_step(k):
            if k == 0:
                for w in waits:
                    landed(*w)
                if vx:
                    for i in (1, 3, 2):
                        send(xs, vx(z, x), vx(z, x), {"sp_1": xat(i)})
                for i in (1, 2, 4, 3) if direct else (1,):
                    for step in (i, -i) if i < 4 else (i,):
                        send(nz[i - 1], vz(z, x), vz(z, x), {"sp_0": zat(step)})
            else:
                landed(nz[k - 1], vz(z, pl.ds(0, 2)) if k < 4 else vz(z, x))
                if k < 4 and not direct:
                    part = vz(zat(-k), x, 1 if k == 3 else 0)
                    send(nz[k], part, part, zr)
                    part = vz(zat(k), x, 2 if k == 3 else 0)
                    send(nz[k], part, part, zl)
            spread(k)

        def x_step(k):
            if k == 0:
                landed(xs, vx(z, pl.ds(0, 3)))
                send(mz[0], vx(z, whole), vx(z, whole), zr)
                send(mz[0], vx(z, whole), vx(z, whole), zl)
                return
            landed(mz[k - 1], vx(pl.ds(0, 2), whole) if k < 4 else vx(z, whole))
            if k < 4:
                part = vx(zat(-k), lowx if k == 3 else whole)
                send(mz[k], part, part, zr)
                part = vx(zat(k), highx if k == 3 else whole)
                send(mz[k], part, part, zl)

        def f_step(k):
            landed(ns[k], vz(z, pl.ds(0, 2 * len(offsets[k]))))
            for offset in offsets[k]:
                at = zat(offset)
                if 0 <= offset < 4:
                    send(last, vz(at, xat(-1)), vz(at, xat(-1)), xr)
                else:
                    send(last, vz(at, xat(1)), vz(at, xat(1)), xl)

        for k in range(5):
            steps[f"{name}Z{k}"] = functools.partial(z_step, k)
            steps[f"{name}F{k}"] = functools.partial(f_step, k)
            if vx:
                steps[f"{name}X{k}"] = functools.partial(x_step, k)
        steps[f"{name}L"] = lambda: landed(last, vz(pl.ds(0, NZ), x))

    def views(GX, GZ):
        halves = (None, pl.ds(0, 32), pl.ds(32, 32))

        def vz(zi, xi, part=0):
            return GZ.at[zi, xi, halves[part], :] if part else GZ.at[zi, xi]

        return (GX is not None) and (lambda zi, xi: GX.at[zi, xi]), vz

    lanes = (pl.ds(WBX, WB - WBX), pl.ds(WBX, 128), pl.ds(WBX + 128, 128))
    plane(
        "L",
        (),
        lambda zi, xi: GB.at[zi, xi, mine, pl.ds(0, WBX)],
        lambda zi, xi, part=0: GB.at[zi, xi, mine, lanes[part]],
    )

    half_z, other_half = pl.ds(0, 4), pl.ds(4, 4)
    ny = sem(), sem()

    def late_part(k, half):
        rows = pl.ds(pl.multiple_of(fat(k) * 16, 16), 16)
        return GB.at[half, :, rows, :]

    def late_y0():
        for n, (a, b) in zip(ny, ((half_z, other_half), (other_half, half_z))):
            send(n, late_part(0, a), late_part(0, a), right, True)
            send(n, late_part(0, b), late_part(0, b), left, True)

    def late_y1():
        landed(ny[0], late_part(0, pl.ds(0, NZ)))
        send(ny[1], late_part(-1, half_z), late_part(-1, half_z), right, True)
        send(ny[1], late_part(1, other_half), late_part(1, other_half), left, True)

    def late_y2():
        landed(ny[1], GB.at[:, :, pl.ds(0, 32), :])

    steps.update(Y0=late_y0, Y1=late_y1, Y2=late_y2)
    plane("1", y1, *views(None, GZ1), direct=True)
    plane("2", y2, *views(GX2, GZ2))
    plane("3", y3, *views(GX3, GZ3))

    ns = sem()

    def start_copies():
        return [copy(ns, SS.at[fat(k)], ST, {"fs": fat(k)}, NSEND + NLONG + i) for i, k in enumerate((1, 2, 3))]

    taken[2].wait()

    @pl.when(f == x)
    def _():
        for i in range(NF):
            SS[i] = jnp.transpose(S0[i]).astype(BF16)
        ST[...] = SS[f]
        for made in start_copies():
            made.start()

    def squares(s):
        w0, w1 = T[0, s].astype(F32), T[1, s].astype(F32)
        square = jnp.sum(w0 * w0 + w1 * w1, axis=1, keepdims=True)
        SC[s] = lax.rsqrt(square * (1.0 / 2048) + EPSILON)

    i0 = lax.broadcasted_iota(jnp.int32, (BLOCK, BLOCK), 0)
    i1 = lax.broadcasted_iota(jnp.int32, (BLOCK, BLOCK), 1)
    causal = i0 >= i1
    tril = jnp.where(causal, 1.0, 0.0).astype(BF16)
    ones = jnp.ones((BLOCK, BLOCK), BF16)
    my_room = room[pl.ds(f, 1), :]

    half = NZ // 2

    def each(body):
        for s in range(4):
            body(s, 0)

    def through(slots, *weights):
        count = len(slots) * 256
        at = slice(slots[0], slots[-1] + 1)
        low = jnp.concatenate([w[:half].reshape(1024, w.shape[-1]) for w in weights], axis=1)
        high = jnp.concatenate([w[half:].reshape(1024, w.shape[-1]) for w in weights], axis=1)
        total = dot(T[0, at].reshape(count, 1024), low) + dot(T[1, at].reshape(count, 1024), high)
        total = total * SC[at].reshape(count, 1)
        return [total[256 * i : 256 * i + 256] for i in range(len(slots))]

    def project(s, both):
        keys = my_room * jax.nn.sigmoid(-both[:, :128])
        K[s] = keys
        value = both[:, 128:].astype(BF16)
        V[s] = value
        lag = SH[s, pl.ds(f, 1), :]
        ends, adds = [], []
        for b in range(2):
            rows = slice(b * BLOCK, (b + 1) * BLOCK)
            lags = three_parts(lag[:, rows])
            spread = [jnp.where(causal, jnp.broadcast_to(p, (BLOCK, BLOCK)), 0.0).astype(BF16) for p in lags]
            parts = [p.astype(BF16) for p in three_parts(jnp.log1p(-keys[rows]))]
            within = dot(
                jnp.concatenate([tril] * 3 + spread, axis=1),
                jnp.concatenate(parts + [ones] * 3, axis=0),
            )
            C[s, rows, :] = within
            end = within[BLOCK - 1 :]
            adds.append(dot(value[rows], (keys[rows] * jnp.exp(end - within)).astype(BF16), TN))
            ends.append(end)
        A0[s] = adds[0]
        SL[s] = pack_state(jnp.exp(ends[1]) * adds[0] + adds[1], ends[0] + ends[1])

    sx, sz, sb, nb = sem(), sem(), sem(), sem()

    def squares_near():
        landed(near, T.at[other, pl.ds(0, 3)])
        for s in range(3):
            squares(s)

    def project_near():
        landed(nshift, SH.at[pl.ds(0, 3)])
        for s, both in enumerate(through((0, 1, 2), GZ1)):
            project(s, both)

    def project_far():
        landed(far_off, T.at[other, 3])
        squares(3)
        project(3, through((3,), GZ1)[0])
        slot_of = lambda sequence: lax.rem(sequence - f + (NF + 1), NF)
        SR[x] = SL[slot_of(x)]
        for k in (1, 3, 2):
            send(sx, SL.at[slot_of(xat(k))], SR.at[x], {"sp_1": xat(k)})

    def total_x():
        landed(sx, SR.at[pl.ds(0, 3)])
        state, decay = unpack_state(SR[0])
        for i in range(1, NX):
            later, fade = unpack_state(SR[i])
            state, decay = jnp.exp(fade) * state + later, decay + fade
        ZS[...] = pack_state(state, decay)
        for k in (4, 3, 5, 2, 6, 1, 7):
            send(sz, ZS, ZR.at[z], {"sp_0": zat(k)})

    def project_rest(s, rest):
        query = rest[:, :128]
        Q[s] = query * jax.nn.sigmoid(query) * HEAD ** (-0.5)
        gate = rest[:, 128:256]
        G[s] = gate * jax.nn.sigmoid(gate) * hgain[...]
        pool = rest[:, 256:].astype(BF16)
        EXT[s, 128:384, :] = pool
        BS[s] = pool[240:256]

    def rest():
        for slots in ((0, 1), (2, 3)):
            for s, projected in zip(slots, through(slots, GX2, GZ2)):
                project_rest(s, projected)
        send(nb, BS, BR, nxt)

    def inner(s, _):
        for b in range(2):
            rows = slice(b * BLOCK, (b + 1) * BLOCK)
            within = C[s, rows, :]
            centre = within[BLOCK // 2 - 1 : BLOCK // 2]
            query, keys = Q[s, rows, :], K[s, rows, :]
            scores = dot(
                (query * jnp.exp(within - centre)).astype(BF16),
                (keys * jnp.exp(centre - within)).astype(BF16),
                NT,
            )
            scores = jnp.where(causal, scores, 0.0).astype(BF16)
            INS[s, rows, :] = dot(scores, V[s, rows, :])
            QE[s, rows, :] = (query * jnp.exp(within)).astype(BF16)
        return 0

    span = lax.shift_left(jnp.int32(2), c * 2 + f // 2)
    ti = lax.broadcasted_iota(jnp.int32, (256, 384), 0)
    si = lax.broadcasted_iota(jnp.int32, (256, 384), 1) - 128
    band = jnp.where((si <= ti) & (si > ti - span) & (si >= -16), 1.0, 0.0).astype(BF16)
    position = here * 256 + lax.broadcasted_iota(jnp.int32, (256, 128), 0)
    inverse = 1.0 / jnp.minimum(position + 1, span).astype(F32)

    def pool(s, _):
        EXT[s, 0:128, :] = jnp.zeros((128, 128), BF16)

        @pl.when(here > 0)
        def _():
            EXT[s, 112:128, :] = BR[s]

        window = dot(band, EXT[s])
        PO[s] = (window * inverse - EXT[s, 128:384, :].astype(F32)).astype(BF16)
        return 0

    given_pool, given_rec = sem(), sem()

    def give_back(buffer, slot, n, sources):
        for s in sources:
            if s == 1:
                ACT[slot + f] = buffer[1]
            else:
                send(n, buffer.at[s], ACT.at[slot + f], {"fs": fat(s - 1)})

    def pooling():
        landed(nb, BR)
        each(pool)
        give_back(PO, 4, given_pool, (0, 2, 3, 1))

    def pass_z(i, state):
        later, fade = unpack_state(ZR[i])
        return jnp.exp(fade) * state + later

    def from_z():
        landed(sz, ZR.at[pl.ds(0, NZ - 1)])

        @pl.when(f != x)
        def _():
            landed(ns, ST)

        state = lax.fori_loop(0, z, pass_z, ST[...].astype(F32))
        for i in range(NX):
            ES[i] = state.astype(BF16)
            if i < NX - 1:
                later, fade = unpack_state(SR[i])
                state = jnp.exp(fade) * state + later
        ER[x] = ES[x]
        for k in (1, 3, 2):
            send(sb, ES.at[xat(k)], ER.at[x], {"sp_1": xat(k)})

    def finish(s, _):
        sequence = fat(s - 1)
        entering = ER[sequence].astype(F32)
        middle = jnp.exp(C[s, BLOCK - 1 : BLOCK, :]) * entering + A0[s]
        for b, state in enumerate((ER[sequence], middle.astype(BF16))):
            rows = slice(b * BLOCK, (b + 1) * BLOCK)
            raw = INS[s, rows, :] + dot(QE[s, rows, :], state, NT)
            square = jnp.mean(raw * raw, axis=1, keepdims=True)
            RO[s, rows, :] = (raw * lax.rsqrt(square + EPSILON) * G[s, rows, :]).astype(BF16)
        return 0

    def finishing():
        landed(sb, ER.at[pl.ds(0, 3)])
        for s in (0, 2, 3, 1):
            finish(s, 0)
            give_back(RO, 0, given_rec, (s,))

    def out_pool():
        landed(given_pool, ACT.at[pl.ds(4, 3)])
        parts = [ACT[4 + i] for i in range(4)]
        b, d = parts[0], jnp.concatenate(parts[1:], axis=1)
        for i in range(4):
            at, cols = slice(2 * i, 2 * i + 2), slice(512 * i, 512 * i + 512)
            total = dot(b, GZ3[at, :, :, 256:].reshape(512, 128), NT)
            PT[:, cols] = total + dot(d, GB[at].reshape(512, WB), NT)

    steps.update(
        SQ=squares_near,
        PR3=project_near,
        PR1=project_far,
        SUMX=total_x,
        REST=rest,
        INNER=lambda: each(inner),
        POOL=pooling,
        PASSZ=from_z,
        FIN=finishing,
        OUTP=out_pool,
    )
    order = ORDER
    assert sorted(order) == sorted(steps)
    for step in order:
        with jax.named_scope(step):
            steps[step]()

    landed(given_rec, ACT.at[pl.ds(0, 3)])

    a, b = (jnp.concatenate([ACT[i], ACT[i + 1]], axis=1) for i in (0, 2))
    my_rows = pl.ds(pl.multiple_of(c * 128, 128), 128)
    their_rows = pl.ds(pl.multiple_of(other * 128, 128), 128)
    swap = sem()
    for i in range(4):
        at, cols = slice(2 * i, 2 * i + 2), slice(512 * i, 512 * i + 512)
        total = PT[:, cols] + dot(a, GX3[at].reshape(512, 256), NT)
        total += dot(b, GZ3[at, :, :, :256].reshape(512, 256), NT)
        PS[:, cols] = total.astype(BF16)
        send(swap, PS.at[their_rows, pl.ds(512 * i, 512)], PR.at[:, pl.ds(512 * i, 512)], {"tp": other})
    landed(swap, PR)
    out[...] = (PS[my_rows, :].astype(F32) + PR[...].astype(F32)).astype(BF16)

    for made in sent[-NSEND:] + sent_long[-NLONG:]:
        made.wait_send()

    @pl.when(f == x)
    def _():
        for made in start_copies():
            made.wait_send()


def per_device(
    tokens,
    norm_gain,
    query_weight,
    forget_weight,
    value_weight,
    outgate_weight,
    pool_in_weight,
    forget_room,
    decay_shift,
    head_gain,
    start_state,
    pool_map,
    pool_scale,
    out_rec_weight,
    out_pool_weight,
):
    vmem = lambda *shape: pltpu.VMEM(shape, F32)
    half = lambda *shape: pltpu.VMEM(shape, BF16)
    mixed = pl.pallas_call(
        kernel,
        out_shape=jax.ShapeDtypeStruct((128, 2048), BF16),
        in_specs=[
            pl.BlockSpec(memory_space=pl.ANY if i in (0, 10, 11) else pltpu.VMEM) for i in range(15)
        ],
        out_specs=pl.BlockSpec(memory_space=pltpu.VMEM),
        scratch_shapes=[
            half(2, 4, 256, 1024),
            half(NZ, NX, 64, WZ[0]),
            half(NZ, NX, 64, WX[0]),
            half(NZ, NX, 64, WZ[1]),
            half(NZ, NX, 64, WX[1]),
            half(NZ, NX, 64, WZ[2]),
            half(NZ, NX, 64, WB),
            vmem(4, 4, 256),
            half(128, 128),
            vmem(4, 256, 128),
            half(4, 256, 128),
            vmem(4, 256, 128),
            vmem(4, 256, 128),
            vmem(4, 256, 128),
            half(4, 256, 128),
            vmem(4, 256, 128),
            vmem(4, 128, 128),
            half(4, 144, 128),
            half(4, 144, 128),
            half(144, 128),
            half(NZ, 144, 128),
            half(4, 128, 128),
            half(4, 128, 128),
            half(4, 384, 128),
            half(4, 16, 128),
            half(4, 16, 128),
            half(4, 256, 128),
            half(4, 256, 128),
            half(8, 256, 128),
            half(256, 2048),
            half(128, 2048),
            vmem(4, 256, 1),
            half(4, 128, 128),
            vmem(4, 128, 128),
            half(2, 256, 256),
            vmem(256, 2048),
            half(4, 16, 256),
            half(4, 16, 256),
            half(4, 16, 128),
            half(16, 640),
            pltpu.SemaphoreType.DMA((NSEND + NLONG + 3,)),
            pltpu.SemaphoreType.DMA((NRECV,)),
            pltpu.SemaphoreType.DMA((3,)),
        ],
        compiler_params=pltpu.CompilerParams(
            collective_id=0, has_side_effects=True, vmem_limit_bytes=60 * 1024 * 1024
        ),
    )(
        tokens[0],
        norm_gain.reshape(16, 128),
        query_weight,
        forget_weight,
        value_weight,
        outgate_weight,
        pool_in_weight,
        forget_room.reshape(4, 128),
        decay_shift[0].T,
        head_gain.reshape(1, 128),
        start_state,
        pool_map,
        pool_scale.reshape(1, 512),
        out_rec_weight.T,
        out_pool_weight.T,
    )
    return mixed[None]


def solution(mesh):
    finer = Mesh(
        mesh.devices.reshape(8, 4, mesh.shape["fs"], mesh.shape["tp"]), ("sp_0", "sp_1", "fs", "tp")
    )
    placed = (
        P("fs", SP, "tp"),
        P(),
        P(SP_FS, "tp"),
        P(SP_FS, "tp"),
        P(SP_FS, "tp"),
        P(SP_FS, "tp"),
        P(SP_FS, "tp"),
        P("tp"),
        P("fs", SP, "tp"),
        P(),
        P("fs", "tp", None, None),
        P("tp", None, None),
        P("tp"),
        P("tp", SP_FS),
        P("tp", SP_FS),
    )
    return jax.shard_map(
        per_device, mesh=finer, in_specs=placed, out_specs=P("fs", SP_TP, None), check_vma=False
    )
```

```python
import functools

import jax
import jax.numpy as jnp
from jax import lax
from jax.experimental import pallas as pl
from jax.experimental.pallas import tpu as pltpu
from jax.sharding import Mesh
from jax.sharding import PartitionSpec as P

HEAD = 128
POOL_DIM = 256
BLOCK = 128
SP_FS = ("sp_0", "sp_1", "fs")
SP = ("sp_0", "sp_1")
SP_TP = ("sp_0", "sp_1", "tp")
EPSILON = 1e-06
MESH = pl.DeviceIdType.MESH
ORDER = (
    "LZ0", "LZ1", "LF0", "1Z0", "2Z0", "3Z0", "1Z1", "1F0", "LZ2", "LX0", "1Z2", "2X0", "T1", "LF1",
    "1F1", "1Z3", "1Z4", "LF2", "LZ3", "2F0", "1F2", "LX1", "T2", "2Z1", "2X1", "LZ4", "1F3", "SQ",
    "1F4", "LX2", "LF3", "3Z1", "2Z2", "3X0", "2X2", "T3", "2F1", "LF4", "LX3", "1L", "PR3", "PR1",
    "2Z3", "2F2", "LL", "3X1", "2X3", "LX4", "Y0", "2Z4", "3Z2", "SUMX", "3F0", "3F1", "2F3", "2X4",
    "2F4", "3F2", "Y1", "2L", "REST", "3Z3", "3X2", "INNER", "PASSZ", "POOL", "3Z4", "3F3", "3X3",
    "FIN", "Y2", "3F4", "3X4", "3L", "OUTP",
)
NRECV, NSEND, NLONG = 77, 40, 13
NZ, NX, NF = 8, 4, 4
WX, WZ, WB, WBX = (128, 256), (256, 256, 256), 512, 256
F32, BF16 = jnp.float32, jnp.bfloat16
NT = (((1,), (1,)), ((), ()))
TN = (((0,), (0,)), ((), ()))


def dot(a, b, dims=(((1,), (0,)), ((), ()))):
    return lax.dot_general(a, b, dims, preferred_element_type=F32)


def pack_state(state, decay):
    high, mid, low = three_parts(decay)
    row = lax.broadcasted_iota(jnp.int32, (16, HEAD), 0)
    tail = jnp.where(row == 0, high, jnp.where(row == 1, mid, jnp.where(row == 2, low, 0.0)))
    return jnp.concatenate([state, tail], axis=0).astype(BF16)


def three_parts(value):
    high = value.astype(BF16).astype(F32)
    rest = value - high
    mid = rest.astype(BF16).astype(F32)
    return high, mid, rest - mid


def unpack_state(packed):
    whole = packed.astype(F32)
    decay = jnp.sum(whole[HEAD : HEAD + 16], axis=0, keepdims=True)
    return whole[:HEAD], decay


def kernel(
    h_tok,
    h_gain,
    h_wq,
    h_wf,
    h_wv,
    h_wo,
    h_wp,
    h_room,
    h_shift,
    h_hgain,
    h_start,
    h_pmap,
    h_pscale,
    h_worec,
    h_wopool,
    out,
    T,
    GZ1,
    GX2,
    GZ2,
    GX3,
    GZ3,
    GB,
    SH,
    ST,
    K,
    V,
    Q,
    G,
    C,
    QE,
    INS,
    A0,
    SL,
    SR,
    ZS,
    ZR,
    ES,
    ER,
    EXT,
    BS,
    BR,
    RO,
    PO,
    ACT,
    PS,
    PR,
    SC,
    SS,
    S0,
    PM,
    PT,
    gain,
    wq,
    wf,
    wv,
    wo,
    wp,
    pscale,
    worec,
    wopool,
    room,
    hgain,
    iz1,
    ix2,
    iz2,
    ixz3,
    send_sems,
    recv_sems,
    local_sems,
):
    z, x = lax.axis_index("sp_0"), lax.axis_index("sp_1")
    f, c = lax.axis_index("fs"), lax.axis_index("tp")
    zat = lambda k: lax.rem(z + (k + NZ), NZ)
    xat = lambda k: lax.rem(x + (k + NX), NX)
    fat = lambda k: lax.rem(f + (k + NF), NF)
    other = 1 - c
    here = z * NX + x
    after = lax.rem(here + 1, NZ * NX)
    ahead = lax.rem(here + NZ * NX - 1, NZ * NX)
    nxt = {"sp_0": after // NX, "sp_1": lax.rem(after, NX)}
    prv = {"sp_0": ahead // NX, "sp_1": lax.rem(ahead, NX)}

    arguments = (
        (h_gain, gain),
        (h_wf, wf),
        (h_wv, wv),
        (h_wq, wq),
        (h_wo, wo),
        (h_wp, wp),
        (h_pmap, PM),
        (h_pscale, pscale),
        (h_worec, worec),
        (h_wopool, wopool),
        (h_tok, T.at[c, 1]),
        (h_shift, SH.at[1]),
        (h_start.at[0], S0),
        (h_room, room),
        (h_hgain, hgain),
    )
    taken = [pltpu.make_async_copy(a, b, local_sems.at[i]) for i, (a, b) in enumerate(arguments)]
    for made in taken:
        made.start()

    barrier = pltpu.get_barrier_semaphore()
    met = [{"tp": other}, nxt, prv]
    met += [{"fs": fat(k)} for k in (1, 2, 3)] + [{"sp_1": xat(k)} for k in (1, 2, 3)]
    met += [{"sp_0": zat(k)} for k in range(1, NZ)]
    for who in met:
        pl.semaphore_signal(barrier, inc=1, device_id=who, device_id_type=MESH)

    count = [0]
    sent, sent_long = [], []

    def sem():
        count[0] += 1
        assert count[0] <= NRECV
        return count[0] - 1

    def copy(n, src, dst, who, slot=0):
        return pltpu.make_async_remote_copy(
            src_ref=src,
            dst_ref=dst,
            send_sem=send_sems.at[slot],
            recv_sem=recv_sems.at[n],
            device_id=who,
            device_id_type=MESH,
        )

    def send(n, src, dst, who, long=False):
        made_before, slots, base = (sent_long, NLONG, NSEND) if long else (sent, NSEND, 0)
        if len(made_before) >= slots:
            made_before[-slots].wait_send()
        made = copy(n, src, dst, who, base + len(made_before) % slots)
        made.start()
        made_before.append(made)

    def landed(n, dst):
        copy(n, dst, dst, {"tp": other}).wait_recv()

    rank = here * NF + f
    row = lax.broadcasted_iota(jnp.int32, (16, 128), 0)
    lane = lax.broadcasted_iota(jnp.int32, (16, 128), 1)
    for made in taken[:3]:
        made.wait()
    gains = jnp.broadcast_to(gain[pl.ds(rank // 8, 1), :], (16, 128))
    gains = jnp.where(lane == lax.rem(rank, 8) * 16 + row, gains, 0.0)
    gains = jnp.sum(gains, axis=1, keepdims=True)
    mine = pl.ds(pl.multiple_of(f * 16, 16), 16)

    def stage(buffer, place, weights):
        for i in range(NF):
            chunk = [w[:, 128 * i : 128 * i + 128] for w in weights]
            buffer[i] = jnp.concatenate(chunk, axis=1)
        place[z, x, mine, :] = buffer[f]

    def scaled(w):
        return (w[...].astype(F32) * gains).astype(BF16)

    stage(iz1, GZ1, (scaled(wf), scaled(wv)))
    pl.semaphore_wait(barrier, len(met))

    def over_y(pairs):
        ns = [sem() for _ in pairs]
        for k in (1, 3, 2):
            to = fat(k)
            for n, (buffer, own) in zip(ns, pairs):
                send(n, own.at[to], buffer.at[z, x, mine, :], {"fs": to})
        return [(n, buffer.at[z, x, pl.ds(0, 48), :]) for n, (buffer, _) in zip(ns, pairs)]

    def over_out():
        ns = sem(), sem()
        for k in (1, 3, 2):
            to = {"fs": fat(k)}
            send(ns[0], ixz3.at[:, pl.ds(0, 256)], GX3.at[z, x, mine, :], to)
            send(ns[1], ixz3.at[:, pl.ds(256, 256)], GZ3.at[z, x, mine, :], to)
        return [(n, b.at[z, x, pl.ds(0, 48), :]) for n, b in zip(ns, (GX3, GZ3))]

    y1 = over_y(((GZ1, iz1),))
    for made in taken[3:12]:
        made.wait()
    folded = [dot(wp[:, 256 * i : 256 * i + 256], PM[i]) for i in range(2)]
    folded = (jnp.concatenate(folded, axis=1) * gains * pscale[...]).astype(BF16)
    turned = jnp.concatenate([worec[...], wopool[...]], axis=1)
    stage(ix2, GX2, (scaled(wq),))
    stage(iz2, GZ2, (scaled(wo), folded))
    ixz3[...] = turned[:, :512]
    GX3[z, x, mine, :] = turned[:, :256]
    GZ3[z, x, mine, :] = turned[:, 256:512]
    GB[z, x, mine, :] = turned[:, 512:]
    y2 = over_y(((GX2, ix2), (GZ2, iz2)))
    y3 = over_out()
    nshift = sem()
    for k in (1, 3, 2):
        send(nshift, SH.at[1], SH.at[(5 - k) % 4], {"fs": fat(k)})

    first, second = pl.ds(0, 128), pl.ds(128, 128)
    right, left = {"fs": fat(1)}, {"fs": fat(3)}
    nt = [sem() for _ in range(3)]
    near, far_off = sem(), sem()

    def relay(n, seq, rows):
        send(n, T.at[c, seq, rows, :], T.at[c, seq, rows, :], {"tp": other}, True)

    for i, (a, b) in enumerate(((first, second), (second, first))):
        send(nt[i], T.at[c, 1, a, :], T.at[c, 0, a, :], right, True)
        send(nt[i], T.at[c, 1, b, :], T.at[c, 2, b, :], left, True)
    send(near, T.at[c, 1], T.at[c, 1], {"tp": other}, True)

    def tokens_1():
        landed(nt[0], T.at[c, 0])
        send(nt[2], T.at[c, 0, first, :], T.at[c, 3, first, :], right, True)
        send(nt[2], T.at[c, 2, second, :], T.at[c, 3, second, :], left, True)
        relay(near, 0, first)
        relay(near, 2, second)

    def tokens_2():
        landed(nt[1], T.at[c, 0])
        relay(near, 0, second)
        relay(near, 2, first)

    def tokens_3():
        landed(nt[2], T.at[c, 3])
        relay(far_off, 3, first)
        relay(far_off, 3, second)

    steps = {"T1": tokens_1, "T2": tokens_2, "T3": tokens_3}

    def plane(name, waits, vx, vz, direct=False):
        zr, zl = {"sp_0": zat(1)}, {"sp_0": zat(-1)}
        xr, xl = {"sp_1": xat(1)}, {"sp_1": xat(-1)}
        whole, lowx, highx = pl.ds(0, 4), pl.ds(0, 2), pl.ds(2, 2)
        nz, ns, last = [sem() for _ in range(4)], [sem() for _ in range(5)], sem()
        if vx:
            xs, mz = sem(), [sem() for _ in range(4)]
        offsets = ((0,), (-1, 1), (-2, 2), (-3, 3), (4,))

        def spread(k):
            for offset in offsets[k]:
                at = zat(offset)
                send(ns[k], vz(at, x), vz(at, x), xr)
                send(ns[k], vz(at, x), vz(at, x), xl)

        def z_step(k):
            if k == 0:
                for w in waits:
                    landed(*w)
                if vx:
                    for i in (1, 3, 2):
                        send(xs, vx(z, x), vx(z, x), {"sp_1": xat(i)})
                for i in (1, 2, 4, 3) if direct else (1,):
                    for step in (i, -i) if i < 4 else (i,):
                        send(nz[i - 1], vz(z, x), vz(z, x), {"sp_0": zat(step)})
            else:
                landed(nz[k - 1], vz(z, pl.ds(0, 2)) if k < 4 else vz(z, x))
                if k < 4 and not direct:
                    part = vz(zat(-k), x, 1 if k == 3 else 0)
                    send(nz[k], part, part, zr)
                    part = vz(zat(k), x, 2 if k == 3 else 0)
                    send(nz[k], part, part, zl)
            spread(k)

        def x_step(k):
            if k == 0:
                landed(xs, vx(z, pl.ds(0, 3)))
                send(mz[0], vx(z, whole), vx(z, whole), zr)
                send(mz[0], vx(z, whole), vx(z, whole), zl)
                return
            landed(mz[k - 1], vx(pl.ds(0, 2), whole) if k < 4 else vx(z, whole))
            if k < 4:
                part = vx(zat(-k), lowx if k == 3 else whole)
                send(mz[k], part, part, zr)
                part = vx(zat(k), highx if k == 3 else whole)
                send(mz[k], part, part, zl)

        def f_step(k):
            landed(ns[k], vz(z, pl.ds(0, 2 * len(offsets[k]))))
            for offset in offsets[k]:
                at = zat(offset)
                if 0 <= offset < 4:
                    send(last, vz(at, xat(-1)), vz(at, xat(-1)), xr)
                else:
                    send(last, vz(at, xat(1)), vz(at, xat(1)), xl)

        for k in range(5):
            steps[f"{name}Z{k}"] = functools.partial(z_step, k)
            steps[f"{name}F{k}"] = functools.partial(f_step, k)
            if vx:
                steps[f"{name}X{k}"] = functools.partial(x_step, k)
        steps[f"{name}L"] = lambda: landed(last, vz(pl.ds(0, NZ), x))

    def views(GX, GZ):
        halves = (None, pl.ds(0, 32), pl.ds(32, 32))

        def vz(zi, xi, part=0):
            return GZ.at[zi, xi, halves[part], :] if part else GZ.at[zi, xi]

        return (GX is not None) and (lambda zi, xi: GX.at[zi, xi]), vz

    lanes = (pl.ds(WBX, 256), pl.ds(WBX, 128), pl.ds(WBX + 128, 128))
    plane(
        "L",
        (),
        lambda zi, xi: GB.at[zi, xi, mine, pl.ds(0, WBX)],
        lambda zi, xi, part=0: GB.at[zi, xi, mine, lanes[part]],
    )

    half_z, other_half = pl.ds(0, 4), pl.ds(4, 4)
    ny = sem(), sem()

    def late_part(k, half):
        rows = pl.ds(pl.multiple_of(fat(k) * 16, 16), 16)
        return GB.at[half, :, rows, :]

    def late_y0():
        for n, (a, b) in zip(ny, ((half_z, other_half), (other_half, half_z))):
            send(n, late_part(0, a), late_part(0, a), right, True)
            send(n, late_part(0, b), late_part(0, b), left, True)

    def late_y1():
        landed(ny[0], late_part(0, pl.ds(0, NZ)))
        send(ny[1], late_part(-1, half_z), late_part(-1, half_z), right, True)
        send(ny[1], late_part(1, other_half), late_part(1, other_half), left, True)

    def late_y2():
        landed(ny[1], GB.at[:, :, pl.ds(0, 32), :])

    steps.update(Y0=late_y0, Y1=late_y1, Y2=late_y2)
    plane("1", y1, *views(None, GZ1), direct=True)
    plane("2", y2, *views(GX2, GZ2))
    plane("3", y3, *views(GX3, GZ3))

    ns = sem()

    def start_copies():
        return [copy(ns, SS.at[fat(k)], ST, {"fs": fat(k)}, NSEND + NLONG + i) for i, k in enumerate((1, 2, 3))]

    for made in taken[12:]:
        made.wait()

    @pl.when(f == x)
    def _():
        for i in range(NF):
            SS[i] = jnp.transpose(S0[i]).astype(BF16)
        ST[...] = SS[f]
        for made in start_copies():
            made.start()

    def squares(s):
        w0, w1 = T[0, s].astype(F32), T[1, s].astype(F32)
        square = jnp.sum(w0 * w0 + w1 * w1, axis=1, keepdims=True)
        SC[s] = lax.rsqrt(square * (1.0 / 2048) + EPSILON)

    i0 = lax.broadcasted_iota(jnp.int32, (BLOCK, BLOCK), 0)
    i1 = lax.broadcasted_iota(jnp.int32, (BLOCK, BLOCK), 1)
    causal = i0 >= i1
    tril = jnp.where(causal, 1.0, 0.0).astype(BF16)
    my_room = room[pl.ds(f, 1), :]

    half = NZ // 2

    def each(body):
        for s in range(4):
            body(s, 0)

    def through(slots, *weights):
        count = len(slots) * 256
        at = slice(slots[0], slots[-1] + 1)
        low = jnp.concatenate([w[:half].reshape(1024, w.shape[-1]) for w in weights], axis=1)
        high = jnp.concatenate([w[half:].reshape(1024, w.shape[-1]) for w in weights], axis=1)
        total = dot(T[0, at].reshape(count, 1024), low) + dot(T[1, at].reshape(count, 1024), high)
        total = total * SC[at].reshape(count, 1)
        return [total[256 * i : 256 * i + 256] for i in range(len(slots))]

    def project(slots):
        keys, values, parts, spread = [], [], [], []
        halves = (slice(0, BLOCK), slice(BLOCK, 2 * BLOCK))
        for s, both in zip(slots, through(slots, GZ1)):
            keys.append(my_room * jax.nn.sigmoid(-both[:, :128]))
            values.append(both[:, 128:].astype(BF16))
            K[s], V[s] = keys[-1], values[-1]
        for s, key in zip(slots, keys):
            logs = [p.astype(BF16) for p in three_parts(jnp.log1p(-key))]
            lags = three_parts(SH[s, pl.ds(f, 1), :])
            for rows in halves:
                parts.append(jnp.concatenate([p[rows] for p in logs], axis=0))
                masked = [jnp.broadcast_to(p[:, rows], (BLOCK, BLOCK)) for p in lags]
                masked = [jnp.where(causal, p, 0.0).astype(BF16) for p in masked]
                spread.append(jnp.concatenate(masked, axis=1))
        within = dot(jnp.concatenate([tril] * 3, axis=1), jnp.concatenate(parts, axis=1))
        shifts = dot(jnp.concatenate(spread, axis=0), jnp.ones((3 * BLOCK, BLOCK), BF16))
        ends, faded = [], []
        for i in range(2 * len(slots)):
            block = slice(i * BLOCK, i * BLOCK + BLOCK)
            total = within[:, block] + shifts[block]
            s, rows = slots[i // 2], halves[i % 2]
            C[s, rows, :] = total
            ends.append(total[BLOCK - 1 :])
            faded.append((keys[i // 2][rows] * jnp.exp(ends[-1] - total)).astype(BF16))
        adds = [dot(values[i // 2][halves[i % 2]], k, TN) for i, k in enumerate(faded)]
        for i, s in enumerate(slots):
            A0[s] = adds[2 * i]
            state = jnp.exp(ends[2 * i + 1]) * adds[2 * i] + adds[2 * i + 1]
            SL[s] = pack_state(state, ends[2 * i] + ends[2 * i + 1])

    sx, sz, sb, nb = sem(), sem(), sem(), sem()

    def squares_near():
        landed(near, T.at[other, pl.ds(0, 3)])
        for s in range(3):
            squares(s)

    def project_near():
        landed(nshift, SH.at[pl.ds(0, 3)])
        project((0, 1, 2))

    def project_far():
        landed(far_off, T.at[other, 3])
        squares(3)
        project((3,))
        slot_of = lambda sequence: lax.rem(sequence - f + (NF + 1), NF)
        SR[x] = SL[slot_of(x)]
        for k in (1, 3, 2):
            send(sx, SL.at[slot_of(xat(k))], SR.at[x], {"sp_1": xat(k)})

    def total_x():
        landed(sx, SR.at[pl.ds(0, 3)])
        state, decay = unpack_state(SR[0])
        for i in range(1, NX):
            later, fade = unpack_state(SR[i])
            state, decay = jnp.exp(fade) * state + later, decay + fade
        ZS[...] = pack_state(state, decay)
        for k in (4, 3, 5, 2, 6, 1, 7):
            send(sz, ZS, ZR.at[z], {"sp_0": zat(k)})

    def project_rest(s, rest):
        query = rest[:, :128]
        Q[s] = query * jax.nn.sigmoid(query) * HEAD ** (-0.5)
        gate = rest[:, 128:256]
        G[s] = gate * jax.nn.sigmoid(gate) * hgain[...]
        pool = rest[:, 256:].astype(BF16)
        EXT[s, 128:384, :] = pool
        BS[s] = pool[240:256]

    def rest():
        for slots in ((0, 1), (2, 3)):
            for s, projected in zip(slots, through(slots, GX2, GZ2)):
                project_rest(s, projected)
        send(nb, BS, BR, nxt)

    def inner(s, _):
        for b in range(2):
            rows = slice(b * BLOCK, (b + 1) * BLOCK)
            within = C[s, rows, :]
            centre = within[BLOCK // 2 - 1 : BLOCK // 2]
            query, keys = Q[s, rows, :], K[s, rows, :]
            scores = dot(
                (query * jnp.exp(within - centre)).astype(BF16),
                (keys * jnp.exp(centre - within)).astype(BF16),
                NT,
            )
            scores = jnp.where(causal, scores, 0.0).astype(BF16)
            INS[s, rows, :] = dot(scores, V[s, rows, :])
            QE[s, rows, :] = (query * jnp.exp(within)).astype(BF16)
        return 0

    span = lax.shift_left(jnp.int32(2), c * 2 + f // 2)
    ti = lax.broadcasted_iota(jnp.int32, (256, 384), 0)
    si = lax.broadcasted_iota(jnp.int32, (256, 384), 1) - 128
    band = jnp.where((si <= ti) & (si > ti - span) & (si >= -16), 1.0, 0.0).astype(BF16)
    position = here * 256 + lax.broadcasted_iota(jnp.int32, (256, 128), 0)
    inverse = 1.0 / jnp.minimum(position + 1, span).astype(F32)

    def pool(s, _):
        EXT[s, 0:128, :] = jnp.zeros((128, 128), BF16)

        @pl.when(here > 0)
        def _():
            EXT[s, 112:128, :] = BR[s]

        window = dot(band, EXT[s])
        PO[s] = (window * inverse - EXT[s, 128:384, :].astype(F32)).astype(BF16)
        return 0

    given_pool, given_rec = sem(), sem()

    def give_back(buffer, slot, n, sources):
        for s in sources:
            if s == 1:
                ACT[slot + f] = buffer[1]
            else:
                send(n, buffer.at[s], ACT.at[slot + f], {"fs": fat(s - 1)})

    def pooling():
        landed(nb, BR)
        each(pool)
        give_back(PO, 4, given_pool, (0, 2, 3, 1))

    def pass_z(i, state):
        later, fade = unpack_state(ZR[i])
        return jnp.exp(fade) * state + later

    def from_z():
        landed(sz, ZR.at[pl.ds(0, NZ - 1)])

        @pl.when(f != x)
        def _():
            landed(ns, ST)

        state = lax.fori_loop(0, z, pass_z, ST[...].astype(F32))
        for i in range(NX):
            ES[i] = state.astype(BF16)
            if i < NX - 1:
                later, fade = unpack_state(SR[i])
                state = jnp.exp(fade) * state + later
        ER[x] = ES[x]
        for k in (1, 3, 2):
            send(sb, ES.at[xat(k)], ER.at[x], {"sp_1": xat(k)})

    def finishing():
        landed(sb, ER.at[pl.ds(0, 3)])
        raws, order = {}, (3, 0, 2, 1)
        for s in order:
            entering = ER[fat(s - 1)]
            middle = jnp.exp(C[s, BLOCK - 1 : BLOCK, :]) * entering.astype(F32) + A0[s]
            carried = [dot(QE[s, :BLOCK, :], entering, NT), dot(QE[s, BLOCK:, :], middle.astype(BF16), NT)]
            raws[s] = INS[s] + jnp.concatenate(carried, axis=0)
        for s in order:
            square = jnp.mean(raws[s] * raws[s], axis=1, keepdims=True)
            RO[s] = (raws[s] * lax.rsqrt(square + EPSILON) * G[s]).astype(BF16)
            give_back(RO, 0, given_rec, (s,))

    def out_pool():
        landed(given_pool, ACT.at[pl.ds(4, 3)])
        act = jnp.concatenate([ACT[4 + i] for i in range(4)], axis=1)
        for i in range(4):
            at, cols = slice(2 * i, 2 * i + 2), slice(512 * i, 512 * i + 512)
            PT[:, cols] = dot(act, GB[at].reshape(512, WB), NT)

    steps.update(
        SQ=squares_near,
        PR3=project_near,
        PR1=project_far,
        SUMX=total_x,
        REST=rest,
        INNER=lambda: each(inner),
        POOL=pooling,
        PASSZ=from_z,
        FIN=finishing,
        OUTP=out_pool,
    )
    order = ORDER
    assert sorted(order) == sorted(steps)
    for step in order:
        with jax.named_scope(step):
            steps[step]()

    landed(given_rec, ACT.at[pl.ds(0, 3)])

    act = jnp.concatenate([ACT[i] for i in range(4)], axis=1)
    my_rows = pl.ds(pl.multiple_of(c * 128, 128), 128)
    their_rows = pl.ds(pl.multiple_of(other * 128, 128), 128)
    swap = sem()
    for i in range(4):
        at, cols = slice(2 * i, 2 * i + 2), slice(512 * i, 512 * i + 512)
        weight = [w[at].reshape(512, w.shape[-1]) for w in (GX3, GZ3)]
        total = PT[:, cols] + dot(act, jnp.concatenate(weight, axis=1), NT)
        PS[:, cols] = total.astype(BF16)
        send(swap, PS.at[their_rows, pl.ds(512 * i, 512)], PR.at[:, pl.ds(512 * i, 512)], {"tp": other})
    landed(swap, PR)
    out[...] = (PS[my_rows, :].astype(F32) + PR[...].astype(F32)).astype(BF16)

    for made in sent[-NSEND:] + sent_long[-NLONG:]:
        made.wait_send()

    @pl.when(f == x)
    def _():
        for made in start_copies():
            made.wait_send()


def per_device(
    tokens,
    norm_gain,
    query_weight,
    forget_weight,
    value_weight,
    outgate_weight,
    pool_in_weight,
    forget_room,
    decay_shift,
    head_gain,
    start_state,
    pool_map,
    pool_scale,
    out_rec_weight,
    out_pool_weight,
):
    vmem = lambda *shape: pltpu.VMEM(shape, F32)
    half = lambda *shape: pltpu.VMEM(shape, BF16)
    mixed = pl.pallas_call(
        kernel,
        out_shape=jax.ShapeDtypeStruct((128, 2048), BF16),
        in_specs=[pl.BlockSpec(memory_space=pltpu.HBM)] * 15,
        out_specs=pl.BlockSpec(memory_space=pltpu.VMEM),
        scratch_shapes=[
            half(2, 4, 256, 1024),
            half(NZ, NX, 64, WZ[0]),
            half(NZ, NX, 64, WX[0]),
            half(NZ, NX, 64, WZ[1]),
            half(NZ, NX, 64, WX[1]),
            half(NZ, NX, 64, WZ[2]),
            half(NZ, NX, 64, WB),
            vmem(4, 4, 256),
            half(128, 128),
            vmem(4, 256, 128),
            half(4, 256, 128),
            vmem(4, 256, 128),
            vmem(4, 256, 128),
            vmem(4, 256, 128),
            half(4, 256, 128),
            vmem(4, 256, 128),
            vmem(4, 128, 128),
            half(4, 144, 128),
            half(4, 144, 128),
            half(144, 128),
            half(NZ, 144, 128),
            half(4, 128, 128),
            half(4, 128, 128),
            half(4, 384, 128),
            half(4, 16, 128),
            half(4, 16, 128),
            half(4, 256, 128),
            half(4, 256, 128),
            half(8, 256, 128),
            half(256, 2048),
            half(128, 2048),
            vmem(4, 256, 1),
            half(4, 128, 128),
            vmem(4, 128, 128),
            half(2, 256, 256),
            vmem(256, 2048),
            vmem(16, 128),
            *[half(16, 512)] * 5,
            vmem(1, 512),
            *[half(16, 512)] * 2,
            vmem(4, 128),
            vmem(1, 128),
            half(4, 16, 256),
            half(4, 16, 128),
            half(4, 16, 256),
            half(16, 512),
            pltpu.SemaphoreType.DMA((NSEND + NLONG + 3,)),
            pltpu.SemaphoreType.DMA((NRECV,)),
            pltpu.SemaphoreType.DMA((15,)),
        ],
        compiler_params=pltpu.CompilerParams(
            collective_id=0, has_side_effects=True, vmem_limit_bytes=60 * 1024 * 1024
        ),
    )(
        tokens[0],
        norm_gain.reshape(16, 128),
        query_weight,
        forget_weight,
        value_weight,
        outgate_weight,
        pool_in_weight,
        forget_room.reshape(4, 128),
        decay_shift[0].T,
        head_gain.reshape(1, 128),
        start_state,
        pool_map,
        pool_scale.reshape(1, 512),
        out_rec_weight.T,
        out_pool_weight.T,
    )
    return mixed[None]


def solution(mesh):
    finer = Mesh(
        mesh.devices.reshape(8, 4, mesh.shape["fs"], mesh.shape["tp"]), ("sp_0", "sp_1", "fs", "tp")
    )
    placed = (
        P("fs", SP, "tp"),
        P(),
        P(SP_FS, "tp"),
        P(SP_FS, "tp"),
        P(SP_FS, "tp"),
        P(SP_FS, "tp"),
        P(SP_FS, "tp"),
        P("tp"),
        P("fs", SP, "tp"),
        P(),
        P("fs", "tp", None, None),
        P("tp", None, None),
        P("tp"),
        P("tp", SP_FS),
        P("tp", SP_FS),
    )
    return jax.shard_map(
        per_device, mesh=finer, in_specs=placed, out_specs=P("fs", SP_TP, None), check_vma=False
    )
```

```python
import functools

import jax
import jax.numpy as jnp
from jax import lax
from jax.experimental import pallas as pl
from jax.experimental.pallas import tpu as pltpu
from jax.sharding import Mesh
from jax.sharding import PartitionSpec as P

HEAD = 128
POOL_DIM = 256
BLOCK = 128
SP_FS = ("sp_0", "sp_1", "fs")
SP = ("sp_0", "sp_1")
SP_TP = ("sp_0", "sp_1", "tp")
EPSILON = 1e-06
MESH = pl.DeviceIdType.MESH
ORDER = (
    "LZ0",
    "LZ1",
    "LF0",
    "1Z0",
    "LX0",
    "3Z0",
    "LZ2",
    "LF1",
    "2Z0",
    "1Z1",
    "1Z2",
    "LF2",
    "T1",
    "2X0",
    "1F0",
    "1Z3",
    "1Z4",
    "LX1",
    "1F1",
    "LZ3",
    "2Z1",
    "1F2",
    "2X1",
    "T2",
    "LX2",
    "LZ4",
    "1F3",
    "3X0",
    "1F4",
    "2F0",
    "SQ",
    "2Z2",
    "LF3",
    "2F1",
    "LX3",
    "LF4",
    "3Z1",
    "T3",
    "1L",
    "PR3",
    "PR1",
    "2Z3",
    "2X2",
    "LX4",
    "LL",
    "Y0",
    "2F2",
    "3X1",
    "2Z4",
    "3Z2",
    "2X3",
    "SUMX",
    "2F3",
    "3F0",
    "3F1",
    "2F4",
    "3Z3",
    "Y1",
    "3F2",
    "2L",
    "2X4",
    "REST",
    "3X2",
    "3F3",
    "INNER",
    "PASSZ",
    "3Z4",
    "POOL",
    "3X3",
    "FIN",
    "3F4",
    "Y2",
    "3X4",
    "OUTP",
    "3L",
)
NRECV, NSEND, NLONG = 77, 40, 13
NZ, NX, NF = 8, 4, 4
WX, WZ, WB, WBX = (128, 256), (256, 256, 256), 512, 256
F32, BF16 = jnp.float32, jnp.bfloat16
NT = (((1,), (1,)), ((), ()))
TN = (((0,), (0,)), ((), ()))


def dot(a, b, dims=(((1,), (0,)), ((), ()))):
    return lax.dot_general(a, b, dims, preferred_element_type=F32)


def pack_state(state, decay):
    high, mid, low = three_parts(decay)
    row = lax.broadcasted_iota(jnp.int32, (16, HEAD), 0)
    tail = jnp.where(row == 0, high, jnp.where(row == 1, mid, jnp.where(row == 2, low, 0.0)))
    return jnp.concatenate([state, tail], axis=0).astype(BF16)


def three_parts(value):
    high = value.astype(BF16).astype(F32)
    rest = value - high
    mid = rest.astype(BF16).astype(F32)
    return high, mid, rest - mid


def unpack_state(packed):
    whole = packed.astype(F32)
    decay = jnp.sum(whole[HEAD : HEAD + 16], axis=0, keepdims=True)
    return whole[:HEAD], decay


def kernel(
    h_tok,
    h_gain,
    h_wq,
    h_wf,
    h_wv,
    h_wo,
    h_wp,
    h_room,
    h_shift,
    h_hgain,
    h_start,
    h_pmap,
    h_pscale,
    h_worec,
    h_wopool,
    out,
    T,
    GZ1,
    GX2,
    GZ2,
    GX3,
    GZ3,
    GB,
    SH,
    ST,
    K,
    V,
    Q,
    G,
    C,
    QE,
    INS,
    A0,
    SL,
    SR,
    ZS,
    ZR,
    ES,
    ER,
    EXT,
    BS,
    BR,
    RO,
    PO,
    ACT,
    PS,
    PR,
    SC,
    SS,
    S0,
    PM,
    PT,
    gain,
    wq,
    wf,
    wv,
    wo,
    wp,
    pscale,
    worec,
    wopool,
    room,
    hgain,
    iz1,
    ix2,
    iz2,
    ixz3,
    send_sems,
    recv_sems,
    local_sems,
):
    z, x = lax.axis_index("sp_0"), lax.axis_index("sp_1")
    f, c = lax.axis_index("fs"), lax.axis_index("tp")
    zat = lambda k: lax.rem(z + (k + NZ), NZ)
    xat = lambda k: lax.rem(x + (k + NX), NX)
    fat = lambda k: lax.rem(f + (k + NF), NF)
    other = 1 - c
    here = z * NX + x
    after = lax.rem(here + 1, NZ * NX)
    ahead = lax.rem(here + NZ * NX - 1, NZ * NX)
    nxt = {"sp_0": after // NX, "sp_1": lax.rem(after, NX)}
    prv = {"sp_0": ahead // NX, "sp_1": lax.rem(ahead, NX)}

    arguments = (
        (h_gain, gain),
        (h_wf, wf),
        (h_wv, wv),
        (h_wq, wq),
        (h_wo, wo),
        (h_wp, wp),
        (h_pmap, PM),
        (h_pscale, pscale),
        (h_worec, worec),
        (h_wopool, wopool),
        (h_tok, T.at[c, 1]),
        (h_shift, SH.at[1]),
        (h_start.at[0], S0),
        (h_room, room),
        (h_hgain, hgain),
    )
    taken = [pltpu.make_async_copy(a, b, local_sems.at[i]) for i, (a, b) in enumerate(arguments)]
    for made in taken:
        made.start()

    barrier = pltpu.get_barrier_semaphore()
    met = [{"tp": other}, nxt, prv]
    met += [{"fs": fat(k)} for k in (1, 2, 3)] + [{"sp_1": xat(k)} for k in (1, 2, 3)]
    met += [{"sp_0": zat(k)} for k in range(1, NZ)]
    for who in met:
        pl.semaphore_signal(barrier, inc=1, device_id=who, device_id_type=MESH)

    count = [0]
    sent, sent_long = [], []

    def sem():
        count[0] += 1
        assert count[0] <= NRECV
        return count[0] - 1

    def copy(n, src, dst, who, slot=0):
        return pltpu.make_async_remote_copy(
            src_ref=src,
            dst_ref=dst,
            send_sem=send_sems.at[slot],
            recv_sem=recv_sems.at[n],
            device_id=who,
            device_id_type=MESH,
        )

    def send(n, src, dst, who, long=False):
        made_before, slots, base = (sent_long, NLONG, NSEND) if long else (sent, NSEND, 0)
        if len(made_before) >= slots:
            made_before[-slots].wait_send()
        made = copy(n, src, dst, who, base + len(made_before) % slots)
        made.start()
        made_before.append(made)

    def landed(n, dst):
        copy(n, dst, dst, {"tp": other}).wait_recv()

    rank = here * NF + f
    row = lax.broadcasted_iota(jnp.int32, (16, 128), 0)
    lane = lax.broadcasted_iota(jnp.int32, (16, 128), 1)
    for made in taken[:3]:
        made.wait()
    gains = jnp.broadcast_to(gain[pl.ds(rank // 8, 1), :], (16, 128))
    gains = jnp.where(lane == lax.rem(rank, 8) * 16 + row, gains, 0.0)
    gains = jnp.sum(gains, axis=1, keepdims=True)
    mine = pl.ds(pl.multiple_of(f * 16, 16), 16)

    def stage(buffer, place, weights):
        for i in range(NF):
            chunk = [w[:, 128 * i : 128 * i + 128] for w in weights]
            buffer[i] = jnp.concatenate(chunk, axis=1)
        place[z, x, mine, :] = buffer[f]

    def scaled(w):
        return (w[...].astype(F32) * gains).astype(BF16)

    stage(iz1, GZ1, (scaled(wf), scaled(wv)))
    pl.semaphore_wait(barrier, len(met))

    def over_y(pairs):
        ns = [sem() for _ in pairs]
        for k in (1, 3, 2):
            to = fat(k)
            for n, (buffer, own) in zip(ns, pairs):
                send(n, own.at[to], buffer.at[z, x, mine, :], {"fs": to})
        return [(n, buffer.at[z, x, pl.ds(0, 48), :]) for n, (buffer, _) in zip(ns, pairs)]

    def over_out():
        ns = sem(), sem()
        for k in (1, 3, 2):
            to = {"fs": fat(k)}
            send(ns[0], ixz3.at[:, pl.ds(0, 256)], GX3.at[z, x, mine, :], to)
            send(ns[1], ixz3.at[:, pl.ds(256, 256)], GZ3.at[z, x, mine, :], to)
        return [(n, b.at[z, x, pl.ds(0, 48), :]) for n, b in zip(ns, (GX3, GZ3))]

    y1 = over_y(((GZ1, iz1),))
    for made in taken[3:12]:
        made.wait()
    folded = [dot(wp[:, 256 * i : 256 * i + 256], PM[i]) for i in range(2)]
    folded = (jnp.concatenate(folded, axis=1) * gains * pscale[...]).astype(BF16)
    turned = jnp.concatenate([worec[...], wopool[...]], axis=1)
    stage(ix2, GX2, (scaled(wq),))
    stage(iz2, GZ2, (scaled(wo), folded))
    ixz3[...] = turned[:, :512]
    GX3[z, x, mine, :] = turned[:, :256]
    GZ3[z, x, mine, :] = turned[:, 256:512]
    GB[z, x, mine, :] = turned[:, 512:]
    y2 = over_y(((GX2, ix2), (GZ2, iz2)))
    y3 = over_out()
    nshift = sem()
    for k in (1, 3, 2):
        send(nshift, SH.at[1], SH.at[(5 - k) % 4], {"fs": fat(k)})

    first, second = pl.ds(0, 128), pl.ds(128, 128)
    right, left = {"fs": fat(1)}, {"fs": fat(3)}
    nt = [sem() for _ in range(3)]
    near, far_off = sem(), sem()

    def relay(n, seq, rows):
        send(n, T.at[c, seq, rows, :], T.at[c, seq, rows, :], {"tp": other}, True)

    for i, (a, b) in enumerate(((first, second), (second, first))):
        send(nt[i], T.at[c, 1, a, :], T.at[c, 0, a, :], right, True)
        send(nt[i], T.at[c, 1, b, :], T.at[c, 2, b, :], left, True)
    send(near, T.at[c, 1], T.at[c, 1], {"tp": other}, True)

    def tokens_1():
        landed(nt[0], T.at[c, 0])
        send(nt[2], T.at[c, 0, first, :], T.at[c, 3, first, :], right, True)
        send(nt[2], T.at[c, 2, second, :], T.at[c, 3, second, :], left, True)
        relay(near, 0, first)
        relay(near, 2, second)

    def tokens_2():
        landed(nt[1], T.at[c, 0])
        relay(near, 0, second)
        relay(near, 2, first)

    def tokens_3():
        landed(nt[2], T.at[c, 3])
        relay(far_off, 3, first)
        relay(far_off, 3, second)

    steps = {"T1": tokens_1, "T2": tokens_2, "T3": tokens_3}

    def plane(name, waits, vx, vz, direct=False):
        zr, zl = {"sp_0": zat(1)}, {"sp_0": zat(-1)}
        xr, xl = {"sp_1": xat(1)}, {"sp_1": xat(-1)}
        whole, lowx, highx = pl.ds(0, 4), pl.ds(0, 2), pl.ds(2, 2)
        nz, ns, last = [sem() for _ in range(4)], [sem() for _ in range(5)], sem()
        if vx:
            xs, mz = sem(), [sem() for _ in range(4)]
        offsets = ((0,), (-1, 1), (-2, 2), (-3, 3), (4,))

        def spread(k):
            for offset in offsets[k]:
                at = zat(offset)
                send(ns[k], vz(at, x), vz(at, x), xr)
                send(ns[k], vz(at, x), vz(at, x), xl)

        def z_step(k):
            if k == 0:
                for w in waits:
                    landed(*w)
                if vx:
                    for i in (1, 3, 2):
                        send(xs, vx(z, x), vx(z, x), {"sp_1": xat(i)})
                for i in (1, 2, 4, 3) if direct else (1,):
                    for step in (i, -i) if i < 4 else (i,):
                        send(nz[i - 1], vz(z, x), vz(z, x), {"sp_0": zat(step)})
            else:
                landed(nz[k - 1], vz(z, pl.ds(0, 2)) if k < 4 else vz(z, x))
                if k < 4 and not direct:
                    part = vz(zat(-k), x, 1 if k == 3 else 0)
                    send(nz[k], part, part, zr)
                    part = vz(zat(k), x, 2 if k == 3 else 0)
                    send(nz[k], part, part, zl)
            spread(k)

        def x_step(k):
            if k == 0:
                landed(xs, vx(z, pl.ds(0, 3)))
                send(mz[0], vx(z, whole), vx(z, whole), zr)
                send(mz[0], vx(z, whole), vx(z, whole), zl)
                return
            landed(mz[k - 1], vx(pl.ds(0, 2), whole) if k < 4 else vx(z, whole))
            if k < 4:
                part = vx(zat(-k), lowx if k == 3 else whole)
                send(mz[k], part, part, zr)
                part = vx(zat(k), highx if k == 3 else whole)
                send(mz[k], part, part, zl)

        def f_step(k):
            landed(ns[k], vz(z, pl.ds(0, 2 * len(offsets[k]))))
            for offset in offsets[k]:
                at = zat(offset)
                if 0 <= offset < 4:
                    send(last, vz(at, xat(-1)), vz(at, xat(-1)), xr)
                else:
                    send(last, vz(at, xat(1)), vz(at, xat(1)), xl)

        for k in range(5):
            steps[f"{name}Z{k}"] = functools.partial(z_step, k)
            steps[f"{name}F{k}"] = functools.partial(f_step, k)
            if vx:
                steps[f"{name}X{k}"] = functools.partial(x_step, k)
        steps[f"{name}L"] = lambda: landed(last, vz(pl.ds(0, NZ), x))

    def views(GX, GZ):
        halves = (None, pl.ds(0, 32), pl.ds(32, 32))

        def vz(zi, xi, part=0):
            return GZ.at[zi, xi, halves[part], :] if part else GZ.at[zi, xi]

        return (GX is not None) and (lambda zi, xi: GX.at[zi, xi]), vz

    lanes = (pl.ds(WBX, 256), pl.ds(WBX, 128), pl.ds(WBX + 128, 128))
    plane(
        "L",
        (),
        lambda zi, xi: GB.at[zi, xi, mine, pl.ds(0, WBX)],
        lambda zi, xi, part=0: GB.at[zi, xi, mine, lanes[part]],
    )

    half_z, other_half = pl.ds(0, 4), pl.ds(4, 4)
    ny = sem(), sem()

    def late_part(k, half):
        rows = pl.ds(pl.multiple_of(fat(k) * 16, 16), 16)
        return GB.at[half, :, rows, :]

    def late_y0():
        for n, (a, b) in zip(ny, ((half_z, other_half), (other_half, half_z))):
            send(n, late_part(0, a), late_part(0, a), right, True)
            send(n, late_part(0, b), late_part(0, b), left, True)

    def late_y1():
        landed(ny[0], late_part(0, pl.ds(0, NZ)))
        send(ny[1], late_part(-1, half_z), late_part(-1, half_z), right, True)
        send(ny[1], late_part(1, other_half), late_part(1, other_half), left, True)

    def late_y2():
        landed(ny[1], GB.at[:, :, pl.ds(0, 32), :])

    steps.update(Y0=late_y0, Y1=late_y1, Y2=late_y2)
    plane("1", y1, *views(None, GZ1), direct=True)
    plane("2", y2, *views(GX2, GZ2))
    plane("3", y3, *views(GX3, GZ3))

    ns = sem()

    def start_copies():
        return [copy(ns, SS.at[fat(k)], ST, {"fs": fat(k)}, NSEND + NLONG + i) for i, k in enumerate((1, 2, 3))]

    for made in taken[12:]:
        made.wait()

    @pl.when(f == x)
    def _():
        for i in range(NF):
            SS[i] = jnp.transpose(S0[i]).astype(BF16)
        ST[...] = SS[f]
        for made in start_copies():
            made.start()

    def squares(s):
        w0, w1 = T[0, s].astype(F32), T[1, s].astype(F32)
        square = jnp.sum(w0 * w0 + w1 * w1, axis=1, keepdims=True)
        SC[s] = lax.rsqrt(square * (1.0 / 2048) + EPSILON)

    i0 = lax.broadcasted_iota(jnp.int32, (BLOCK, BLOCK), 0)
    i1 = lax.broadcasted_iota(jnp.int32, (BLOCK, BLOCK), 1)
    causal = i0 >= i1
    tril = jnp.where(causal, 1.0, 0.0).astype(BF16)
    my_room = room[pl.ds(f, 1), :]

    half = NZ // 2

    def each(body):
        for s in range(4):
            body(s, 0)

    def through(slots, *weights):
        count = len(slots) * 256
        at = slice(slots[0], slots[-1] + 1)
        low = jnp.concatenate([w[:half].reshape(1024, w.shape[-1]) for w in weights], axis=1)
        high = jnp.concatenate([w[half:].reshape(1024, w.shape[-1]) for w in weights], axis=1)
        total = dot(T[0, at].reshape(count, 1024), low) + dot(T[1, at].reshape(count, 1024), high)
        total = total * SC[at].reshape(count, 1)
        return [total[256 * i : 256 * i + 256] for i in range(len(slots))]

    def project(slots):
        keys, values, parts, spread = [], [], [], []
        halves = (slice(0, BLOCK), slice(BLOCK, 2 * BLOCK))
        for s, both in zip(slots, through(slots, GZ1)):
            keys.append(my_room * jax.nn.sigmoid(-both[:, :128]))
            values.append(both[:, 128:].astype(BF16))
            K[s], V[s] = keys[-1], values[-1]
        for s, key in zip(slots, keys):
            logs = [p.astype(BF16) for p in three_parts(jnp.log1p(-key))]
            lags = three_parts(SH[s, pl.ds(f, 1), :])
            for rows in halves:
                parts.append(jnp.concatenate([p[rows] for p in logs], axis=0))
                masked = [jnp.broadcast_to(p[:, rows], (BLOCK, BLOCK)) for p in lags]
                masked = [jnp.where(causal, p, 0.0).astype(BF16) for p in masked]
                spread.append(jnp.concatenate(masked, axis=1))
        within = dot(jnp.concatenate([tril] * 3, axis=1), jnp.concatenate(parts, axis=1))
        shifts = dot(jnp.concatenate(spread, axis=0), jnp.ones((3 * BLOCK, BLOCK), BF16))
        ends, faded = [], []
        for i in range(2 * len(slots)):
            block = slice(i * BLOCK, i * BLOCK + BLOCK)
            total = within[:, block] + shifts[block]
            s, rows = slots[i // 2], halves[i % 2]
            C[s, rows, :] = total
            ends.append(total[BLOCK - 1 :])
            faded.append((keys[i // 2][rows] * jnp.exp(ends[-1] - total)).astype(BF16))
        adds = [dot(values[i // 2][halves[i % 2]], k, TN) for i, k in enumerate(faded)]
        for i, s in enumerate(slots):
            A0[s] = adds[2 * i]
            state = jnp.exp(ends[2 * i + 1]) * adds[2 * i] + adds[2 * i + 1]
            SL[s] = pack_state(state, ends[2 * i] + ends[2 * i + 1])

    sx, sz, sb, nb = sem(), sem(), sem(), sem()

    def squares_near():
        landed(near, T.at[other, pl.ds(0, 3)])
        for s in range(3):
            squares(s)

    def project_near():
        landed(nshift, SH.at[pl.ds(0, 3)])
        project((0, 1, 2))

    def project_far():
        landed(far_off, T.at[other, 3])
        squares(3)
        project((3,))
        slot_of = lambda sequence: lax.rem(sequence - f + (NF + 1), NF)
        SR[x] = SL[slot_of(x)]
        for k in (1, 3, 2):
            send(sx, SL.at[slot_of(xat(k))], SR.at[x], {"sp_1": xat(k)})

    def total_x():
        landed(sx, SR.at[pl.ds(0, 3)])
        state, decay = unpack_state(SR[0])
        for i in range(1, NX):
            later, fade = unpack_state(SR[i])
            state, decay = jnp.exp(fade) * state + later, decay + fade
        ZS[...] = pack_state(state, decay)
        for k in (4, 3, 5, 2, 6, 1, 7):
            send(sz, ZS, ZR.at[z], {"sp_0": zat(k)})

    def project_rest(s, rest):
        query = rest[:, :128]
        Q[s] = query * jax.nn.sigmoid(query) * HEAD ** (-0.5)
        gate = rest[:, 128:256]
        G[s] = gate * jax.nn.sigmoid(gate) * hgain[...]
        pool = rest[:, 256:].astype(BF16)
        EXT[s, 128:384, :] = pool
        BS[s] = pool[240:256]

    def rest():
        for slots in ((0, 1), (2, 3)):
            for s, projected in zip(slots, through(slots, GX2, GZ2)):
                project_rest(s, projected)
        send(nb, BS, BR, nxt)

    def inner(s, _):
        for b in range(2):
            rows = slice(b * BLOCK, (b + 1) * BLOCK)
            within = C[s, rows, :]
            centre = within[BLOCK // 2 - 1 : BLOCK // 2]
            query, keys = Q[s, rows, :], K[s, rows, :]
            scores = dot(
                (query * jnp.exp(within - centre)).astype(BF16),
                (keys * jnp.exp(centre - within)).astype(BF16),
                NT,
            )
            scores = jnp.where(causal, scores, 0.0).astype(BF16)
            INS[s, rows, :] = dot(scores, V[s, rows, :])
            QE[s, rows, :] = (query * jnp.exp(within)).astype(BF16)
        return 0

    span = lax.shift_left(jnp.int32(2), c * 2 + f // 2)
    ti = lax.broadcasted_iota(jnp.int32, (256, 384), 0)
    si = lax.broadcasted_iota(jnp.int32, (256, 384), 1) - 128
    band = jnp.where((si <= ti) & (si > ti - span) & (si >= -16), 1.0, 0.0).astype(BF16)
    position = here * 256 + lax.broadcasted_iota(jnp.int32, (256, 128), 0)
    inverse = 1.0 / jnp.minimum(position + 1, span).astype(F32)

    def pool(s, _):
        EXT[s, 0:128, :] = jnp.zeros((128, 128), BF16)

        @pl.when(here > 0)
        def _():
            EXT[s, 112:128, :] = BR[s]

        window = dot(band, EXT[s])
        PO[s] = (window * inverse - EXT[s, 128:384, :].astype(F32)).astype(BF16)
        return 0

    given_pool, given_rec = sem(), sem()

    def give_back(buffer, slot, n, sources):
        for s in sources:
            if s == 1:
                ACT[slot + f] = buffer[1]
            else:
                send(n, buffer.at[s], ACT.at[slot + f], {"fs": fat(s - 1)})

    def pooling():
        landed(nb, BR)
        each(pool)
        give_back(PO, 4, given_pool, (0, 2, 3, 1))

    def pass_z(i, state):
        later, fade = unpack_state(ZR[i])
        return jnp.exp(fade) * state + later

    def from_z():
        landed(sz, ZR.at[pl.ds(0, NZ - 1)])

        @pl.when(f != x)
        def _():
            landed(ns, ST)

        state = lax.fori_loop(0, z, pass_z, ST[...].astype(F32))
        for i in range(NX):
            ES[i] = state.astype(BF16)
            if i < NX - 1:
                later, fade = unpack_state(SR[i])
                state = jnp.exp(fade) * state + later
        ER[x] = ES[x]
        for k in (1, 3, 2):
            send(sb, ES.at[xat(k)], ER.at[x], {"sp_1": xat(k)})

    def finishing():
        landed(sb, ER.at[pl.ds(0, 3)])
        raws, order = {}, (3, 0, 2, 1)
        for s in order:
            entering = ER[fat(s - 1)]
            middle = jnp.exp(C[s, BLOCK - 1 : BLOCK, :]) * entering.astype(F32) + A0[s]
            carried = [dot(QE[s, :BLOCK, :], entering, NT), dot(QE[s, BLOCK:, :], middle.astype(BF16), NT)]
            raws[s] = INS[s] + jnp.concatenate(carried, axis=0)
        for s in order:
            square = jnp.mean(raws[s] * raws[s], axis=1, keepdims=True)
            RO[s] = (raws[s] * lax.rsqrt(square + EPSILON) * G[s]).astype(BF16)
            give_back(RO, 0, given_rec, (s,))

    def out_pool():
        landed(given_pool, ACT.at[pl.ds(4, 3)])
        act = jnp.concatenate([ACT[4 + i] for i in range(4)], axis=1)
        for i in range(4):
            at, cols = slice(2 * i, 2 * i + 2), slice(512 * i, 512 * i + 512)
            PT[:, cols] = dot(act, GB[at].reshape(512, WB), NT)

    steps.update(
        SQ=squares_near,
        PR3=project_near,
        PR1=project_far,
        SUMX=total_x,
        REST=rest,
        INNER=lambda: each(inner),
        POOL=pooling,
        PASSZ=from_z,
        FIN=finishing,
        OUTP=out_pool,
    )
    order = ORDER
    assert sorted(order) == sorted(steps)
    for step in order:
        with jax.named_scope(step):
            steps[step]()

    landed(given_rec, ACT.at[pl.ds(0, 3)])

    act = jnp.concatenate([ACT[i] for i in range(4)], axis=1)
    my_rows = pl.ds(pl.multiple_of(c * 128, 128), 128)
    their_rows = pl.ds(pl.multiple_of(other * 128, 128), 128)
    swap = sem()
    for i in range(4):
        at, cols = slice(2 * i, 2 * i + 2), slice(512 * i, 512 * i + 512)
        weight = [w[at].reshape(512, w.shape[-1]) for w in (GX3, GZ3)]
        total = PT[:, cols] + dot(act, jnp.concatenate(weight, axis=1), NT)
        PS[:, cols] = total.astype(BF16)
        send(swap, PS.at[their_rows, pl.ds(512 * i, 512)], PR.at[:, pl.ds(512 * i, 512)], {"tp": other})
    landed(swap, PR)
    out[...] = (PS[my_rows, :].astype(F32) + PR[...].astype(F32)).astype(BF16)

    for made in sent[-NSEND:] + sent_long[-NLONG:]:
        made.wait_send()

    @pl.when(f == x)
    def _():
        for made in start_copies():
            made.wait_send()


def per_device(
    tokens,
    norm_gain,
    query_weight,
    forget_weight,
    value_weight,
    outgate_weight,
    pool_in_weight,
    forget_room,
    decay_shift,
    head_gain,
    start_state,
    pool_map,
    pool_scale,
    out_rec_weight,
    out_pool_weight,
):
    vmem = lambda *shape: pltpu.VMEM(shape, F32)
    half = lambda *shape: pltpu.VMEM(shape, BF16)
    mixed = pl.pallas_call(
        kernel,
        out_shape=jax.ShapeDtypeStruct((128, 2048), BF16),
        in_specs=[pl.BlockSpec(memory_space=pltpu.HBM)] * 15,
        out_specs=pl.BlockSpec(memory_space=pltpu.VMEM),
        scratch_shapes=[
            half(2, 4, 256, 1024),
            half(NZ, NX, 64, WZ[0]),
            half(NZ, NX, 64, WX[0]),
            half(NZ, NX, 64, WZ[1]),
            half(NZ, NX, 64, WX[1]),
            half(NZ, NX, 64, WZ[2]),
            half(NZ, NX, 64, WB),
            vmem(4, 4, 256),
            half(128, 128),
            vmem(4, 256, 128),
            half(4, 256, 128),
            vmem(4, 256, 128),
            vmem(4, 256, 128),
            vmem(4, 256, 128),
            half(4, 256, 128),
            vmem(4, 256, 128),
            vmem(4, 128, 128),
            half(4, 144, 128),
            half(4, 144, 128),
            half(144, 128),
            half(NZ, 144, 128),
            half(4, 128, 128),
            half(4, 128, 128),
            half(4, 384, 128),
            half(4, 16, 128),
            half(4, 16, 128),
            half(4, 256, 128),
            half(4, 256, 128),
            half(8, 256, 128),
            half(256, 2048),
            half(128, 2048),
            vmem(4, 256, 1),
            half(4, 128, 128),
            vmem(4, 128, 128),
            half(2, 256, 256),
            vmem(256, 2048),
            vmem(16, 128),
            *[half(16, 512)] * 5,
            vmem(1, 512),
            *[half(16, 512)] * 2,
            vmem(4, 128),
            vmem(1, 128),
            half(4, 16, 256),
            half(4, 16, 128),
            half(4, 16, 256),
            half(16, 512),
            pltpu.SemaphoreType.DMA((NSEND + NLONG + 3,)),
            pltpu.SemaphoreType.DMA((NRECV,)),
            pltpu.SemaphoreType.DMA((15,)),
        ],
        compiler_params=pltpu.CompilerParams(
            collective_id=0, has_side_effects=True, vmem_limit_bytes=60 * 1024 * 1024
        ),
    )(
        tokens[0],
        norm_gain.reshape(16, 128),
        query_weight,
        forget_weight,
        value_weight,
        outgate_weight,
        pool_in_weight,
        forget_room.reshape(4, 128),
        decay_shift[0].T,
        head_gain.reshape(1, 128),
        start_state,
        pool_map,
        pool_scale.reshape(1, 512),
        out_rec_weight.T,
        out_pool_weight.T,
    )
    return mixed[None]


def solution(mesh):
    finer = Mesh(
        mesh.devices.reshape(8, 4, mesh.shape["fs"], mesh.shape["tp"]), ("sp_0", "sp_1", "fs", "tp")
    )
    placed = (
        P("fs", SP, "tp"),
        P(),
        P(SP_FS, "tp"),
        P(SP_FS, "tp"),
        P(SP_FS, "tp"),
        P(SP_FS, "tp"),
        P(SP_FS, "tp"),
        P("tp"),
        P("fs", SP, "tp"),
        P(),
        P("fs", "tp", None, None),
        P("tp", None, None),
        P("tp"),
        P("tp", SP_FS),
        P("tp", SP_FS),
    )
    return jax.shard_map(
        per_device, mesh=finer, in_specs=placed, out_specs=P("fs", SP_TP, None), check_vma=False
    )
```

```python
import functools

import jax
import jax.numpy as jnp
from jax import lax
from jax.experimental import pallas as pl
from jax.experimental.pallas import tpu as pltpu
from jax.sharding import Mesh
from jax.sharding import PartitionSpec as P

HEAD = 128
POOL_DIM = 256
BLOCK = 128
SP_FS = ("sp_0", "sp_1", "fs")
SP = ("sp_0", "sp_1")
SP_TP = ("sp_0", "sp_1", "tp")
EPSILON = 1e-06
MESH = pl.DeviceIdType.MESH
ORDER = (
    "LZ0",
    "LZ1",
    "LF0",
    "1Z0",
    "LX0",
    "3Z0",
    "LZ2",
    "LF1",
    "2Z0",
    "1Z1",
    "1Z2",
    "LF2",
    "T1",
    "2X0",
    "1F0",
    "1Z3",
    "1Z4",
    "LX1",
    "1F1",
    "LZ3",
    "2Z1",
    "1F2",
    "2X1",
    "T2",
    "LX2",
    "LZ4",
    "1F3",
    "3X0",
    "1F4",
    "2F0",
    "SQ",
    "2Z2",
    "LF3",
    "2F1",
    "LX3",
    "LF4",
    "3Z1",
    "T3",
    "1L",
    "PR3",
    "PR1",
    "2Z3",
    "2X2",
    "LX4",
    "LL",
    "Y0",
    "2F2",
    "3X1",
    "2Z4",
    "3Z2",
    "2X3",
    "SUMX",
    "2F3",
    "3F0",
    "3F1",
    "2F4",
    "3Z3",
    "Y1",
    "3F2",
    "2L",
    "2X4",
    "REST",
    "3X2",
    "3F3",
    "INNER",
    "PASSZ",
    "3Z4",
    "POOL",
    "3X3",
    "FIN",
    "3F4",
    "Y2",
    "3X4",
    "OUTP",
    "3L",
)
NRECV, NSEND, NLONG = 77, 40, 13
NZ, NX, NF = 8, 4, 4
WX, WZ, WB, WBX = (128, 256), (256, 256, 256), 512, 256
F32, BF16 = jnp.float32, jnp.bfloat16
NT = (((1,), (1,)), ((), ()))
TN = (((0,), (0,)), ((), ()))


def dot(a, b, dims=(((1,), (0,)), ((), ()))):
    return lax.dot_general(a, b, dims, preferred_element_type=F32)


def pack_state(state, decay):
    high, mid, low = three_parts(decay)
    row = lax.broadcasted_iota(jnp.int32, (16, HEAD), 0)
    tail = jnp.where(row == 0, high, jnp.where(row == 1, mid, jnp.where(row == 2, low, 0.0)))
    return jnp.concatenate([state, tail], axis=0).astype(BF16)


def three_parts(value):
    high = value.astype(BF16).astype(F32)
    rest = value - high
    mid = rest.astype(BF16).astype(F32)
    return high, mid, rest - mid


def unpack_state(packed):
    whole = packed.astype(F32)
    decay = jnp.sum(whole[HEAD : HEAD + 16], axis=0, keepdims=True)
    return whole[:HEAD], decay


def kernel(
    h_tok,
    h_gain,
    h_wq,
    h_wf,
    h_wv,
    h_wo,
    h_wp,
    h_room,
    h_shift,
    h_hgain,
    h_start,
    h_pmap,
    h_pscale,
    h_worec,
    h_wopool,
    out,
    T,
    GZ1,
    GX2,
    GZ2,
    GX3,
    GZ3,
    GB,
    SH,
    ST,
    K,
    V,
    Q,
    G,
    C,
    QE,
    INS,
    A0,
    SL,
    SR,
    ZS,
    ZR,
    ES,
    ER,
    EXT,
    BS,
    BR,
    RO,
    PO,
    ACT,
    PS,
    PR,
    SC,
    SS,
    S0,
    PM,
    PT,
    gain,
    wq,
    wf,
    wv,
    wo,
    wp,
    pscale,
    worec,
    wopool,
    room,
    hgain,
    iz1,
    ix2,
    iz2,
    ixz3,
    send_sems,
    recv_sems,
    local_sems,
):
    z, x = lax.axis_index("sp_0"), lax.axis_index("sp_1")
    f, c = lax.axis_index("fs"), lax.axis_index("tp")
    zat = lambda k: lax.rem(z + (k + NZ), NZ)
    xat = lambda k: lax.rem(x + (k + NX), NX)
    fat = lambda k: lax.rem(f + (k + NF), NF)
    other = 1 - c
    here = z * NX + x
    after = lax.rem(here + 1, NZ * NX)
    ahead = lax.rem(here + NZ * NX - 1, NZ * NX)
    nxt = {"sp_0": after // NX, "sp_1": lax.rem(after, NX)}
    prv = {"sp_0": ahead // NX, "sp_1": lax.rem(ahead, NX)}

    arguments = (
        (h_gain, gain),
        (h_wf, wf),
        (h_wv, wv),
        (h_wq, wq),
        (h_wo, wo),
        (h_wp, wp),
        (h_pmap, PM),
        (h_pscale, pscale),
        (h_worec, worec),
        (h_wopool, wopool),
        (h_tok, T.at[c, 1]),
        (h_shift, SH.at[1]),
        (h_start.at[0], S0),
        (h_room, room),
        (h_hgain, hgain),
    )
    taken = [pltpu.make_async_copy(a, b, local_sems.at[i]) for i, (a, b) in enumerate(arguments)]
    for made in taken:
        made.start()

    barrier = pltpu.get_barrier_semaphore()
    met = [{"tp": other}, nxt, prv]
    met += [{"fs": fat(k)} for k in (1, 2, 3)] + [{"sp_1": xat(k)} for k in (1, 2, 3)]
    met += [{"sp_0": zat(k)} for k in range(1, NZ)]
    for who in met:
        pl.semaphore_signal(barrier, inc=1, device_id=who, device_id_type=MESH)

    count = [0]
    sent, sent_long = [], []

    def sem():
        count[0] += 1
        assert count[0] <= NRECV
        return count[0] - 1

    def copy(n, src, dst, who, slot=0):
        return pltpu.make_async_remote_copy(
            src_ref=src,
            dst_ref=dst,
            send_sem=send_sems.at[slot],
            recv_sem=recv_sems.at[n],
            device_id=who,
            device_id_type=MESH,
        )

    def send(n, src, dst, who, long=False):
        made_before, slots, base = (sent_long, NLONG, NSEND) if long else (sent, NSEND, 0)
        if len(made_before) >= slots:
            made_before[-slots].wait_send()
        made = copy(n, src, dst, who, base + len(made_before) % slots)
        made.start()
        made_before.append(made)

    def landed(n, dst):
        copy(n, dst, dst, {"tp": other}).wait_recv()

    rank = here * NF + f
    row = lax.broadcasted_iota(jnp.int32, (16, 128), 0)
    lane = lax.broadcasted_iota(jnp.int32, (16, 128), 1)
    for made in taken[:3]:
        made.wait()
    gains = jnp.broadcast_to(gain[pl.ds(rank // 8, 1), :], (16, 128))
    gains = jnp.where(lane == lax.rem(rank, 8) * 16 + row, gains, 0.0)
    gains = jnp.sum(gains, axis=1, keepdims=True)
    mine = pl.ds(pl.multiple_of(f * 16, 16), 16)

    def stage(buffer, place, weights):
        for i in range(NF):
            chunk = [w[:, 128 * i : 128 * i + 128] for w in weights]
            buffer[i] = jnp.concatenate(chunk, axis=1)
        place[z, x, mine, :] = buffer[f]

    def scaled(w):
        return (w[...].astype(F32) * gains).astype(BF16)

    stage(iz1, GZ1, (scaled(wf), scaled(wv)))
    pl.semaphore_wait(barrier, len(met))

    def over_y(pairs):
        ns = [sem() for _ in pairs]
        for k in (1, 3, 2):
            to = fat(k)
            for n, (buffer, own) in zip(ns, pairs):
                send(n, own.at[to], buffer.at[z, x, mine, :], {"fs": to})
        return [(n, buffer.at[z, x, pl.ds(0, 48), :]) for n, (buffer, _) in zip(ns, pairs)]

    def over_out():
        ns = sem(), sem()
        for k in (1, 3, 2):
            to = {"fs": fat(k)}
            send(ns[0], ixz3.at[:, pl.ds(0, 256)], GX3.at[z, x, mine, :], to)
            send(ns[1], ixz3.at[:, pl.ds(256, 256)], GZ3.at[z, x, mine, :], to)
        return [(n, b.at[z, x, pl.ds(0, 48), :]) for n, b in zip(ns, (GX3, GZ3))]

    y1 = over_y(((GZ1, iz1),))
    for made in taken[3:12]:
        made.wait()
    folded = [dot(wp[:, 256 * i : 256 * i + 256], PM[i]) for i in range(2)]
    folded = (jnp.concatenate(folded, axis=1) * gains * pscale[...]).astype(BF16)
    turned = jnp.concatenate([worec[...], wopool[...]], axis=1)
    stage(ix2, GX2, (scaled(wq),))
    stage(iz2, GZ2, (scaled(wo), folded))
    ixz3[...] = turned[:, :512]
    GX3[z, x, mine, :] = turned[:, :256]
    GZ3[z, x, mine, :] = turned[:, 256:512]
    GB[z, x, mine, :] = turned[:, 512:]
    y2 = over_y(((GX2, ix2), (GZ2, iz2)))
    y3 = over_out()
    nshift = sem()
    for k in (1, 3, 2):
        send(nshift, SH.at[1], SH.at[(5 - k) % 4], {"fs": fat(k)})

    first, second = pl.ds(0, 128), pl.ds(128, 128)
    right, left = {"fs": fat(1)}, {"fs": fat(3)}
    nt = [sem() for _ in range(3)]
    near, far_off = sem(), sem()

    def relay(n, seq, rows):
        send(n, T.at[c, seq, rows, :], T.at[c, seq, rows, :], {"tp": other}, True)

    for i, (a, b) in enumerate(((first, second), (second, first))):
        send(nt[i], T.at[c, 1, a, :], T.at[c, 0, a, :], right, True)
        send(nt[i], T.at[c, 1, b, :], T.at[c, 2, b, :], left, True)
    send(near, T.at[c, 1], T.at[c, 1], {"tp": other}, True)

    def tokens_1():
        landed(nt[0], T.at[c, 0])
        send(nt[2], T.at[c, 0, first, :], T.at[c, 3, first, :], right, True)
        send(nt[2], T.at[c, 2, second, :], T.at[c, 3, second, :], left, True)
        relay(near, 0, first)
        relay(near, 2, second)

    def tokens_2():
        landed(nt[1], T.at[c, 0])
        relay(near, 0, second)
        relay(near, 2, first)

    def tokens_3():
        landed(nt[2], T.at[c, 3])
        relay(far_off, 3, first)
        relay(far_off, 3, second)

    steps = {"T1": tokens_1, "T2": tokens_2, "T3": tokens_3}

    def plane(name, waits, vx, vz, direct=False):
        zr, zl = {"sp_0": zat(1)}, {"sp_0": zat(-1)}
        xr, xl = {"sp_1": xat(1)}, {"sp_1": xat(-1)}
        whole, lowx, highx = pl.ds(0, 4), pl.ds(0, 2), pl.ds(2, 2)
        nz, ns, last = [sem() for _ in range(4)], [sem() for _ in range(5)], sem()
        if vx:
            xs, mz = sem(), [sem() for _ in range(4)]
        offsets = ((0,), (-1, 1), (-2, 2), (-3, 3), (4,))

        def spread(k):
            for offset in offsets[k]:
                at = zat(offset)
                send(ns[k], vz(at, x), vz(at, x), xr)
                send(ns[k], vz(at, x), vz(at, x), xl)

        def z_step(k):
            if k == 0:
                for w in waits:
                    landed(*w)
                if vx:
                    for i in (1, 3, 2):
                        send(xs, vx(z, x), vx(z, x), {"sp_1": xat(i)})
                for i in (1, 2, 4, 3) if direct else (1,):
                    for step in (i, -i) if i < 4 else (i,):
                        send(nz[i - 1], vz(z, x), vz(z, x), {"sp_0": zat(step)})
            else:
                landed(nz[k - 1], vz(z, pl.ds(0, 2)) if k < 4 else vz(z, x))
                if k < 4 and not direct:
                    part = vz(zat(-k), x, 1 if k == 3 else 0)
                    send(nz[k], part, part, zr)
                    part = vz(zat(k), x, 2 if k == 3 else 0)
                    send(nz[k], part, part, zl)
            spread(k)

        def x_step(k):
            if k == 0:
                landed(xs, vx(z, pl.ds(0, 3)))
                send(mz[0], vx(z, whole), vx(z, whole), zr)
                send(mz[0], vx(z, whole), vx(z, whole), zl)
                return
            landed(mz[k - 1], vx(pl.ds(0, 2), whole) if k < 4 else vx(z, whole))
            if k < 4:
                part = vx(zat(-k), lowx if k == 3 else whole)
                send(mz[k], part, part, zr)
                part = vx(zat(k), highx if k == 3 else whole)
                send(mz[k], part, part, zl)

        def f_step(k):
            landed(ns[k], vz(z, pl.ds(0, 2 * len(offsets[k]))))
            for offset in offsets[k]:
                at = zat(offset)
                if 0 <= offset < 4:
                    send(last, vz(at, xat(-1)), vz(at, xat(-1)), xr)
                else:
                    send(last, vz(at, xat(1)), vz(at, xat(1)), xl)

        for k in range(5):
            steps[f"{name}Z{k}"] = functools.partial(z_step, k)
            steps[f"{name}F{k}"] = functools.partial(f_step, k)
            if vx:
                steps[f"{name}X{k}"] = functools.partial(x_step, k)
        steps[f"{name}L"] = lambda: landed(last, vz(pl.ds(0, NZ), x))

    def views(GX, GZ):
        halves = (None, pl.ds(0, 32), pl.ds(32, 32))

        def vz(zi, xi, part=0):
            return GZ.at[zi, xi, halves[part], :] if part else GZ.at[zi, xi]

        return (GX is not None) and (lambda zi, xi: GX.at[zi, xi]), vz

    lanes = (pl.ds(WBX, 256), pl.ds(WBX, 128), pl.ds(WBX + 128, 128))
    plane(
        "L",
        (),
        lambda zi, xi: GB.at[zi, xi, mine, pl.ds(0, WBX)],
        lambda zi, xi, part=0: GB.at[zi, xi, mine, lanes[part]],
    )

    half_z, other_half = pl.ds(0, 4), pl.ds(4, 4)
    ny = sem(), sem()

    def late_part(k, half):
        rows = pl.ds(pl.multiple_of(fat(k) * 16, 16), 16)
        return GB.at[half, :, rows, :]

    def late_y0():
        for n, (a, b) in zip(ny, ((half_z, other_half), (other_half, half_z))):
            send(n, late_part(0, a), late_part(0, a), right, True)
            send(n, late_part(0, b), late_part(0, b), left, True)

    def late_y1():
        landed(ny[0], late_part(0, pl.ds(0, NZ)))
        send(ny[1], late_part(-1, half_z), late_part(-1, half_z), right, True)
        send(ny[1], late_part(1, other_half), late_part(1, other_half), left, True)

    def late_y2():
        landed(ny[1], GB.at[:, :, pl.ds(0, 32), :])

    steps.update(Y0=late_y0, Y1=late_y1, Y2=late_y2)
    plane("1", y1, *views(None, GZ1), direct=True)
    plane("2", y2, *views(GX2, GZ2))
    plane("3", y3, *views(GX3, GZ3))

    ns = sem()

    def start_copies():
        return [copy(ns, SS.at[fat(k)], ST, {"fs": fat(k)}, NSEND + NLONG + i) for i, k in enumerate((1, 2, 3))]

    for made in taken[12:]:
        made.wait()

    @pl.when(f == x)
    def _():
        for i in range(NF):
            SS[i] = jnp.transpose(S0[i]).astype(BF16)
        ST[...] = SS[f]
        for made in start_copies():
            made.start()

    def squares(s):
        w0, w1 = T[0, s].astype(F32), T[1, s].astype(F32)
        square = jnp.sum(w0 * w0 + w1 * w1, axis=1, keepdims=True)
        SC[s] = lax.rsqrt(square * (1.0 / 2048) + EPSILON)

    i0 = lax.broadcasted_iota(jnp.int32, (BLOCK, BLOCK), 0)
    i1 = lax.broadcasted_iota(jnp.int32, (BLOCK, BLOCK), 1)
    causal = i0 >= i1
    tril = jnp.where(causal, 1.0, 0.0).astype(BF16)
    my_room = room[pl.ds(f, 1), :]

    half = NZ // 2

    def each(body):
        for s in range(4):
            body(s, 0)

    def through(slots, *weights):
        count = len(slots) * 256
        at = slice(slots[0], slots[-1] + 1)
        low = jnp.concatenate([w[:half].reshape(1024, w.shape[-1]) for w in weights], axis=1)
        high = jnp.concatenate([w[half:].reshape(1024, w.shape[-1]) for w in weights], axis=1)
        total = dot(T[0, at].reshape(count, 1024), low) + dot(T[1, at].reshape(count, 1024), high)
        total = total * SC[at].reshape(count, 1)
        return [total[256 * i : 256 * i + 256] for i in range(len(slots))]

    def project(slots):
        keys, values, parts, spread = [], [], [], []
        halves = (slice(0, BLOCK), slice(BLOCK, 2 * BLOCK))
        for s, both in zip(slots, through(slots, GZ1)):
            keys.append(my_room * jax.nn.sigmoid(-both[:, :128]))
            values.append(both[:, 128:].astype(BF16))
            K[s], V[s] = keys[-1], values[-1]
        for s, key in zip(slots, keys):
            logs = [p.astype(BF16) for p in three_parts(jnp.log1p(-key))]
            lags = three_parts(SH[s, pl.ds(f, 1), :])
            for rows in halves:
                parts.append(jnp.concatenate([p[rows] for p in logs], axis=0))
                masked = [jnp.broadcast_to(p[:, rows], (BLOCK, BLOCK)) for p in lags]
                masked = [jnp.where(causal, p, 0.0).astype(BF16) for p in masked]
                spread.append(jnp.concatenate(masked, axis=1))
        within = dot(jnp.concatenate([tril] * 3, axis=1), jnp.concatenate(parts, axis=1))
        shifts = dot(jnp.concatenate(spread, axis=0), jnp.ones((3 * BLOCK, BLOCK), BF16))
        ends, faded = [], []
        for i in range(2 * len(slots)):
            block = slice(i * BLOCK, i * BLOCK + BLOCK)
            total = within[:, block] + shifts[block]
            s, rows = slots[i // 2], halves[i % 2]
            C[s, rows, :] = total
            ends.append(total[BLOCK - 1 :])
            faded.append((keys[i // 2][rows] * jnp.exp(ends[-1] - total)).astype(BF16))
        adds = [dot(values[i // 2][halves[i % 2]], k, TN) for i, k in enumerate(faded)]
        for i, s in enumerate(slots):
            A0[s] = adds[2 * i]
            state = jnp.exp(ends[2 * i + 1]) * adds[2 * i] + adds[2 * i + 1]
            SL[s] = pack_state(state, ends[2 * i] + ends[2 * i + 1])

    sx, sz, sb, nb = sem(), sem(), sem(), sem()

    def squares_near():
        landed(near, T.at[other, pl.ds(0, 3)])
        for s in range(3):
            squares(s)

    def project_near():
        landed(nshift, SH.at[pl.ds(0, 3)])
        project((0, 1, 2))

    def project_far():
        landed(far_off, T.at[other, 3])
        squares(3)
        project((3,))
        slot_of = lambda sequence: lax.rem(sequence - f + (NF + 1), NF)
        SR[x] = SL[slot_of(x)]
        for k in (1, 3, 2):
            send(sx, SL.at[slot_of(xat(k))], SR.at[x], {"sp_1": xat(k)})

    def total_x():
        landed(sx, SR.at[pl.ds(0, 3)])
        state, decay = unpack_state(SR[0])
        for i in range(1, NX):
            later, fade = unpack_state(SR[i])
            state, decay = jnp.exp(fade) * state + later, decay + fade
        ZS[...] = pack_state(state, decay)
        for k in (4, 3, 5, 2, 6, 1, 7):
            send(sz, ZS, ZR.at[z], {"sp_0": zat(k)})

    def project_rest(s, rest):
        query = rest[:, :128]
        Q[s] = query * jax.nn.sigmoid(query) * HEAD ** (-0.5)
        gate = rest[:, 128:256]
        G[s] = gate * jax.nn.sigmoid(gate) * hgain[...]
        pool = rest[:, 256:].astype(BF16)
        EXT[s, 128:384, :] = pool
        BS[s] = pool[240:256]

    def rest():
        for slots in ((0, 1), (2, 3)):
            for s, projected in zip(slots, through(slots, GX2, GZ2)):
                project_rest(s, projected)
        send(nb, BS, BR, nxt)

    def inner(s, _):
        for b in range(2):
            rows = slice(b * BLOCK, (b + 1) * BLOCK)
            within = C[s, rows, :]
            centre = within[BLOCK // 2 - 1 : BLOCK // 2]
            query, keys = Q[s, rows, :], K[s, rows, :]
            scores = dot(
                (query * jnp.exp(within - centre)).astype(BF16),
                (keys * jnp.exp(centre - within)).astype(BF16),
                NT,
            )
            scores = jnp.where(causal, scores, 0.0).astype(BF16)
            INS[s, rows, :] = dot(scores, V[s, rows, :])
            QE[s, rows, :] = (query * jnp.exp(within)).astype(BF16)
        return 0

    span = lax.shift_left(jnp.int32(2), c * 2 + f // 2)
    ti = lax.broadcasted_iota(jnp.int32, (256, 384), 0)
    si = lax.broadcasted_iota(jnp.int32, (256, 384), 1) - 128
    band = jnp.where((si <= ti) & (si > ti - span) & (si >= -16), 1.0, 0.0).astype(BF16)
    position = here * 256 + lax.broadcasted_iota(jnp.int32, (256, 128), 0)
    inverse = 1.0 / jnp.minimum(position + 1, span).astype(F32)

    def pool(s, _):
        EXT[s, 0:128, :] = jnp.zeros((128, 128), BF16)

        @pl.when(here > 0)
        def _():
            EXT[s, 112:128, :] = BR[s]

        window = dot(band, EXT[s])
        PO[s] = (window * inverse - EXT[s, 128:384, :].astype(F32)).astype(BF16)
        return 0

    given_pool, given_rec = sem(), sem()

    def give_back(buffer, slot, n, sources):
        for s in sources:
            if s == 1:
                ACT[slot + f] = buffer[1]
            else:
                send(n, buffer.at[s], ACT.at[slot + f], {"fs": fat(s - 1)})

    def pooling():
        landed(nb, BR)
        each(pool)
        give_back(PO, 4, given_pool, (0, 2, 3, 1))

    def pass_z(i, state):
        later, fade = unpack_state(ZR[i])
        return jnp.exp(fade) * state + later

    def from_z():
        landed(sz, ZR.at[pl.ds(0, NZ - 1)])

        @pl.when(f != x)
        def _():
            landed(ns, ST)

        state = lax.fori_loop(0, z, pass_z, ST[...].astype(F32))
        for i in range(NX):
            ES[i] = state.astype(BF16)
            if i < NX - 1:
                later, fade = unpack_state(SR[i])
                state = jnp.exp(fade) * state + later
        ER[x] = ES[x]
        for k in (1, 3, 2):
            send(sb, ES.at[xat(k)], ER.at[x], {"sp_1": xat(k)})

    def finishing():
        landed(sb, ER.at[pl.ds(0, 3)])
        raws, order = {}, (3, 0, 2, 1)
        for s in order:
            entering = ER[fat(s - 1)]
            middle = jnp.exp(C[s, BLOCK - 1 : BLOCK, :]) * entering.astype(F32) + A0[s]
            carried = [dot(QE[s, :BLOCK, :], entering, NT), dot(QE[s, BLOCK:, :], middle.astype(BF16), NT)]
            raws[s] = INS[s] + jnp.concatenate(carried, axis=0)
        for s in order:
            square = jnp.mean(raws[s] * raws[s], axis=1, keepdims=True)
            RO[s] = (raws[s] * lax.rsqrt(square + EPSILON) * G[s]).astype(BF16)
            give_back(RO, 0, given_rec, (s,))

    def out_pool():
        landed(given_pool, ACT.at[pl.ds(4, 3)])
        act = jnp.concatenate([ACT[4 + i] for i in range(4)], axis=1)
        for i in range(4):
            at, cols = slice(2 * i, 2 * i + 2), slice(512 * i, 512 * i + 512)
            PT[:, cols] = dot(act, GB[at].reshape(512, WB), NT)

    steps.update(
        SQ=squares_near,
        PR3=project_near,
        PR1=project_far,
        SUMX=total_x,
        REST=rest,
        INNER=lambda: each(inner),
        POOL=pooling,
        PASSZ=from_z,
        FIN=finishing,
        OUTP=out_pool,
    )
    order = ORDER
    assert sorted(order) == sorted(steps)
    for step in order:
        with jax.named_scope(step):
            steps[step]()

    landed(given_rec, ACT.at[pl.ds(0, 3)])

    act = jnp.concatenate([ACT[i] for i in range(4)], axis=1)
    my_rows = pl.ds(pl.multiple_of(c * 128, 128), 128)
    their_rows = pl.ds(pl.multiple_of(other * 128, 128), 128)
    swap = sem()
    for i in range(4):
        at, cols = slice(2 * i, 2 * i + 2), slice(512 * i, 512 * i + 512)
        weight = [w[at].reshape(512, w.shape[-1]) for w in (GX3, GZ3)]
        total = PT[:, cols] + dot(act, jnp.concatenate(weight, axis=1), NT)
        PS[:, cols] = total.astype(BF16)
        send(swap, PS.at[their_rows, pl.ds(512 * i, 512)], PR.at[:, pl.ds(512 * i, 512)], {"tp": other})
    landed(swap, PR)
    out[...] = (PS[my_rows, :].astype(F32) + PR[...].astype(F32)).astype(BF16)

    for made in sent[-NSEND:] + sent_long[-NLONG:]:
        made.wait_send()

    @pl.when(f == x)
    def _():
        for made in start_copies():
            made.wait_send()


def per_device(
    tokens,
    norm_gain,
    query_weight,
    forget_weight,
    value_weight,
    outgate_weight,
    pool_in_weight,
    forget_room,
    decay_shift,
    head_gain,
    start_state,
    pool_map,
    pool_scale,
    out_rec_weight,
    out_pool_weight,
):
    vmem = lambda *shape: pltpu.VMEM(shape, F32)
    half = lambda *shape: pltpu.VMEM(shape, BF16)
    mixed = pl.pallas_call(
        kernel,
        out_shape=jax.ShapeDtypeStruct((128, 2048), BF16),
        in_specs=[pl.BlockSpec(memory_space=pltpu.HBM)] * 15,
        out_specs=pl.BlockSpec(memory_space=pltpu.VMEM),
        scratch_shapes=[
            half(2, 4, 256, 1024),
            half(NZ, NX, 64, WZ[0]),
            half(NZ, NX, 64, WX[0]),
            half(NZ, NX, 64, WZ[1]),
            half(NZ, NX, 64, WX[1]),
            half(NZ, NX, 64, WZ[2]),
            half(NZ, NX, 64, WB),
            vmem(4, 4, 256),
            half(128, 128),
            vmem(4, 256, 128),
            half(4, 256, 128),
            vmem(4, 256, 128),
            vmem(4, 256, 128),
            vmem(4, 256, 128),
            half(4, 256, 128),
            vmem(4, 256, 128),
            vmem(4, 128, 128),
            half(4, 144, 128),
            half(4, 144, 128),
            half(144, 128),
            half(NZ, 144, 128),
            half(4, 128, 128),
            half(4, 128, 128),
            half(4, 384, 128),
            half(4, 16, 128),
            half(4, 16, 128),
            half(4, 256, 128),
            half(4, 256, 128),
            half(8, 256, 128),
            half(256, 2048),
            half(128, 2048),
            vmem(4, 256, 1),
            half(4, 128, 128),
            vmem(4, 128, 128),
            half(2, 256, 256),
            vmem(256, 2048),
            vmem(16, 128),
            *[half(16, 512)] * 5,
            vmem(1, 512),
            *[half(16, 512)] * 2,
            vmem(4, 128),
            vmem(1, 128),
            half(4, 16, 256),
            half(4, 16, 128),
            half(4, 16, 256),
            half(16, 512),
            pltpu.SemaphoreType.DMA((NSEND + NLONG + 3,)),
            pltpu.SemaphoreType.DMA((NRECV,)),
            pltpu.SemaphoreType.DMA((15,)),
        ],
        compiler_params=pltpu.CompilerParams(
            collective_id=0, has_side_effects=True, vmem_limit_bytes=48 * 1024 * 1024
        ),
    )(
        *[pltpu.with_memory_space_constraint(a, pltpu.HBM) for a in (
        tokens[0],
        norm_gain.reshape(16, 128),
        query_weight,
        forget_weight,
        value_weight,
        outgate_weight,
        pool_in_weight,
        forget_room.reshape(4, 128),
        decay_shift[0].T,
        head_gain.reshape(1, 128),
        start_state,
        pool_map,
        pool_scale.reshape(1, 512),
        out_rec_weight.T,
        out_pool_weight.T,
    )]
    )
    return mixed[None]


def solution(mesh):
    finer = Mesh(
        mesh.devices.reshape(8, 4, mesh.shape["fs"], mesh.shape["tp"]), ("sp_0", "sp_1", "fs", "tp")
    )
    placed = (
        P("fs", SP, "tp"),
        P(),
        P(SP_FS, "tp"),
        P(SP_FS, "tp"),
        P(SP_FS, "tp"),
        P(SP_FS, "tp"),
        P(SP_FS, "tp"),
        P("tp"),
        P("fs", SP, "tp"),
        P(),
        P("fs", "tp", None, None),
        P("tp", None, None),
        P("tp"),
        P("tp", SP_FS),
        P("tp", SP_FS),
    )
    return jax.shard_map(
        per_device, mesh=finer, in_specs=placed, out_specs=P("fs", SP_TP, None), check_vma=False
    )
```

```python
import functools

import jax
import jax.numpy as jnp
from jax import lax
from jax.experimental import pallas as pl
from jax.experimental.pallas import tpu as pltpu
from jax.sharding import Mesh
from jax.sharding import PartitionSpec as P

HEAD = 128
POOL_DIM = 256
BLOCK = 128
SP_FS = ("sp_0", "sp_1", "fs")
SP = ("sp_0", "sp_1")
SP_TP = ("sp_0", "sp_1", "tp")
EPSILON = 1e-06
MESH = pl.DeviceIdType.MESH
ORDER = (
    "LZ0",
    "LZ1",
    "LF0",
    "1Z0",
    "LX0",
    "3Z0",
    "LZ2",
    "LF1",
    "2Z0",
    "1Z1",
    "1Z2",
    "LF2",
    "T1",
    "2X0",
    "1F0",
    "1Z3",
    "1Z4",
    "LX1",
    "1F1",
    "LZ3",
    "2Z1",
    "1F2",
    "2X1",
    "T2",
    "LX2",
    "LZ4",
    "1F3",
    "3X0",
    "1F4",
    "2F0",
    "SQ",
    "2Z2",
    "LF3",
    "2F1",
    "LX3",
    "LF4",
    "3Z1",
    "T3",
    "1L",
    "PR3",
    "PR1",
    "2Z3",
    "2X2",
    "LX4",
    "LL",
    "Y0",
    "2F2",
    "3X1",
    "2Z4",
    "3Z2",
    "2X3",
    "SUMX",
    "2F3",
    "3F0",
    "3F1",
    "2F4",
    "3Z3",
    "Y1",
    "3F2",
    "2L",
    "2X4",
    "REST",
    "3X2",
    "3F3",
    "PASSZ",
    "INNER",
    "3Z4",
    "POOL",
    "3X3",
    "FIN",
    "3F4",
    "Y2",
    "3X4",
    "OUTP",
    "3L",
)
NRECV, NSEND, NLONG = 77, 40, 13
NZ, NX, NF = 8, 4, 4
WX, WZ, WB, WBX = (128, 256), (256, 256, 256), 512, 256
F32, BF16 = jnp.float32, jnp.bfloat16
NT = (((1,), (1,)), ((), ()))
TN = (((0,), (0,)), ((), ()))


def dot(a, b, dims=(((1,), (0,)), ((), ()))):
    return lax.dot_general(a, b, dims, preferred_element_type=F32)


def pack_state(state, decay):
    high, mid, low = three_parts(decay)
    row = lax.broadcasted_iota(jnp.int32, (16, HEAD), 0)
    tail = jnp.where(row == 0, high, jnp.where(row == 1, mid, jnp.where(row == 2, low, 0.0)))
    return jnp.concatenate([state, tail], axis=0).astype(BF16)


def three_parts(value):
    high = value.astype(BF16).astype(F32)
    rest = value - high
    mid = rest.astype(BF16).astype(F32)
    return high, mid, rest - mid


def unpack_state(packed):
    whole = packed.astype(F32)
    decay = jnp.sum(whole[HEAD : HEAD + 16], axis=0, keepdims=True)
    return whole[:HEAD], decay


def kernel(
    h_tok,
    h_gain,
    h_wq,
    h_wf,
    h_wv,
    h_wo,
    h_wp,
    h_room,
    h_shift,
    h_hgain,
    h_start,
    h_pmap,
    h_pscale,
    h_worec,
    h_wopool,
    out,
    T,
    GZ1,
    GX2,
    GZ2,
    GX3,
    GZ3,
    GB,
    SH,
    ST,
    K,
    V,
    Q,
    G,
    C,
    QE,
    INS,
    A0,
    SL,
    SR,
    ZS,
    ZR,
    ES,
    ER,
    EXT,
    BS,
    BR,
    RO,
    PO,
    ACT,
    PS,
    PR,
    SC,
    SS,
    S0,
    PM,
    PT,
    gain,
    wq,
    wf,
    wv,
    wo,
    wp,
    pscale,
    worec,
    wopool,
    room,
    hgain,
    iz1,
    ix2,
    iz2,
    ixz3,
    send_sems,
    recv_sems,
    local_sems,
):
    z, x = lax.axis_index("sp_0"), lax.axis_index("sp_1")
    f, c = lax.axis_index("fs"), lax.axis_index("tp")
    zat = lambda k: lax.rem(z + (k + NZ), NZ)
    xat = lambda k: lax.rem(x + (k + NX), NX)
    fat = lambda k: lax.rem(f + (k + NF), NF)
    other = 1 - c
    here = z * NX + x
    after = lax.rem(here + 1, NZ * NX)
    ahead = lax.rem(here + NZ * NX - 1, NZ * NX)
    nxt = {"sp_0": after // NX, "sp_1": lax.rem(after, NX)}
    prv = {"sp_0": ahead // NX, "sp_1": lax.rem(ahead, NX)}

    arguments = (
        (h_gain, gain),
        (h_wf, wf),
        (h_wv, wv),
        (h_wq, wq),
        (h_wo, wo),
        (h_wp, wp),
        (h_pmap, PM),
        (h_pscale, pscale),
        (h_worec, worec),
        (h_wopool, wopool),
        (h_tok, T.at[c, 1]),
        (h_shift, SH.at[1]),
        (h_start.at[0], S0),
        (h_room, room),
        (h_hgain, hgain),
    )
    taken = [pltpu.make_async_copy(a, b, local_sems.at[i]) for i, (a, b) in enumerate(arguments)]
    for made in taken:
        made.start()

    barrier = pltpu.get_barrier_semaphore()
    met = [{"tp": other}, nxt, prv]
    met += [{"fs": fat(k)} for k in (1, 2, 3)] + [{"sp_1": xat(k)} for k in (1, 2, 3)]
    met += [{"sp_0": zat(k)} for k in range(1, NZ)]
    for who in met:
        pl.semaphore_signal(barrier, inc=1, device_id=who, device_id_type=MESH)

    count = [0]
    sent, sent_long = [], []

    def sem():
        count[0] += 1
        assert count[0] <= NRECV
        return count[0] - 1

    def copy(n, src, dst, who, slot=0):
        return pltpu.make_async_remote_copy(
            src_ref=src,
            dst_ref=dst,
            send_sem=send_sems.at[slot],
            recv_sem=recv_sems.at[n],
            device_id=who,
            device_id_type=MESH,
        )

    waited = set()

    def finish_send(made):
        if id(made) not in waited:
            waited.add(id(made))
            made.wait_send()

    def send(n, src, dst, who, long=False):
        made_before, slots, base = (sent_long, NLONG, NSEND) if long else (sent, NSEND, 0)
        if len(made_before) >= slots:
            finish_send(made_before[-slots])
        made = copy(n, src, dst, who, base + len(made_before) % slots)
        made.start()
        made_before.append(made)

    def landed(n, dst):
        copy(n, dst, dst, {"tp": other}).wait_recv()

    rank = here * NF + f
    row = lax.broadcasted_iota(jnp.int32, (16, 128), 0)
    lane = lax.broadcasted_iota(jnp.int32, (16, 128), 1)
    for made in taken[:3]:
        made.wait()
    gains = jnp.broadcast_to(gain[pl.ds(rank // 8, 1), :], (16, 128))
    gains = jnp.where(lane == lax.rem(rank, 8) * 16 + row, gains, 0.0)
    gains = jnp.sum(gains, axis=1, keepdims=True)
    mine = pl.ds(pl.multiple_of(f * 16, 16), 16)

    def stage(buffer, place, weights):
        for i in range(NF):
            chunk = [w[:, 128 * i : 128 * i + 128] for w in weights]
            buffer[i] = jnp.concatenate(chunk, axis=1)
        place[z, x, mine, :] = buffer[f]

    def scaled(w):
        return (w[...].astype(F32) * gains).astype(BF16)

    stage(iz1, GZ1, (scaled(wf), scaled(wv)))
    pl.semaphore_wait(barrier, len(met))

    def over_y(pairs):
        ns = [sem() for _ in pairs]
        for k in (1, 3, 2):
            to = fat(k)
            for n, (buffer, own) in zip(ns, pairs):
                send(n, own.at[to], buffer.at[z, x, mine, :], {"fs": to})
        return [(n, buffer.at[z, x, pl.ds(0, 48), :]) for n, (buffer, _) in zip(ns, pairs)]

    def over_out():
        ns = sem(), sem()
        for k in (1, 3, 2):
            to = {"fs": fat(k)}
            send(ns[0], ixz3.at[:, pl.ds(0, 256)], GX3.at[z, x, mine, :], to)
            send(ns[1], ixz3.at[:, pl.ds(256, 256)], GZ3.at[z, x, mine, :], to)
        return [(n, b.at[z, x, pl.ds(0, 48), :]) for n, b in zip(ns, (GX3, GZ3))]

    y1 = over_y(((GZ1, iz1),))
    for made in taken[3:12]:
        made.wait()
    folded = [dot(wp[:, 256 * i : 256 * i + 256], PM[i]) for i in range(2)]
    folded = (jnp.concatenate(folded, axis=1) * gains * pscale[...]).astype(BF16)
    turned = jnp.concatenate([worec[...], wopool[...]], axis=1)
    stage(ix2, GX2, (scaled(wq),))
    stage(iz2, GZ2, (scaled(wo), folded))
    ixz3[...] = turned[:, :512]
    GX3[z, x, mine, :] = turned[:, :256]
    GZ3[z, x, mine, :] = turned[:, 256:512]
    GB[z, x, mine, :] = turned[:, 512:]
    y2 = over_y(((GX2, ix2), (GZ2, iz2)))
    y3 = over_out()
    nshift = sem()
    for k in (1, 3, 2):
        send(nshift, SH.at[1], SH.at[(5 - k) % 4], {"fs": fat(k)})

    first, second = pl.ds(0, 128), pl.ds(128, 128)
    right, left = {"fs": fat(1)}, {"fs": fat(3)}
    nt = [sem() for _ in range(3)]
    near, far_off = sem(), sem()

    def relay(n, seq, rows):
        send(n, T.at[c, seq, rows, :], T.at[c, seq, rows, :], {"tp": other}, True)

    for i, (a, b) in enumerate(((first, second), (second, first))):
        send(nt[i], T.at[c, 1, a, :], T.at[c, 0, a, :], right, True)
        send(nt[i], T.at[c, 1, b, :], T.at[c, 2, b, :], left, True)
    send(near, T.at[c, 1], T.at[c, 1], {"tp": other}, True)

    def tokens_1():
        landed(nt[0], T.at[c, 0])
        send(nt[2], T.at[c, 0, first, :], T.at[c, 3, first, :], right, True)
        send(nt[2], T.at[c, 2, second, :], T.at[c, 3, second, :], left, True)
        relay(near, 0, first)
        relay(near, 2, second)

    def tokens_2():
        landed(nt[1], T.at[c, 0])
        relay(near, 0, second)
        relay(near, 2, first)

    def tokens_3():
        landed(nt[2], T.at[c, 3])
        relay(far_off, 3, first)
        relay(far_off, 3, second)

    steps = {"T1": tokens_1, "T2": tokens_2, "T3": tokens_3}

    def plane(name, waits, vx, vz, direct=False):
        zr, zl = {"sp_0": zat(1)}, {"sp_0": zat(-1)}
        xr, xl = {"sp_1": xat(1)}, {"sp_1": xat(-1)}
        whole, lowx, highx = pl.ds(0, 4), pl.ds(0, 2), pl.ds(2, 2)
        nz, ns, last = [sem() for _ in range(4)], [sem() for _ in range(5)], sem()
        if vx:
            xs, mz = sem(), [sem() for _ in range(4)]
        offsets = ((0,), (-1, 1), (-2, 2), (-3, 3), (4,))

        def spread(k):
            for offset in offsets[k]:
                at = zat(offset)
                send(ns[k], vz(at, x), vz(at, x), xr)
                send(ns[k], vz(at, x), vz(at, x), xl)

        def z_step(k):
            if k == 0:
                for w in waits:
                    landed(*w)
                if vx:
                    for i in (1, 3, 2):
                        send(xs, vx(z, x), vx(z, x), {"sp_1": xat(i)})
                for i in (1, 2, 4, 3) if direct else (1,):
                    for step in (i, -i) if i < 4 else (i,):
                        send(nz[i - 1], vz(z, x), vz(z, x), {"sp_0": zat(step)})
            else:
                landed(nz[k - 1], vz(z, pl.ds(0, 2)) if k < 4 else vz(z, x))
                if k < 4 and not direct:
                    part = vz(zat(-k), x, 1 if k == 3 else 0)
                    send(nz[k], part, part, zr)
                    part = vz(zat(k), x, 2 if k == 3 else 0)
                    send(nz[k], part, part, zl)
            spread(k)

        def x_step(k):
            if k == 0:
                landed(xs, vx(z, pl.ds(0, 3)))
                send(mz[0], vx(z, whole), vx(z, whole), zr)
                send(mz[0], vx(z, whole), vx(z, whole), zl)
                return
            landed(mz[k - 1], vx(pl.ds(0, 2), whole) if k < 4 else vx(z, whole))
            if k < 4:
                part = vx(zat(-k), lowx if k == 3 else whole)
                send(mz[k], part, part, zr)
                part = vx(zat(k), highx if k == 3 else whole)
                send(mz[k], part, part, zl)

        def f_step(k):
            landed(ns[k], vz(z, pl.ds(0, 2 * len(offsets[k]))))
            for offset in offsets[k]:
                at = zat(offset)
                if 0 <= offset < 4:
                    send(last, vz(at, xat(-1)), vz(at, xat(-1)), xr)
                else:
                    send(last, vz(at, xat(1)), vz(at, xat(1)), xl)

        for k in range(5):
            steps[f"{name}Z{k}"] = functools.partial(z_step, k)
            steps[f"{name}F{k}"] = functools.partial(f_step, k)
            if vx:
                steps[f"{name}X{k}"] = functools.partial(x_step, k)
        steps[f"{name}L"] = lambda: landed(last, vz(pl.ds(0, NZ), x))

    def views(GX, GZ):
        halves = (None, pl.ds(0, 32), pl.ds(32, 32))

        def vz(zi, xi, part=0):
            return GZ.at[zi, xi, halves[part], :] if part else GZ.at[zi, xi]

        return (GX is not None) and (lambda zi, xi: GX.at[zi, xi]), vz

    lanes = (pl.ds(WBX, 256), pl.ds(WBX, 128), pl.ds(WBX + 128, 128))
    plane(
        "L",
        (),
        lambda zi, xi: GB.at[zi, xi, mine, pl.ds(0, WBX)],
        lambda zi, xi, part=0: GB.at[zi, xi, mine, lanes[part]],
    )

    half_z, other_half = pl.ds(0, 4), pl.ds(4, 4)
    ny = sem(), sem()

    def late_part(k, half):
        rows = pl.ds(pl.multiple_of(fat(k) * 16, 16), 16)
        return GB.at[half, :, rows, :]

    def late_y0():
        for n, (a, b) in zip(ny, ((half_z, other_half), (other_half, half_z))):
            send(n, late_part(0, a), late_part(0, a), right, True)
            send(n, late_part(0, b), late_part(0, b), left, True)

    def late_y1():
        landed(ny[0], late_part(0, pl.ds(0, NZ)))
        send(ny[1], late_part(-1, half_z), late_part(-1, half_z), right, True)
        send(ny[1], late_part(1, other_half), late_part(1, other_half), left, True)

    def late_y2():
        landed(ny[1], GB.at[:, :, pl.ds(0, 32), :])

    steps.update(Y0=late_y0, Y1=late_y1, Y2=late_y2)
    plane("1", y1, *views(None, GZ1), direct=True)
    plane("2", y2, *views(GX2, GZ2))
    plane("3", y3, *views(GX3, GZ3))

    ns = sem()

    def start_copies():
        return [copy(ns, SS.at[fat(k)], ST, {"fs": fat(k)}, NSEND + NLONG + i) for i, k in enumerate((1, 2, 3))]

    for made in taken[12:]:
        made.wait()

    @pl.when(f == x)
    def _():
        for i in range(NF):
            SS[i] = jnp.transpose(S0[i]).astype(BF16)
        ST[...] = SS[f]
        for made in start_copies():
            made.start()

    def squares(s):
        w0, w1 = T[0, s].astype(F32), T[1, s].astype(F32)
        square = jnp.sum(w0 * w0 + w1 * w1, axis=1, keepdims=True)
        SC[s] = lax.rsqrt(square * (1.0 / 2048) + EPSILON)

    i0 = lax.broadcasted_iota(jnp.int32, (BLOCK, BLOCK), 0)
    i1 = lax.broadcasted_iota(jnp.int32, (BLOCK, BLOCK), 1)
    causal = i0 >= i1
    tril = jnp.where(causal, 1.0, 0.0).astype(BF16)
    my_room = room[pl.ds(f, 1), :]

    half = NZ // 2

    def each(body):
        for s in range(4):
            body(s, 0)

    def through(slots, *weights):
        count = len(slots) * 256
        at = slice(slots[0], slots[-1] + 1)
        low = jnp.concatenate([w[:half].reshape(1024, w.shape[-1]) for w in weights], axis=1)
        high = jnp.concatenate([w[half:].reshape(1024, w.shape[-1]) for w in weights], axis=1)
        total = dot(T[0, at].reshape(count, 1024), low) + dot(T[1, at].reshape(count, 1024), high)
        total = total * SC[at].reshape(count, 1)
        return [total[256 * i : 256 * i + 256] for i in range(len(slots))]

    def project(slots):
        keys, values, parts, spread = [], [], [], []
        halves = (slice(0, BLOCK), slice(BLOCK, 2 * BLOCK))
        for s, both in zip(slots, through(slots, GZ1)):
            keys.append(my_room * jax.nn.sigmoid(-both[:, :128]))
            values.append(both[:, 128:].astype(BF16))
            K[s], V[s] = keys[-1], values[-1]
        for s, key in zip(slots, keys):
            logs = [p.astype(BF16) for p in three_parts(jnp.log1p(-key))]
            lags = three_parts(SH[s, pl.ds(f, 1), :])
            for rows in halves:
                parts.append(jnp.concatenate([p[rows] for p in logs], axis=0))
                masked = [jnp.broadcast_to(p[:, rows], (BLOCK, BLOCK)) for p in lags]
                masked = [jnp.where(causal, p, 0.0).astype(BF16) for p in masked]
                spread.append(jnp.concatenate(masked, axis=1))
        within = dot(jnp.concatenate([tril] * 3, axis=1), jnp.concatenate(parts, axis=1))
        shifts = dot(jnp.concatenate(spread, axis=0), jnp.ones((3 * BLOCK, BLOCK), BF16))
        ends, faded = [], []
        for i in range(2 * len(slots)):
            block = slice(i * BLOCK, i * BLOCK + BLOCK)
            total = within[:, block] + shifts[block]
            s, rows = slots[i // 2], halves[i % 2]
            C[s, rows, :] = total
            ends.append(total[BLOCK - 1 :])
            faded.append((keys[i // 2][rows] * jnp.exp(ends[-1] - total)).astype(BF16))
        adds = [dot(values[i // 2][halves[i % 2]], k, TN) for i, k in enumerate(faded)]
        for i, s in enumerate(slots):
            A0[s] = adds[2 * i]
            state = jnp.exp(ends[2 * i + 1]) * adds[2 * i] + adds[2 * i + 1]
            SL[s] = pack_state(state, ends[2 * i] + ends[2 * i + 1])

    sx, sz, sb, nb = sem(), sem(), sem(), sem()

    def squares_near():
        landed(near, T.at[other, pl.ds(0, 3)])
        for s in range(3):
            squares(s)

    def project_near():
        landed(nshift, SH.at[pl.ds(0, 3)])
        project((0, 1, 2))

    def project_far():
        landed(far_off, T.at[other, 3])
        squares(3)
        project((3,))
        slot_of = lambda sequence: lax.rem(sequence - f + (NF + 1), NF)
        SR[x] = SL[slot_of(x)]
        for k in (1, 3, 2):
            send(sx, SL.at[slot_of(xat(k))], SR.at[x], {"sp_1": xat(k)})

    def total_x():
        landed(sx, SR.at[pl.ds(0, 3)])
        state, decay = unpack_state(SR[0])
        for i in range(1, NX):
            later, fade = unpack_state(SR[i])
            state, decay = jnp.exp(fade) * state + later, decay + fade
        ZS[...] = pack_state(state, decay)
        for k in (4, 3, 5, 2, 6, 1, 7):
            send(sz, ZS, ZR.at[z], {"sp_0": zat(k)})

    def project_rest(s, rest):
        query = rest[:, :128]
        Q[s] = query * jax.nn.sigmoid(query) * HEAD ** (-0.5)
        gate = rest[:, 128:256]
        G[s] = gate * jax.nn.sigmoid(gate) * hgain[...]
        pool = rest[:, 256:].astype(BF16)
        EXT[s, 128:384, :] = pool
        BS[s] = pool[240:256]

    def rest():
        for slots in ((0, 1), (2, 3)):
            for s, projected in zip(slots, through(slots, GX2, GZ2)):
                project_rest(s, projected)
        send(nb, BS, BR, nxt)

    def inner(s, _):
        for b in range(2):
            rows = slice(b * BLOCK, (b + 1) * BLOCK)
            within = C[s, rows, :]
            centre = within[BLOCK // 2 - 1 : BLOCK // 2]
            query, keys = Q[s, rows, :], K[s, rows, :]
            scores = dot(
                (query * jnp.exp(within - centre)).astype(BF16),
                (keys * jnp.exp(centre - within)).astype(BF16),
                NT,
            )
            scores = jnp.where(causal, scores, 0.0).astype(BF16)
            INS[s, rows, :] = dot(scores, V[s, rows, :])
            QE[s, rows, :] = (query * jnp.exp(within)).astype(BF16)
        return 0

    span = lax.shift_left(jnp.int32(2), c * 2 + f // 2)
    ti = lax.broadcasted_iota(jnp.int32, (256, 384), 0)
    si = lax.broadcasted_iota(jnp.int32, (256, 384), 1) - 128
    band = jnp.where((si <= ti) & (si > ti - span) & (si >= -16), 1.0, 0.0).astype(BF16)
    position = here * 256 + lax.broadcasted_iota(jnp.int32, (256, 128), 0)
    inverse = 1.0 / jnp.minimum(position + 1, span).astype(F32)

    def pool(s, _):
        EXT[s, 0:128, :] = jnp.zeros((128, 128), BF16)

        @pl.when(here > 0)
        def _():
            EXT[s, 112:128, :] = BR[s]

        window = dot(band, EXT[s])
        PO[s] = (window * inverse - EXT[s, 128:384, :].astype(F32)).astype(BF16)
        return 0

    given_pool, given_rec = sem(), sem()

    def give_back(buffer, slot, n, sources):
        for s in sources:
            if s == 1:
                ACT[slot + f] = buffer[1]
            else:
                send(n, buffer.at[s], ACT.at[slot + f], {"fs": fat(s - 1)})

    def pooling():
        landed(nb, BR)
        each(pool)
        give_back(PO, 4, given_pool, (0, 2, 3, 1))

    def pass_z(i, state):
        later, fade = unpack_state(ZR[i])
        return jnp.exp(fade) * state + later

    def from_z():
        landed(sz, ZR.at[pl.ds(0, NZ - 1)])

        @pl.when(f != x)
        def _():
            landed(ns, ST)

        state = lax.fori_loop(0, z, pass_z, ST[...].astype(F32))
        for i in range(NX):
            ES[i] = state.astype(BF16)
            if i < NX - 1:
                later, fade = unpack_state(SR[i])
                state = jnp.exp(fade) * state + later
        ER[x] = ES[x]
        for k in (1, 3, 2):
            send(sb, ES.at[xat(k)], ER.at[x], {"sp_1": xat(k)})

    def finishing():
        landed(sb, ER.at[pl.ds(0, 3)])
        raws, order = {}, (3, 0, 2, 1)
        for s in order:
            entering = ER[fat(s - 1)]
            middle = jnp.exp(C[s, BLOCK - 1 : BLOCK, :]) * entering.astype(F32) + A0[s]
            carried = [dot(QE[s, :BLOCK, :], entering, NT), dot(QE[s, BLOCK:, :], middle.astype(BF16), NT)]
            raws[s] = INS[s] + jnp.concatenate(carried, axis=0)
        for s in order:
            square = jnp.mean(raws[s] * raws[s], axis=1, keepdims=True)
            RO[s] = (raws[s] * lax.rsqrt(square + EPSILON) * G[s]).astype(BF16)
            give_back(RO, 0, given_rec, (s,))

    def out_pool():
        landed(given_pool, ACT.at[pl.ds(4, 3)])
        act = jnp.concatenate([ACT[4 + i] for i in range(4)], axis=1)
        for i in range(4):
            at, cols = slice(2 * i, 2 * i + 2), slice(512 * i, 512 * i + 512)
            PT[:, cols] = dot(act, GB[at].reshape(512, WB), NT)

    steps.update(
        SQ=squares_near,
        PR3=project_near,
        PR1=project_far,
        SUMX=total_x,
        REST=rest,
        INNER=lambda: each(inner),
        POOL=pooling,
        PASSZ=from_z,
        FIN=finishing,
        OUTP=out_pool,
    )
    order = ORDER
    assert sorted(order) == sorted(steps)
    for step in order:
        with jax.named_scope(step):
            steps[step]()

    for made in sent[-NSEND:-12] + sent_long[-NLONG:]:
        finish_send(made)
    landed(given_rec, ACT.at[pl.ds(0, 3)])

    act = jnp.concatenate([ACT[i] for i in range(4)], axis=1)
    my_rows = pl.ds(pl.multiple_of(c * 128, 128), 128)
    their_rows = pl.ds(pl.multiple_of(other * 128, 128), 128)
    swap = sem()
    for i in range(4):
        at, cols = slice(2 * i, 2 * i + 2), slice(512 * i, 512 * i + 512)
        weight = [w[at].reshape(512, w.shape[-1]) for w in (GX3, GZ3)]
        total = PT[:, cols] + dot(act, jnp.concatenate(weight, axis=1), NT)
        PS[:, cols] = total.astype(BF16)
        send(swap, PS.at[their_rows, pl.ds(512 * i, 512)], PR.at[:, pl.ds(512 * i, 512)], {"tp": other})
    landed(swap, PR)
    out[...] = (PS[my_rows, :].astype(F32) + PR[...].astype(F32)).astype(BF16)

    for made in sent[-NSEND:] + sent_long[-NLONG:]:
        finish_send(made)

    @pl.when(f == x)
    def _():
        for made in start_copies():
            made.wait_send()


def per_device(
    tokens,
    norm_gain,
    query_weight,
    forget_weight,
    value_weight,
    outgate_weight,
    pool_in_weight,
    forget_room,
    decay_shift,
    head_gain,
    start_state,
    pool_map,
    pool_scale,
    out_rec_weight,
    out_pool_weight,
):
    vmem = lambda *shape: pltpu.VMEM(shape, F32)
    half = lambda *shape: pltpu.VMEM(shape, BF16)
    mixed = pl.pallas_call(
        kernel,
        out_shape=jax.ShapeDtypeStruct((128, 2048), BF16),
        in_specs=[pl.BlockSpec(memory_space=pltpu.HBM)] * 15,
        out_specs=pl.BlockSpec(memory_space=pltpu.VMEM),
        scratch_shapes=[
            half(2, 4, 256, 1024),
            half(NZ, NX, 64, WZ[0]),
            half(NZ, NX, 64, WX[0]),
            half(NZ, NX, 64, WZ[1]),
            half(NZ, NX, 64, WX[1]),
            half(NZ, NX, 64, WZ[2]),
            half(NZ, NX, 64, WB),
            vmem(4, 4, 256),
            half(128, 128),
            vmem(4, 256, 128),
            half(4, 256, 128),
            vmem(4, 256, 128),
            vmem(4, 256, 128),
            vmem(4, 256, 128),
            half(4, 256, 128),
            vmem(4, 256, 128),
            vmem(4, 128, 128),
            half(4, 144, 128),
            half(4, 144, 128),
            half(144, 128),
            half(NZ, 144, 128),
            half(4, 128, 128),
            half(4, 128, 128),
            half(4, 384, 128),
            half(4, 16, 128),
            half(4, 16, 128),
            half(4, 256, 128),
            half(4, 256, 128),
            half(8, 256, 128),
            half(256, 2048),
            half(128, 2048),
            vmem(4, 256, 1),
            half(4, 128, 128),
            vmem(4, 128, 128),
            half(2, 256, 256),
            vmem(256, 2048),
            vmem(16, 128),
            *[half(16, 512)] * 5,
            vmem(1, 512),
            *[half(16, 512)] * 2,
            vmem(4, 128),
            vmem(1, 128),
            half(4, 16, 256),
            half(4, 16, 128),
            half(4, 16, 256),
            half(16, 512),
            pltpu.SemaphoreType.DMA((NSEND + NLONG + 3,)),
            pltpu.SemaphoreType.DMA((NRECV,)),
            pltpu.SemaphoreType.DMA((15,)),
        ],
        compiler_params=pltpu.CompilerParams(
            collective_id=0, has_side_effects=True, vmem_limit_bytes=48 * 1024 * 1024
        ),
    )(
        *[pltpu.with_memory_space_constraint(a, pltpu.HBM) for a in (
        tokens[0],
        norm_gain.reshape(16, 128),
        query_weight,
        forget_weight,
        value_weight,
        outgate_weight,
        pool_in_weight,
        forget_room.reshape(4, 128),
        decay_shift[0].T,
        head_gain.reshape(1, 128),
        start_state,
        pool_map,
        pool_scale.reshape(1, 512),
        out_rec_weight.T,
        out_pool_weight.T,
    )]
    )
    return mixed[None]


def solution(mesh):
    finer = Mesh(
        mesh.devices.reshape(8, 4, mesh.shape["fs"], mesh.shape["tp"]), ("sp_0", "sp_1", "fs", "tp")
    )
    placed = (
        P("fs", SP, "tp"),
        P(),
        P(SP_FS, "tp"),
        P(SP_FS, "tp"),
        P(SP_FS, "tp"),
        P(SP_FS, "tp"),
        P(SP_FS, "tp"),
        P("tp"),
        P("fs", SP, "tp"),
        P(),
        P("fs", "tp", None, None),
        P("tp", None, None),
        P("tp"),
        P("tp", SP_FS),
        P("tp", SP_FS),
    )
    return jax.shard_map(
        per_device, mesh=finer, in_specs=placed, out_specs=P("fs", SP_TP, None), check_vma=False
    )
```

```python
import functools

import jax
import jax.numpy as jnp
from jax import lax
from jax.experimental import pallas as pl
from jax.experimental.pallas import tpu as pltpu
from jax.sharding import Mesh
from jax.sharding import PartitionSpec as P

HEAD = 128
POOL_DIM = 256
BLOCK = 128
SP_FS = ("sp_0", "sp_1", "fs")
SP = ("sp_0", "sp_1")
SP_TP = ("sp_0", "sp_1", "tp")
EPSILON = 1e-06
MESH = pl.DeviceIdType.MESH
ORDER = (
    "LZ0",
    "LZ1",
    "LF0",
    "1Z0",
    "LX0",
    "3Z0",
    "LZ2",
    "LF1",
    "2Z0",
    "1Z1",
    "1Z2",
    "LF2",
    "T1",
    "2X0",
    "1F0",
    "1Z3",
    "1Z4",
    "LX1",
    "1F1",
    "LZ3",
    "2Z1",
    "1F2",
    "2X1",
    "T2",
    "LX2",
    "LZ4",
    "1F3",
    "3X0",
    "1F4",
    "2F0",
    "SQ",
    "2Z2",
    "LF3",
    "2F1",
    "LX3",
    "LF4",
    "3Z1",
    "T3",
    "1L",
    "PR3",
    "PR1",
    "2Z3",
    "2X2",
    "LX4",
    "LL",
    "Y0",
    "2F2",
    "3X1",
    "2Z4",
    "3Z2",
    "2X3",
    "SUMX",
    "2F3",
    "3F0",
    "3F1",
    "2F4",
    "3Z3",
    "Y1",
    "3F2",
    "2L",
    "2X4",
    "REST",
    "3X2",
    "3F3",
    "PASSZ",
    "INNER",
    "3Z4",
    "POOL",
    "3X3",
    "FIN",
    "3F4",
    "Y2",
    "3X4",
    "OUTP",
    "3L",
)
NRECV, NSEND, NLONG = 77, 40, 13
NZ, NX, NF = 8, 4, 4
WX, WZ, WB, WBX = (128, 256), (256, 256, 256), 512, 256
F32, BF16 = jnp.float32, jnp.bfloat16
NT = (((1,), (1,)), ((), ()))
TN = (((0,), (0,)), ((), ()))


def dot(a, b, dims=(((1,), (0,)), ((), ()))):
    return lax.dot_general(a, b, dims, preferred_element_type=F32)


def pack_state(state, decay):
    high, mid, low = three_parts(decay)
    row = lax.broadcasted_iota(jnp.int32, (16, HEAD), 0)
    tail = jnp.where(row == 0, high, jnp.where(row == 1, mid, jnp.where(row == 2, low, 0.0)))
    return jnp.concatenate([state, tail], axis=0).astype(BF16)


def three_parts(value):
    high = value.astype(BF16).astype(F32)
    rest = value - high
    mid = rest.astype(BF16).astype(F32)
    return high, mid, rest - mid


def unpack_state(packed):
    whole = packed.astype(F32)
    decay = jnp.sum(whole[HEAD : HEAD + 16], axis=0, keepdims=True)
    return whole[:HEAD], decay


def kernel(
    h_tok,
    h_gain,
    h_wq,
    h_wf,
    h_wv,
    h_wo,
    h_wp,
    h_room,
    h_shift,
    h_hgain,
    h_start,
    h_pmap,
    h_pscale,
    h_worec,
    h_wopool,
    out,
    T,
    GZ1,
    GX2,
    GZ2,
    GX3,
    GZ3,
    GB,
    SH,
    ST,
    K,
    V,
    Q,
    G,
    C,
    QE,
    INS,
    A0,
    SL,
    SR,
    ZS,
    ZR,
    ES,
    ER,
    EXT,
    BS,
    BR,
    RO,
    PO,
    ACT,
    PS,
    PR,
    SC,
    SS,
    S0,
    PM,
    PT,
    gain,
    wq,
    wf,
    wv,
    wo,
    wp,
    pscale,
    worec,
    wopool,
    room,
    hgain,
    iz1,
    ix2,
    iz2,
    ixz3,
    send_sems,
    recv_sems,
    local_sems,
):
    z, x = lax.axis_index("sp_0"), lax.axis_index("sp_1")
    f, c = lax.axis_index("fs"), lax.axis_index("tp")
    zat = lambda k: lax.rem(z + (k + NZ), NZ)
    xat = lambda k: lax.rem(x + (k + NX), NX)
    fat = lambda k: lax.rem(f + (k + NF), NF)
    other = 1 - c
    here = z * NX + x
    after = lax.rem(here + 1, NZ * NX)
    ahead = lax.rem(here + NZ * NX - 1, NZ * NX)
    nxt = {"sp_0": after // NX, "sp_1": lax.rem(after, NX)}
    prv = {"sp_0": ahead // NX, "sp_1": lax.rem(ahead, NX)}

    arguments = (
        (h_gain, gain),
        (h_wf, wf),
        (h_wv, wv),
        (h_wq, wq),
        (h_wo, wo),
        (h_wp, wp),
        (h_pmap, PM),
        (h_pscale, pscale),
        (h_worec, worec),
        (h_wopool, wopool),
        (h_tok, T.at[c, 1]),
        (h_shift, SH.at[1]),
        (h_start.at[0], S0),
        (h_room, room),
        (h_hgain, hgain),
    )
    taken = [pltpu.make_async_copy(a, b, local_sems.at[i]) for i, (a, b) in enumerate(arguments)]
    for made in taken:
        made.start()

    barrier = pltpu.get_barrier_semaphore()
    met = [{"tp": other}, nxt, prv]
    met += [{"fs": fat(k)} for k in (1, 2, 3)] + [{"sp_1": xat(k)} for k in (1, 2, 3)]
    met += [{"sp_0": zat(k)} for k in range(1, NZ)]
    for who in met:
        pl.semaphore_signal(barrier, inc=1, device_id=who, device_id_type=MESH)

    count = [0]
    sent, sent_long = [], []

    def sem():
        count[0] += 1
        assert count[0] <= NRECV
        return count[0] - 1

    def copy(n, src, dst, who, slot=0):
        return pltpu.make_async_remote_copy(
            src_ref=src,
            dst_ref=dst,
            send_sem=send_sems.at[slot],
            recv_sem=recv_sems.at[n],
            device_id=who,
            device_id_type=MESH,
        )

    waited = set()

    def finish_send(made):
        if id(made) not in waited:
            waited.add(id(made))
            made.wait_send()

    def send(n, src, dst, who, long=False):
        made_before, slots, base = (sent_long, NLONG, NSEND) if long else (sent, NSEND, 0)
        if len(made_before) >= slots:
            finish_send(made_before[-slots])
        made = copy(n, src, dst, who, base + len(made_before) % slots)
        made.start()
        made_before.append(made)

    def landed(n, dst):
        copy(n, dst, dst, {"tp": other}).wait_recv()

    rank = here * NF + f
    row = lax.broadcasted_iota(jnp.int32, (16, 128), 0)
    lane = lax.broadcasted_iota(jnp.int32, (16, 128), 1)
    for made in taken[:3]:
        made.wait()
    gains = jnp.broadcast_to(gain[pl.ds(rank // 8, 1), :], (16, 128))
    gains = jnp.where(lane == lax.rem(rank, 8) * 16 + row, gains, 0.0)
    gains = jnp.sum(gains, axis=1, keepdims=True)
    mine = pl.ds(pl.multiple_of(f * 16, 16), 16)

    def stage(buffer, place, weights):
        for i in range(NF):
            chunk = [w[:, 128 * i : 128 * i + 128] for w in weights]
            buffer[i] = jnp.concatenate(chunk, axis=1)
        place[z, x, mine, :] = buffer[f]

    def scaled(w):
        return (w[...].astype(F32) * gains).astype(BF16)

    stage(iz1, GZ1, (scaled(wf), scaled(wv)))
    pl.semaphore_wait(barrier, len(met))

    def over_y(pairs):
        ns = [sem() for _ in pairs]
        for k in (1, 3, 2):
            to = fat(k)
            for n, (buffer, own) in zip(ns, pairs):
                send(n, own.at[to], buffer.at[z, x, mine, :], {"fs": to})
        return [(n, buffer.at[z, x, pl.ds(0, 48), :]) for n, (buffer, _) in zip(ns, pairs)]

    def over_out():
        ns = sem(), sem()
        for k in (1, 3, 2):
            to = {"fs": fat(k)}
            send(ns[0], ixz3.at[:, pl.ds(0, 256)], GX3.at[z, x, mine, :], to)
            send(ns[1], ixz3.at[:, pl.ds(256, 256)], GZ3.at[z, x, mine, :], to)
        return [(n, b.at[z, x, pl.ds(0, 48), :]) for n, b in zip(ns, (GX3, GZ3))]

    y1 = over_y(((GZ1, iz1),))
    for made in taken[3:12]:
        made.wait()
    folded = [dot(wp[:, 256 * i : 256 * i + 256], PM[i]) for i in range(2)]
    folded = (jnp.concatenate(folded, axis=1) * gains * pscale[...]).astype(BF16)
    turned = jnp.concatenate([worec[...], wopool[...]], axis=1)
    stage(ix2, GX2, (scaled(wq),))
    stage(iz2, GZ2, (scaled(wo), folded))
    ixz3[...] = turned[:, :512]
    GX3[z, x, mine, :] = turned[:, :256]
    GZ3[z, x, mine, :] = turned[:, 256:512]
    GB[z, x, mine, :] = turned[:, 512:]
    y2 = over_y(((GX2, ix2), (GZ2, iz2)))
    y3 = over_out()
    nshift = sem()
    for k in (1, 3, 2):
        send(nshift, SH.at[1], SH.at[(5 - k) % 4], {"fs": fat(k)})

    first, second = pl.ds(0, 128), pl.ds(128, 128)
    right, left = {"fs": fat(1)}, {"fs": fat(3)}
    nt = [sem() for _ in range(3)]
    near, far_off = sem(), sem()

    def relay(n, seq, rows):
        send(n, T.at[c, seq, rows, :], T.at[c, seq, rows, :], {"tp": other}, True)

    for i, (a, b) in enumerate(((first, second), (second, first))):
        send(nt[i], T.at[c, 1, a, :], T.at[c, 0, a, :], right, True)
        send(nt[i], T.at[c, 1, b, :], T.at[c, 2, b, :], left, True)
    send(near, T.at[c, 1], T.at[c, 1], {"tp": other}, True)

    def tokens_1():
        landed(nt[0], T.at[c, 0])
        send(nt[2], T.at[c, 0, first, :], T.at[c, 3, first, :], right, True)
        send(nt[2], T.at[c, 2, second, :], T.at[c, 3, second, :], left, True)
        relay(near, 0, first)
        relay(near, 2, second)

    def tokens_2():
        landed(nt[1], T.at[c, 0])
        relay(near, 0, second)
        relay(near, 2, first)

    def tokens_3():
        landed(nt[2], T.at[c, 3])
        relay(far_off, 3, first)
        relay(far_off, 3, second)

    steps = {"T1": tokens_1, "T2": tokens_2, "T3": tokens_3}

    def plane(name, waits, vx, vz, direct=False):
        zr, zl = {"sp_0": zat(1)}, {"sp_0": zat(-1)}
        xr, xl = {"sp_1": xat(1)}, {"sp_1": xat(-1)}
        whole, lowx, highx = pl.ds(0, 4), pl.ds(0, 2), pl.ds(2, 2)
        nz, ns, last = [sem() for _ in range(4)], [sem() for _ in range(5)], sem()
        if vx:
            xs, mz = sem(), [sem() for _ in range(4)]
        offsets = ((0,), (-1, 1), (-2, 2), (-3, 3), (4,))

        def spread(k):
            for offset in offsets[k]:
                at = zat(offset)
                send(ns[k], vz(at, x), vz(at, x), xr)
                send(ns[k], vz(at, x), vz(at, x), xl)

        def z_step(k):
            if k == 0:
                for w in waits:
                    landed(*w)
                if vx:
                    for i in (1, 3, 2):
                        send(xs, vx(z, x), vx(z, x), {"sp_1": xat(i)})
                for i in (1, 2, 4, 3) if direct else (1,):
                    for step in (i, -i) if i < 4 else (i,):
                        send(nz[i - 1], vz(z, x), vz(z, x), {"sp_0": zat(step)})
            else:
                landed(nz[k - 1], vz(z, pl.ds(0, 2)) if k < 4 else vz(z, x))
                if k < 4 and not direct:
                    part = vz(zat(-k), x, 1 if k == 3 else 0)
                    send(nz[k], part, part, zr)
                    part = vz(zat(k), x, 2 if k == 3 else 0)
                    send(nz[k], part, part, zl)
            spread(k)

        def x_step(k):
            if k == 0:
                landed(xs, vx(z, pl.ds(0, 3)))
                send(mz[0], vx(z, whole), vx(z, whole), zr)
                send(mz[0], vx(z, whole), vx(z, whole), zl)
                return
            landed(mz[k - 1], vx(pl.ds(0, 2), whole) if k < 4 else vx(z, whole))
            if k < 4:
                part = vx(zat(-k), lowx if k == 3 else whole)
                send(mz[k], part, part, zr)
                part = vx(zat(k), highx if k == 3 else whole)
                send(mz[k], part, part, zl)

        def f_step(k):
            landed(ns[k], vz(z, pl.ds(0, 2 * len(offsets[k]))))
            for offset in offsets[k]:
                at = zat(offset)
                if 0 <= offset < 4:
                    send(last, vz(at, xat(-1)), vz(at, xat(-1)), xr)
                else:
                    send(last, vz(at, xat(1)), vz(at, xat(1)), xl)

        for k in range(5):
            steps[f"{name}Z{k}"] = functools.partial(z_step, k)
            steps[f"{name}F{k}"] = functools.partial(f_step, k)
            if vx:
                steps[f"{name}X{k}"] = functools.partial(x_step, k)
        steps[f"{name}L"] = lambda: landed(last, vz(pl.ds(0, NZ), x))

    def views(GX, GZ):
        halves = (None, pl.ds(0, 32), pl.ds(32, 32))

        def vz(zi, xi, part=0):
            return GZ.at[zi, xi, halves[part], :] if part else GZ.at[zi, xi]

        return (GX is not None) and (lambda zi, xi: GX.at[zi, xi]), vz

    lanes = (pl.ds(WBX, 256), pl.ds(WBX, 128), pl.ds(WBX + 128, 128))
    plane(
        "L",
        (),
        lambda zi, xi: GB.at[zi, xi, mine, pl.ds(0, WBX)],
        lambda zi, xi, part=0: GB.at[zi, xi, mine, lanes[part]],
    )

    half_z, other_half = pl.ds(0, 4), pl.ds(4, 4)
    ny = sem(), sem()

    def late_part(k, half):
        rows = pl.ds(pl.multiple_of(fat(k) * 16, 16), 16)
        return GB.at[half, :, rows, :]

    def late_y0():
        for n, (a, b) in zip(ny, ((half_z, other_half), (other_half, half_z))):
            send(n, late_part(0, a), late_part(0, a), right, True)
            send(n, late_part(0, b), late_part(0, b), left, True)

    def late_y1():
        landed(ny[0], late_part(0, pl.ds(0, NZ)))
        send(ny[1], late_part(-1, half_z), late_part(-1, half_z), right, True)
        send(ny[1], late_part(1, other_half), late_part(1, other_half), left, True)

    def late_y2():
        landed(ny[1], GB.at[:, :, pl.ds(0, 32), :])

    steps.update(Y0=late_y0, Y1=late_y1, Y2=late_y2)
    plane("1", y1, *views(None, GZ1), direct=True)
    plane("2", y2, *views(GX2, GZ2))
    plane("3", y3, *views(GX3, GZ3))

    ns = sem()

    def start_copies():
        return [copy(ns, SS.at[fat(k)], ST, {"fs": fat(k)}, NSEND + NLONG + i) for i, k in enumerate((1, 2, 3))]

    for made in taken[12:]:
        made.wait()

    @pl.when(f == x)
    def _():
        for i in range(NF):
            SS[i] = jnp.transpose(S0[i]).astype(BF16)
        ST[...] = SS[f]
        for made in start_copies():
            made.start()

    def squares(s):
        w0, w1 = T[0, s].astype(F32), T[1, s].astype(F32)
        square = jnp.sum(w0 * w0 + w1 * w1, axis=1, keepdims=True)
        SC[s] = lax.rsqrt(square * (1.0 / 2048) + EPSILON)

    i0 = lax.broadcasted_iota(jnp.int32, (BLOCK, BLOCK), 0)
    i1 = lax.broadcasted_iota(jnp.int32, (BLOCK, BLOCK), 1)
    causal = i0 >= i1
    tril = jnp.where(causal, 1.0, 0.0).astype(BF16)
    my_room = room[pl.ds(f, 1), :]

    half = NZ // 2

    def each(body):
        for s in range(4):
            body(s, 0)

    def through(slots, *weights):
        count = len(slots) * 256
        at = slice(slots[0], slots[-1] + 1)
        low = jnp.concatenate([w[:half].reshape(1024, w.shape[-1]) for w in weights], axis=1)
        high = jnp.concatenate([w[half:].reshape(1024, w.shape[-1]) for w in weights], axis=1)
        total = dot(T[0, at].reshape(count, 1024), low) + dot(T[1, at].reshape(count, 1024), high)
        if slots == (3,):
            squares(3)
        total = total * SC[at].reshape(count, 1)
        return [total[256 * i : 256 * i + 256] for i in range(len(slots))]

    def project(slots):
        keys, values, parts, spread = [], [], [], []
        halves = (slice(0, BLOCK), slice(BLOCK, 2 * BLOCK))
        for s, both in zip(slots, through(slots, GZ1)):
            keys.append(my_room * jax.nn.sigmoid(-both[:, :128]))
            values.append(both[:, 128:].astype(BF16))
            K[s], V[s] = keys[-1], values[-1]
        for s, key in zip(slots, keys):
            logs = [p.astype(BF16) for p in three_parts(jnp.log1p(-key))]
            lags = three_parts(SH[s, pl.ds(f, 1), :])
            for rows in halves:
                parts.append(jnp.concatenate([p[rows] for p in logs], axis=0))
                masked = [jnp.broadcast_to(p[:, rows], (BLOCK, BLOCK)) for p in lags]
                masked = [jnp.where(causal, p, 0.0).astype(BF16) for p in masked]
                spread.append(jnp.concatenate(masked, axis=1))
        within = dot(jnp.concatenate([tril] * 3, axis=1), jnp.concatenate(parts, axis=1))
        shifts = dot(jnp.concatenate(spread, axis=0), jnp.ones((3 * BLOCK, BLOCK), BF16))
        ends, faded = [], []
        for i in range(2 * len(slots)):
            block = slice(i * BLOCK, i * BLOCK + BLOCK)
            total = within[:, block] + shifts[block]
            s, rows = slots[i // 2], halves[i % 2]
            C[s, rows, :] = total
            ends.append(total[BLOCK - 1 :])
            faded.append((keys[i // 2][rows] * jnp.exp(ends[-1] - total)).astype(BF16))
        adds = [dot(values[i // 2][halves[i % 2]], k, TN) for i, k in enumerate(faded)]
        for i, s in enumerate(slots):
            A0[s] = adds[2 * i]
            state = jnp.exp(ends[2 * i + 1]) * adds[2 * i] + adds[2 * i + 1]
            SL[s] = pack_state(state, ends[2 * i] + ends[2 * i + 1])

    sx, sz, sb, nb = sem(), sem(), sem(), sem()

    def squares_near():
        landed(near, T.at[other, pl.ds(0, 3)])
        for s in range(3):
            squares(s)

    def project_near():
        landed(nshift, SH.at[pl.ds(0, 3)])
        project((0, 1, 2))

    def project_far():
        landed(far_off, T.at[other, 3])
        project((3,))
        slot_of = lambda sequence: lax.rem(sequence - f + (NF + 1), NF)
        SR[x] = SL[slot_of(x)]
        for k in (1, 3, 2):
            send(sx, SL.at[slot_of(xat(k))], SR.at[x], {"sp_1": xat(k)})

    def total_x():
        landed(sx, SR.at[pl.ds(0, 3)])
        state, decay = unpack_state(SR[0])
        for i in range(1, NX):
            later, fade = unpack_state(SR[i])
            state, decay = jnp.exp(fade) * state + later, decay + fade
        ZS[...] = pack_state(state, decay)
        for k in (4, 3, 5, 2, 6, 1, 7):
            send(sz, ZS, ZR.at[z], {"sp_0": zat(k)})

    def project_rest(s, rest):
        query = rest[:, :128]
        Q[s] = query * jax.nn.sigmoid(query) * HEAD ** (-0.5)
        gate = rest[:, 128:256]
        G[s] = gate * jax.nn.sigmoid(gate) * hgain[...]
        pool = rest[:, 256:].astype(BF16)
        EXT[s, 128:384, :] = pool
        BS[s] = pool[240:256]

    def rest():
        for slots in ((0, 1), (2, 3)):
            for s, projected in zip(slots, through(slots, GX2, GZ2)):
                project_rest(s, projected)
        send(nb, BS, BR, nxt)

    def inner(s, _):
        for b in range(2):
            rows = slice(b * BLOCK, (b + 1) * BLOCK)
            within = C[s, rows, :]
            centre = within[BLOCK // 2 - 1 : BLOCK // 2]
            query, keys = Q[s, rows, :], K[s, rows, :]
            scores = dot(
                (query * jnp.exp(within - centre)).astype(BF16),
                (keys * jnp.exp(centre - within)).astype(BF16),
                NT,
            )
            scores = jnp.where(causal, scores, 0.0).astype(BF16)
            INS[s, rows, :] = dot(scores, V[s, rows, :])
            QE[s, rows, :] = (query * jnp.exp(within)).astype(BF16)
        return 0

    span = lax.shift_left(jnp.int32(2), c * 2 + f // 2)
    ti = lax.broadcasted_iota(jnp.int32, (256, 384), 0)
    si = lax.broadcasted_iota(jnp.int32, (256, 384), 1) - 128
    band = jnp.where((si <= ti) & (si > ti - span) & (si >= -16), 1.0, 0.0).astype(BF16)
    position = here * 256 + lax.broadcasted_iota(jnp.int32, (256, 128), 0)
    inverse = 1.0 / jnp.minimum(position + 1, span).astype(F32)

    def pool(s, _):
        EXT[s, 0:128, :] = jnp.zeros((128, 128), BF16)

        @pl.when(here > 0)
        def _():
            EXT[s, 112:128, :] = BR[s]

        window = dot(band, EXT[s])
        PO[s] = (window * inverse - EXT[s, 128:384, :].astype(F32)).astype(BF16)
        return 0

    given_pool, given_rec = sem(), sem()

    def give_back(buffer, slot, n, sources):
        for s in sources:
            if s == 1:
                ACT[slot + f] = buffer[1]
            else:
                send(n, buffer.at[s], ACT.at[slot + f], {"fs": fat(s - 1)})

    def pooling():
        landed(nb, BR)
        each(pool)
        give_back(PO, 4, given_pool, (0, 2, 3, 1))

    def pass_z(i, state):
        later, fade = unpack_state(ZR[i])
        return jnp.exp(fade) * state + later

    def from_z():
        landed(sz, ZR.at[pl.ds(0, NZ - 1)])

        @pl.when(f != x)
        def _():
            landed(ns, ST)

        state = lax.fori_loop(0, z, pass_z, ST[...].astype(F32))
        for i in range(NX):
            ES[i] = state.astype(BF16)
            if i < NX - 1:
                later, fade = unpack_state(SR[i])
                state = jnp.exp(fade) * state + later
        ER[x] = ES[x]
        for k in (1, 3, 2):
            send(sb, ES.at[xat(k)], ER.at[x], {"sp_1": xat(k)})

    def finishing():
        landed(sb, ER.at[pl.ds(0, 3)])
        raws, order = {}, (3, 0, 2, 1)
        for s in order:
            entering = ER[fat(s - 1)]
            middle = jnp.exp(C[s, BLOCK - 1 : BLOCK, :]) * entering.astype(F32) + A0[s]
            carried = [dot(QE[s, :BLOCK, :], entering, NT), dot(QE[s, BLOCK:, :], middle.astype(BF16), NT)]
            raws[s] = INS[s] + jnp.concatenate(carried, axis=0)
        for s in order:
            square = jnp.mean(raws[s] * raws[s], axis=1, keepdims=True)
            RO[s] = (raws[s] * lax.rsqrt(square + EPSILON) * G[s]).astype(BF16)
            give_back(RO, 0, given_rec, (s,))

    def out_pool():
        landed(given_pool, ACT.at[pl.ds(4, 3)])
        act = jnp.concatenate([ACT[4 + i] for i in range(4)], axis=1)
        for i in range(4):
            at, cols = slice(2 * i, 2 * i + 2), slice(512 * i, 512 * i + 512)
            PT[:, cols] = dot(act, GB[at].reshape(512, WB), NT)

    steps.update(
        SQ=squares_near,
        PR3=project_near,
        PR1=project_far,
        SUMX=total_x,
        REST=rest,
        INNER=lambda: each(inner),
        POOL=pooling,
        PASSZ=from_z,
        FIN=finishing,
        OUTP=out_pool,
    )
    order = ORDER
    assert sorted(order) == sorted(steps)
    for step in order:
        with jax.named_scope(step):
            steps[step]()

    for made in sent[-NSEND:-12] + sent_long[-NLONG:]:
        finish_send(made)
    landed(given_rec, ACT.at[pl.ds(0, 3)])

    act = jnp.concatenate([ACT[i] for i in range(4)], axis=1)
    my_rows = pl.ds(pl.multiple_of(c * 128, 128), 128)
    their_rows = pl.ds(pl.multiple_of(other * 128, 128), 128)
    swap = sem()
    for i in range(4):
        at, cols = slice(2 * i, 2 * i + 2), slice(512 * i, 512 * i + 512)
        weight = [w[at].reshape(512, w.shape[-1]) for w in (GX3, GZ3)]
        total = PT[:, cols] + dot(act, jnp.concatenate(weight, axis=1), NT)
        PS[:, cols] = total.astype(BF16)
        send(swap, PS.at[their_rows, pl.ds(512 * i, 512)], PR.at[:, pl.ds(512 * i, 512)], {"tp": other})
    landed(swap, PR)
    out[...] = (PS[my_rows, :].astype(F32) + PR[...].astype(F32)).astype(BF16)

    for made in sent[-NSEND:] + sent_long[-NLONG:]:
        finish_send(made)

    @pl.when(f == x)
    def _():
        for made in start_copies():
            made.wait_send()


def per_device(
    tokens,
    norm_gain,
    query_weight,
    forget_weight,
    value_weight,
    outgate_weight,
    pool_in_weight,
    forget_room,
    decay_shift,
    head_gain,
    start_state,
    pool_map,
    pool_scale,
    out_rec_weight,
    out_pool_weight,
):
    vmem = lambda *shape: pltpu.VMEM(shape, F32)
    half = lambda *shape: pltpu.VMEM(shape, BF16)
    mixed = pl.pallas_call(
        kernel,
        out_shape=jax.ShapeDtypeStruct((128, 2048), BF16),
        in_specs=[pl.BlockSpec(memory_space=pltpu.HBM)] * 15,
        out_specs=pl.BlockSpec(memory_space=pltpu.VMEM),
        scratch_shapes=[
            half(2, 4, 256, 1024),
            half(NZ, NX, 64, WZ[0]),
            half(NZ, NX, 64, WX[0]),
            half(NZ, NX, 64, WZ[1]),
            half(NZ, NX, 64, WX[1]),
            half(NZ, NX, 64, WZ[2]),
            half(NZ, NX, 64, WB),
            vmem(4, 4, 256),
            half(128, 128),
            vmem(4, 256, 128),
            half(4, 256, 128),
            vmem(4, 256, 128),
            vmem(4, 256, 128),
            vmem(4, 256, 128),
            half(4, 256, 128),
            vmem(4, 256, 128),
            vmem(4, 128, 128),
            half(4, 144, 128),
            half(4, 144, 128),
            half(144, 128),
            half(NZ, 144, 128),
            half(4, 128, 128),
            half(4, 128, 128),
            half(4, 384, 128),
            half(4, 16, 128),
            half(4, 16, 128),
            half(4, 256, 128),
            half(4, 256, 128),
            half(8, 256, 128),
            half(256, 2048),
            half(128, 2048),
            vmem(4, 256, 1),
            half(4, 128, 128),
            vmem(4, 128, 128),
            half(2, 256, 256),
            vmem(256, 2048),
            vmem(16, 128),
            *[half(16, 512)] * 5,
            vmem(1, 512),
            *[half(16, 512)] * 2,
            vmem(4, 128),
            vmem(1, 128),
            half(4, 16, 256),
            half(4, 16, 128),
            half(4, 16, 256),
            half(16, 512),
            pltpu.SemaphoreType.DMA((NSEND + NLONG + 3,)),
            pltpu.SemaphoreType.DMA((NRECV,)),
            pltpu.SemaphoreType.DMA((15,)),
        ],
        compiler_params=pltpu.CompilerParams(
            collective_id=0, has_side_effects=True, vmem_limit_bytes=48 * 1024 * 1024
        ),
    )(
        *[pltpu.with_memory_space_constraint(a, pltpu.HBM) for a in (
        tokens[0],
        norm_gain.reshape(16, 128),
        query_weight,
        forget_weight,
        value_weight,
        outgate_weight,
        pool_in_weight,
        forget_room.reshape(4, 128),
        decay_shift[0].T,
        head_gain.reshape(1, 128),
        start_state,
        pool_map,
        pool_scale.reshape(1, 512),
        out_rec_weight.T,
        out_pool_weight.T,
    )]
    )
    return mixed[None]


def solution(mesh):
    finer = Mesh(
        mesh.devices.reshape(8, 4, mesh.shape["fs"], mesh.shape["tp"]), ("sp_0", "sp_1", "fs", "tp")
    )
    placed = (
        P("fs", SP, "tp"),
        P(),
        P(SP_FS, "tp"),
        P(SP_FS, "tp"),
        P(SP_FS, "tp"),
        P(SP_FS, "tp"),
        P(SP_FS, "tp"),
        P("tp"),
        P("fs", SP, "tp"),
        P(),
        P("fs", "tp", None, None),
        P("tp", None, None),
        P("tp"),
        P("tp", SP_FS),
        P("tp", SP_FS),
    )
    return jax.shard_map(
        per_device, mesh=finer, in_specs=placed, out_specs=P("fs", SP_TP, None), check_vma=False
    )
```
